32 devices in a mesh: ep: 8 (over z, core), tp: 4 (over y, x).
Axes of the slice: x: 2, y: 2, z: 4, core: 2. Of those that a mesh axis runs over, the one named last changes fastest.
Arguments:
- first_batch_queries: bfloat16 [2048, 1024], P('ep', 'tp'), may hold values from -6 to 6
- first_batch_keys: bfloat16 [2048, 1024], P('ep', 'tp'), may hold values from -6 to 6
- first_batch_values: bfloat16 [2048, 2048], P('ep', 'tp'), may hold values from -6 to 6
- output_gate_preactivation: bfloat16 [2048, 2048], P('ep', 'tp'), may hold values from -6 to 6
- decay_preactivation: bfloat16 [2048, 1024], P('ep', 'tp'), may hold values from -6 to 6
- channel_decay_bias: float32 [1024], P('tp')
- added_log_decay: float32 [16, 2048], P('tp', 'ep'), may hold values from -0.7 to 0
- head_norm_gain: float32 [2048], P('tp'), may hold values from 0.1 to 1.9
- attention_output_weight: bfloat16 [2048, 2048], P(None, 'tp'), may hold values from -0.125 to 0.125
- second_batch_rows: bfloat16 [768, 2048], P('ep'), may hold values from -6 to 6
- expert_norm_gain: float32 [2048], replicated, may hold values from 0.1 to 1.9
- routed_expert_index: int32 [768, 4], P('ep'), may hold values from 0 to 7, all different within a row; in each aligned block of 96 rows (0 to 95, 96 to 191, ...) at most 72 rows name the same one
- router_chosen_scores: float32 [768, 4], P('ep'), may hold values from 0.1 to 1
- expert_gate_weight: bfloat16 [8, 2048, 4096], P('ep', None, 'tp'), may hold values from -0.125 to 0.125
- expert_up_weight: bfloat16 [8, 2048, 4096], P('ep', None, 'tp'), may hold values from -0.125 to 0.125
- expert_down_weight: bfloat16 [8, 4096, 2048], P('ep', None, 'tp'), may hold values from -0.09375 to 0.09375
- shared_gate_weight: bfloat16 [2048, 1024], P(None, 'tp'), may hold values from -0.125 to 0.125
- shared_up_weight: bfloat16 [2048, 1024], P(None, 'tp'), may hold values from -0.125 to 0.125
- shared_down_weight: bfloat16 [1024, 2048], P(None, 'tp'), may hold values from -0.1875 to 0.1875
Outputs:
- token_mixed: bfloat16 [2048, 2048], P('ep', 'tp')
- channel_mixed: bfloat16 [768, 2048], P('ep', 'tp')
The draws below stay inside these ranges and needn't reach their ends.
Inputs may be any that keep to these rules, and one draw needn't show every extreme that they name: `routed_expert_index`: in each aligned block of 96 rows (the rows of one index of ep) no expert is named by more than 72 rows, a bound that some block reaches; a row names 4 different experts.
All inputs are finite; a program needn't handle non-finite values.
Results may differ from the reference program's by a relative error of at most 0.018.
Values may be sent and summed in bfloat16 or wider, within the bound.
No kernel may reach another device: no remote copies, remote signals or barrier semaphores. Data moves between devices by JAX's collectives and lax.ppermute only.
A program may use at most 64 MiB of HBM per device.

```python
import math
from functools import partial
import jax
import jax.numpy as jnp
import numpy as np
from jax import lax

D = 2048
ATTENTION_HEADS = 16
DK = 64
DV = 128
BLOCK = 64
FFE = 4096
FFS = 1024
TOPK = 4
TOK_A = 256
TOK_B = 96
FIRST_TOKENS = 2048
TOKENS_B = 768
EXPERTS = 8
CAP = 72


def draw_channel_decay_bias(key, part):
    key_kind, key_slow, key_fast = jax.random.split(jax.random.fold_in(key, 11), 3)
    share = 0.5
    slow_head = jax.random.uniform(key_kind, (ATTENTION_HEADS, 1), jnp.float32) < share
    slow_level = math.log(0.34 * FIRST_TOKENS) + jax.random.uniform(key_slow, (ATTENTION_HEADS, DK), jnp.float32, -0.5, 0.5)
    fast_level = jax.random.uniform(key_fast, (ATTENTION_HEADS, DK), jnp.float32, -1.0, 1.5)
    return jnp.where(slow_head, slow_level, fast_level).reshape(ATTENTION_HEADS * DK).astype(jnp.float32)


def draw_added_log_decay(key, part):
    key_rate, key_locations, key_dimension = jax.random.split(jax.random.fold_in(key, 23), 3)
    devices = FIRST_TOKENS // TOK_A
    device_rates = jnp.exp(jax.random.uniform(key_rate, (devices,), jnp.float32, math.log(0.1), math.log(1.0))) / FIRST_TOKENS
    baseline_log_decay = -jnp.repeat(device_rates, TOK_A)
    position_index = jnp.arange(FIRST_TOKENS, dtype=jnp.int32)
    half_length = FIRST_TOKENS // 2
    halves_start = jnp.array([0, half_length], dtype=jnp.int32)
    spike_positions = jax.random.randint(key_locations, (ATTENTION_HEADS, 2), 0, half_length) + halves_start[None, :]
    spike_magnitude = jnp.log(jax.random.uniform(key_dimension, (ATTENTION_HEADS, 2), jnp.float32, 0.5, 0.8))
    decay_spikes = jnp.sum(jnp.where(position_index[None, None, :] == spike_positions[:, :, None], spike_magnitude[:, :, None], 0.0), axis=1)
    return (baseline_log_decay[None, :] + decay_spikes).astype(jnp.float32)


def block_scale(rng, shape, cuts, low, top_value):
    gain, own = 1.0, jax.random.fold_in(rng, 6)
    for dim, parts in cuts:
        steps = jnp.exp(jax.random.uniform(jax.random.fold_in(own, dim), (parts,), jnp.float32, low / len(cuts), top_value / len(cuts)))
        gain = gain * jnp.repeat(steps, shape[dim] // parts).reshape([-1 if axis == dim else 1 for axis in range(len(shape))])
    return gain


def shared_out(key, own, number, rows, amount, top, bound, slope):
    sequence = jax.random.permutation(key, amount)
    heavy_load, ordinary = load_shares(amount, rows * top, bound, slope, True), load_shares(amount, rows * top, bound, slope, False)
    places = jnp.arange(amount)

    def named(lengths, rotation):
        used = int((lengths > 0).sum())
        fixed = max(1, used // 4)
        shifted = fixed + (places - fixed + rotation * (used - fixed)) % max(1, amount - fixed)
        return jnp.zeros((amount,), jnp.int32).at[sequence[jnp.where(places < fixed, places, shifted)]].set(jnp.asarray(lengths, jnp.int32))

    lengths = jnp.where(number % 4 == 0, named(heavy_load, number // 4), named(ordinary, number - number // 4 - 1))
    mixed = jax.random.permutation(jax.random.fold_in(own, 3), amount)
    source_of, receiver = mixed[0:amount // 2 * 2:2], mixed[1:amount // 2 * 2:2]
    room = jnp.minimum(lengths[source_of] - 1, bound - lengths[receiver]) // 2
    room = jnp.where((source_of == sequence[0]) | (receiver == sequence[0]) | (lengths[receiver] == 0), 0, jnp.maximum(room, 0))
    shifted = jax.random.randint(jax.random.fold_in(own, 4), (amount // 2,), 0, 1 << 20) % (room + 1)
    lengths = lengths.at[source_of].add(-shifted).at[receiver].add(shifted)
    labels = jnp.searchsorted(jnp.cumsum(lengths), jnp.arange(rows * top), side="right").astype(jnp.int32)
    table = labels.reshape(top, rows).T
    table = table[jax.random.permutation(jax.random.fold_in(own, 1), rows)]
    rotation = jax.random.randint(jax.random.fold_in(own, 2), (rows, 1), 0, top)
    return jnp.take_along_axis(table, (jnp.arange(top)[None, :] + rotation) % top, axis=1)


def load_shares(count, total, reach, skew, full):
    weights = [(1 << 20) // math.isqrt(grade ** skew) + 1 for grade in range(1, count + 1)]
    largest = reach if full else min(reach, max(-(-total // count), total * weights[0] // sum(weights)))
    least = 1 if total - largest >= count - 1 else 0
    counts, surplus = [largest] + [least] * (count - 1), total - largest - least * (count - 1)
    while surplus > 0:
        candidates = [i for i in range(1, count) if counts[i] < largest] or [i for i in range(1, count) if counts[i] < reach]
        whole, budget = sum([weights[i] for i in candidates]), surplus
        for i in candidates:
            extra = min(reach - counts[i], max(1, budget * weights[i] // whole), surplus)
            counts[i] = counts[i] + extra
            surplus = surplus - extra
    return np.array(counts)


def normal_values(key, dims, deviation, limit, pieces=(), kind=jnp.bfloat16):
    values = deviation * jax.random.normal(key, dims, jnp.float32)
    if pieces:
        values = values * block_scale(key, dims, pieces, -0.22, 0.18)
    return jnp.clip(values, -limit, limit).astype(kind)


def setup_inputs(seed: int = 0) -> dict:
    streams_of = jax.random.split(jax.random.key(seed), 20)
    first_batch_queries = normal_values(streams_of[0], (FIRST_TOKENS, ATTENTION_HEADS * DK), 1.0, 6.0, ((0, 8), (1, 4)))
    first_batch_keys = normal_values(streams_of[1], (FIRST_TOKENS, ATTENTION_HEADS * DK), 1.0, 6.0, ((0, 8), (1, 4)))
    first_batch_values = normal_values(streams_of[2], (FIRST_TOKENS, ATTENTION_HEADS * DV), 1.0, 6.0, ((0, 8), (1, 4)))
    output_gate_preactivation = normal_values(streams_of[3], (FIRST_TOKENS, ATTENTION_HEADS * DV), 1.0, 6.0, ((0, 8), (1, 4)))
    decay_preactivation = normal_values(streams_of[4], (FIRST_TOKENS, ATTENTION_HEADS * DK), 1.0, 6.0, ((0, 8), (1, 4)))
    channel_decay_bias = draw_channel_decay_bias(jax.random.fold_in(streams_of[19], 71), 0)
    added_log_decay = draw_added_log_decay(jax.random.fold_in(streams_of[19], 71), 0)
    head_norm_gain = jnp.clip(1.0 + 0.18 * jax.random.normal(streams_of[7], (ATTENTION_HEADS * DV,), jnp.float32), 0.1, 1.9)
    attention_output_weight = normal_values(streams_of[8], (ATTENTION_HEADS * DV, D), (ATTENTION_HEADS * DV) ** -0.5, 0.125, ((1, 4),))
    second_batch_rows = normal_values(streams_of[9], (TOKENS_B, D), 1.0, 6.0, ((0, 8),))
    expert_norm_gain = jnp.clip(1.0 + 0.18 * jax.random.normal(streams_of[10], (D,), jnp.float32), 0.1, 1.9)
    routed_expert_index_keys = jax.random.split(jax.random.fold_in(streams_of[11], 1), TOKENS_B // TOK_B)
    routed_expert_index_turns = jax.random.permutation(jax.random.fold_in(streams_of[11], 3), TOKENS_B // TOK_B)
    routed_expert_index = jax.vmap(lambda own, number: shared_out(jax.random.fold_in(streams_of[11], 2), own, number, TOK_B, EXPERTS, TOPK, CAP, 1))(routed_expert_index_keys, routed_expert_index_turns).reshape((TOKENS_B, TOPK))
    router_chosen_scores = jnp.clip(jnp.exp(math.log(1.0) - 2.3025851 * jax.random.uniform(streams_of[12], (TOKENS_B, TOPK), jnp.float32) ** block_scale(streams_of[12], (TOKENS_B, TOPK), ((0, 8),), -0.2, 0.2)), 0.1, 1.0)
    expert_gate_weight = normal_values(streams_of[13], (EXPERTS, D, FFE), D ** -0.5, 0.125, ((0, 8), (2, 4)))
    expert_up_weight = normal_values(streams_of[14], (EXPERTS, D, FFE), D ** -0.5, 0.125, ((0, 8), (2, 4)))
    expert_down_weight = normal_values(streams_of[15], (EXPERTS, FFE, D), FFE ** -0.5, 0.09375, ((0, 8), (2, 4)))
    shared_gate_weight = normal_values(streams_of[16], (D, FFS), D ** -0.5, 0.125, ((1, 4),))
    shared_up_weight = normal_values(streams_of[17], (D, FFS), D ** -0.5, 0.125, ((1, 4),))
    shared_down_weight = normal_values(streams_of[18], (FFS, D), FFS ** -0.5, 0.1875, ((1, 4),))
    return {"first_batch_queries": first_batch_queries, "first_batch_keys": first_batch_keys, "first_batch_values": first_batch_values, "output_gate_preactivation": output_gate_preactivation, "decay_preactivation": decay_preactivation, "channel_decay_bias": channel_decay_bias, "added_log_decay": added_log_decay, "head_norm_gain": head_norm_gain, "attention_output_weight": attention_output_weight, "second_batch_rows": second_batch_rows, "expert_norm_gain": expert_norm_gain, "routed_expert_index": routed_expert_index, "router_chosen_scores": router_chosen_scores, "expert_gate_weight": expert_gate_weight, "expert_up_weight": expert_up_weight, "expert_down_weight": expert_down_weight, "shared_gate_weight": shared_gate_weight, "shared_up_weight": shared_up_weight, "shared_down_weight": shared_down_weight}


epsilon = 1e-06
temper = 16.0
routed_scale = 2.5
largest_value = lax.Precision.HIGHEST

def head_norm(tensor, gain_rows):
    mean_square = lax.optimization_barrier(jnp.mean(tensor * tensor, axis=-1, keepdims=True))
    return tensor * lax.rsqrt(mean_square + epsilon) * gain_rows

def log_decay_values(decay_preactivation, channel_decay_bias, added_log_decay):
    number_of_heads = added_log_decay.shape[0]
    row_count = decay_preactivation.shape[0]
    logits = decay_preactivation.astype(jnp.float32) + channel_decay_bias[None, :]
    baseline_log_decay = (jax.nn.log_sigmoid(logits) / temper).reshape(row_count, number_of_heads, -1)
    return baseline_log_decay + jnp.transpose(added_log_decay)[:, :, None]

def gated_linear(queries, keys_all, values, decay_factors):
    row_count, number_of_heads, key_channel_width = queries.shape
    value_width = values.shape[-1]
    block_count = row_count // BLOCK

    def split_into_blocks(tensor):
        return tensor.reshape(block_count, BLOCK, number_of_heads, tensor.shape[-1]).transpose(0, 2, 1, 3)
    lower_mask = jnp.tril(jnp.ones((BLOCK, BLOCK), bool))

    def advance(carry_state, inputs):
        query_block, block_of_keys, block_of_values, decay_block = inputs
        running_state = jnp.cumsum(decay_block, axis=1)
        query_decayed = query_block * jnp.exp(running_state)
        key_raised = block_of_keys * jnp.exp(-running_state)
        attention_scores = jnp.einsum('hqd,hkd->hqk', query_decayed, key_raised, precision=largest_value)
        attention_scores = jnp.where(lower_mask, attention_scores, 0.0)
        within_block = jnp.einsum('gnx,gxy->gny', attention_scores, block_of_values, precision=largest_value)
        carried = jnp.einsum('hqd,hdv->hqv', query_decayed, carry_state, precision=largest_value)
        block_number_total = running_state[:, -1:, :]
        state_update = jnp.einsum('ien,ieg->ing', block_of_keys * jnp.exp(block_number_total - running_state), block_of_values, precision=largest_value)
        new_state = jnp.exp(block_number_total[:, 0, :])[..., None] * carry_state + state_update
        return (new_state, within_block + carried)
    start_state = jnp.zeros((number_of_heads, key_channel_width, value_width), jnp.float32)
    _, outputs = lax.scan(advance, start_state, (split_into_blocks(queries), split_into_blocks(keys_all), split_into_blocks(values), split_into_blocks(decay_factors)))
    return outputs.transpose(0, 2, 1, 3).reshape(row_count, number_of_heads, value_width)

def expert_slots(route_rows, experts, capacity):
    flat_ids = route_rows.reshape(-1)
    targets = jnp.arange(experts, dtype=jnp.int32)
    onehot = (flat_ids[:, None] == targets[None, :]).astype(jnp.int32)
    earlier = jnp.cumsum(onehot, axis=0) - onehot
    return (flat_ids * capacity + lax.optimization_barrier(jnp.sum(earlier * onehot, axis=1))).astype(jnp.int32)

def slot_owner(slot_ids, slot_count, top_count):
    matches = slot_ids[None, :] == jnp.arange(slot_count, dtype=jnp.int32)[:, None]
    token_ids = jnp.arange(slot_ids.shape[0], dtype=jnp.int32) // top_count
    return (lax.optimization_barrier(jnp.sum(jnp.where(matches, token_ids[None, :] + 1, 0), axis=1)) - 1).astype(jnp.int32)

def reference(first_batch_queries, first_batch_keys, first_batch_values, output_gate_preactivation, decay_preactivation, channel_decay_bias, added_log_decay, head_norm_gain, attention_output_weight, second_batch_rows, expert_norm_gain, routed_expert_index, router_chosen_scores, expert_gate_weight, expert_up_weight, expert_down_weight, shared_gate_weight, shared_up_weight, shared_down_weight):
    decay_factors = log_decay_values(decay_preactivation, channel_decay_bias, added_log_decay)
    queries = first_batch_queries.astype(jnp.float32).reshape(FIRST_TOKENS, ATTENTION_HEADS, DK)
    keys_all = first_batch_keys.astype(jnp.float32).reshape(FIRST_TOKENS, ATTENTION_HEADS, DK)
    values = first_batch_values.astype(jnp.float32).reshape(FIRST_TOKENS, ATTENTION_HEADS, DV)
    head_values = gated_linear(queries, keys_all, values, decay_factors)
    gate_rows = jax.nn.silu(output_gate_preactivation.astype(jnp.float32)).reshape(FIRST_TOKENS, ATTENTION_HEADS, DV)
    mixed_heads = head_norm(head_values, head_norm_gain.reshape(ATTENTION_HEADS, DV)) * gate_rows
    mixed_heads = mixed_heads.reshape(FIRST_TOKENS, ATTENTION_HEADS * DV).astype(jnp.bfloat16)
    token_mixed = jnp.dot(mixed_heads, attention_output_weight, preferred_element_type=jnp.float32).astype(jnp.bfloat16)
    features = second_batch_rows.astype(jnp.float32)
    normed = features * lax.rsqrt(lax.optimization_barrier(jnp.mean(features * features, axis=1, keepdims=True)) + epsilon)
    normed = (normed * expert_norm_gain[None, :]).astype(jnp.bfloat16)
    sources = TOKENS_B // TOK_B
    slot_count = EXPERTS * CAP
    block_routes = routed_expert_index.reshape(sources, TOK_B, TOPK)
    slot_ids = jax.vmap(partial(expert_slots, experts=EXPERTS, capacity=CAP))(block_routes)
    owners = jax.vmap(partial(slot_owner, slot_count=slot_count, top_count=TOPK))(slot_ids)
    offsets = (jnp.arange(sources, dtype=jnp.int32) * TOK_B)[:, None]
    global_owner = jnp.where(owners >= 0, owners + offsets, -1)
    per_expert = global_owner.reshape(sources, EXPERTS, CAP).transpose(1, 0, 2).reshape(EXPERTS, sources * CAP)

    def run_expert(inputs):
        owner_rows, gate_weight, up_weight, down_weight = inputs
        picked_rows = jnp.take(normed, jnp.maximum(owner_rows, 0), axis=0)
        rows_in = jnp.where((owner_rows >= 0)[:, None], picked_rows, jnp.zeros((), jnp.bfloat16))
        gate_value = jnp.dot(rows_in, gate_weight, preferred_element_type=jnp.float32)
        up_value = jnp.dot(rows_in, up_weight, preferred_element_type=jnp.float32)
        hidden = (jax.nn.silu(gate_value) * up_value).astype(jnp.bfloat16)
        return jnp.dot(hidden, down_weight, preferred_element_type=jnp.float32).astype(jnp.bfloat16)
    results = lax.map(run_expert, (per_expert, expert_gate_weight, expert_up_weight, expert_down_weight))
    expert_ids = block_routes.reshape(sources, -1)
    source_ids = jnp.arange(sources, dtype=jnp.int32)[:, None]
    flat_index = expert_ids * (sources * CAP) + source_ids * CAP + (slot_ids - expert_ids * CAP)
    picked = jnp.take(results.reshape(-1, D), flat_index.reshape(-1).astype(jnp.int32), axis=0)
    picked = picked.astype(jnp.float32).reshape(TOKENS_B, TOPK, D)
    weights = routed_scale * router_chosen_scores / lax.optimization_barrier(jnp.sum(router_chosen_scores, axis=1, keepdims=True))
    shared_gate_value = jnp.dot(normed, shared_gate_weight, preferred_element_type=jnp.float32)
    shared_up_value = jnp.dot(normed, shared_up_weight, preferred_element_type=jnp.float32)
    shared_hidden = (jax.nn.silu(shared_gate_value) * shared_up_value).astype(jnp.bfloat16)
    shared_total = jnp.dot(shared_hidden, shared_down_weight, preferred_element_type=jnp.float32)
    channel_mixed = (lax.optimization_barrier(jnp.sum(weights[:, :, None] * picked, axis=1)) + shared_total).astype(jnp.bfloat16)
    return (token_mixed, channel_mixed)
```

```python
import math

import jax
import jax.numpy as jnp
from jax import lax
from jax.sharding import PartitionSpec as P


BLOCK = 64
epsilon = 1e-06
temper = 16.0
routed_scale = 2.5
highest = lax.Precision.HIGHEST
f32 = jnp.float32
bf16 = jnp.bfloat16
AXES = ("ep", "tp")


class Places:
    def __init__(self):
        self.ep, self.tp = lax.axis_size("ep"), lax.axis_size("tp")
        self.side = math.isqrt(self.tp)
        self.chips = self.ep // 2
        assert self.side * self.side == self.tp and self.chips * 2 == self.ep
        e, j = lax.axis_index("ep"), lax.axis_index("tp")
        self.e, self.j = e, j
        self.z, self.c = e // 2, e % 2
        self.y, self.x = j // self.side, j % self.side
        self.u = jnp.where(self.c == 0, self.x, self.y)
        self.v = jnp.where(self.c == 0, self.y, self.x)

    def column(self, u, v):
        n = self.side
        u, v = u % n, v % n
        return jnp.where(self.c == 0, v * n + u, u * n + v)

    def pairs(self, move):
        n = self.side
        out = []
        for e in range(self.ep):
            for j in range(self.tp):
                z, c, y, x = move(e // 2, e % 2, j // n, j % n)
                if 0 <= z < self.chips:
                    out.append((e * self.tp + j, (z * 2 + c) * self.tp + (y % n) * n + x % n))
        return out

    def send(self, value, move):
        return lax.ppermute(value, AXES, self.pairs(move))

    def along_z(self, value, k):
        return self.send(value, lambda z, c, y, x: ((z + k) % self.chips, c, y, x))

    def up_z(self, value, k):
        return self.send(value, lambda z, c, y, x: (z + k, c, y, x))

    def to_sibling(self, value):
        return self.send(value, lambda z, c, y, x: (z, 1 - c, y, x))

    def along_u(self, value, k):
        return self.send(value, lambda z, c, y, x: (z, c, y, x + k) if c == 0 else (z, c, y + k, x))

    def along_v(self, value, k):
        return self.send(value, lambda z, c, y, x: (z, c, y + k, x) if c == 0 else (z, c, y, x + k))

    def along_tp(self, value, dy, dx):
        return self.send(value, lambda z, c, y, x: (z, c, y + dy, x + dx))


def log_decay_values(decay_preactivation, channel_decay_bias, added_log_decay):
    heads, rows = added_log_decay.shape
    logits = decay_preactivation.astype(f32) + channel_decay_bias[None, :]
    base = (jax.nn.log_sigmoid(logits) / temper).reshape(rows, heads, -1)
    return base + jnp.transpose(added_log_decay)[:, :, None]


def mixer_heads(at, q, k, v, gate_pre, decay_pre, decay_bias, added, gain):
    heads, rows = added.shape
    dk = q.shape[1] // heads
    dv = v.shape[1] // heads
    blocks = rows // BLOCK

    def split(tensor, width):
        return tensor.astype(f32).reshape(blocks, BLOCK, heads, width).transpose(0, 2, 1, 3)

    queries, keys, values = split(q, dk), split(k, dk), split(v, dv)
    decay = split(log_decay_values(decay_pre, decay_bias, added), dk)
    lower = jnp.tril(jnp.ones((BLOCK, BLOCK), f32))
    running = jnp.einsum("ij,nhjd->nhid", lower, decay, precision=highest)
    total = running[:, :, -1, :]
    query_decayed = queries * jnp.exp(running)
    key_raised = keys * jnp.exp(-running)
    scores = jnp.einsum("nhqd,nhkd->nhqk", query_decayed, key_raised, precision=highest)
    scores = jnp.where(lower > 0, scores, 0.0)
    within = jnp.einsum("nhqk,nhkv->nhqv", scores, values, precision=highest)
    updates = jnp.einsum(
        "nhkd,nhkv->nhdv", keys * jnp.exp(total[:, :, None, :] - running), values, precision=highest
    )
    state = updates[0]
    before = [jnp.zeros_like(state)]
    for b in range(1, blocks):
        before.append(state)
        state = jnp.exp(total[b])[..., None] * state + updates[b]
    before = jnp.stack(before)
    device_log = jnp.sum(total, axis=0)
    sibling_state = at.to_sibling(state.astype(bf16)).astype(f32)
    sibling_log = at.to_sibling(device_log)
    first = at.c == 0
    chip_state = jnp.where(
        first,
        jnp.exp(sibling_log)[..., None] * state + sibling_state,
        jnp.exp(device_log)[..., None] * sibling_state + state,
    ).astype(bf16)
    chip_log = device_log + sibling_log
    incoming = jnp.zeros_like(state)
    between = jnp.zeros_like(device_log)
    for hop in range(1, at.chips):
        inside = at.z >= hop
        got_state = at.up_z(chip_state, hop)
        got_log = at.up_z(chip_log, hop)
        incoming = incoming + jnp.where(
            inside, jnp.exp(between)[..., None] * got_state.astype(f32), 0.0
        )
        between = between + jnp.where(inside, got_log, 0.0)
    incoming = jnp.where(
        first, incoming, jnp.exp(sibling_log)[..., None] * incoming + sibling_state
    )
    lead_in = jnp.exp(jnp.cumsum(total, axis=0) - total)
    states = before + lead_in[..., None] * incoming[None]
    carried = jnp.einsum("nhqd,nhdv->nhqv", query_decayed, states, precision=highest)
    head_values = (within + carried).transpose(0, 2, 1, 3).reshape(rows, heads, dv)
    gate = jax.nn.silu(gate_pre.astype(f32)).reshape(rows, heads, dv)
    mean_square = jnp.mean(head_values * head_values, axis=-1, keepdims=True)
    mixed = head_values * lax.rsqrt(mean_square + epsilon) * gain.reshape(heads, dv) * gate
    return mixed.reshape(rows, heads * dv).astype(bf16)


def routing_rows(index, scores, experts, width):
    tokens = index.shape[0]
    targets = jnp.arange(experts, dtype=jnp.int32)
    hit = index[:, :, None] == targets[None, None, :]
    weights = routed_scale * scores / jnp.sum(scores, axis=1, keepdims=True)
    named = jnp.any(hit, axis=1)
    weight = jnp.sum(jnp.where(hit, weights[:, :, None], 0.0), axis=1)
    strict = jnp.triu(jnp.ones((tokens, tokens), bf16), 1)
    earlier = lax.dot_general(
        named.astype(bf16), strict, (((0,), (0,)), ((), ())), preferred_element_type=f32
    )
    ranks = jnp.where(named.T, earlier, -1.0).astype(bf16)
    lanes = -(-tokens // 128) * 128
    ranks = jnp.pad(ranks, ((0, 0), (0, lanes - tokens)))
    table = jnp.concatenate([ranks, weight.T.astype(bf16)], axis=1)
    return jnp.pad(table, ((0, -experts % 8), (0, width - table.shape[1]))), lanes


def dot(a, b):
    return jnp.dot(a, b, preferred_element_type=f32)


def local(
    first_batch_queries,
    first_batch_keys,
    first_batch_values,
    output_gate_preactivation,
    decay_preactivation,
    channel_decay_bias,
    added_log_decay,
    head_norm_gain,
    attention_output_weight,
    second_batch_rows,
    expert_norm_gain,
    routed_expert_index,
    router_chosen_scores,
    expert_gate_weight,
    expert_up_weight,
    expert_down_weight,
    shared_gate_weight,
    shared_up_weight,
    shared_down_weight,
):
    at = Places()
    n, chips, experts = at.side, at.chips, at.ep
    tokens, top_count = routed_expert_index.shape
    capacity = tokens * top_count * 3 // (2 * experts)
    width = second_batch_rows.shape[1]
    gate_weight, up_weight, down_weight = (
        expert_gate_weight[0],
        expert_up_weight[0],
        expert_down_weight[0],
    )
    hidden = gate_weight.shape[1]
    columns = down_weight.shape[1]

    def down_rows(k):
        return jnp.concatenate(
            [
                lax.dynamic_slice_in_dim(down_weight, at.column(at.u - i, at.v + k) * hidden, hidden, 0)
                for i in range(n)
            ],
            axis=0,
        )

    features = second_batch_rows.astype(f32)
    normed = features * lax.rsqrt(jnp.mean(features * features, axis=1, keepdims=True) + epsilon)
    normed = (normed * expert_norm_gain[None, :]).astype(bf16)
    part = width // n
    mine = (at.x + at.y) % n
    table, lanes = routing_rows(routed_expert_index, router_chosen_scores, experts, part)
    extra = table.shape[0]
    own_part = lax.dynamic_slice_in_dim(normed, mine * part, part, 1)
    packed = jnp.concatenate([own_part, table], axis=0)
    far = [at.along_z(packed, k) for k in range(1, chips)]
    far_rows = jnp.concatenate([a[:tokens] for a in far], axis=0)
    far_tables = [a[tokens:] for a in far]
    traded = [at.along_v(down_rows(k), k) for k in range(1, n)]
    pieces = jnp.stack([far_rows] + [at.along_u(far_rows, i) for i in range(1, n)])
    ordered = [
        lax.dynamic_index_in_dim(pieces, (mine - q) % n, 0, keepdims=False) for q in range(n)
    ]
    rows_here = jnp.concatenate(
        [normed, jnp.concatenate(ordered, axis=1)], axis=0
    )
    tables_here = jnp.concatenate([table] + far_tables, axis=0)[:, : 2 * lanes]
    rows_there = at.to_sibling(rows_here)
    tables_there = at.to_sibling(tables_here)
    rows_all = jnp.concatenate([rows_here, rows_there], axis=0).reshape(2 * chips, tokens, width)
    tables_all = jnp.concatenate([tables_here, tables_there], axis=0).reshape(
        2 * chips, extra, 2 * lanes
    )
    mine_rows = lax.dynamic_index_in_dim(tables_all, at.e, 1, keepdims=False)
    ranks = mine_rows[:, :tokens].astype(f32)
    weights = mine_rows[:, lanes : lanes + tokens]
    slots = lax.broadcasted_iota(f32, (2 * chips, capacity, tokens), 1)
    picks = ranks[:, None, :] == slots
    section = jnp.einsum(
        "sct,std->scd", picks.astype(bf16), rows_all, preferred_element_type=f32
    ).astype(bf16)
    section = section.reshape(2 * chips * capacity, width)
    gate_value = dot(section, gate_weight)
    up_value = dot(section, up_weight)
    routed_hidden = (jax.nn.silu(gate_value) * up_value).astype(bf16)
    gathered = jnp.concatenate(
        [routed_hidden] + [at.along_u(routed_hidden, i) for i in range(1, n)], axis=1
    )
    own = dot(gathered, down_rows(0))
    partial = [dot(gathered, traded[k - 1]).astype(bf16) for k in range(1, n)]
    back = [at.along_v(partial[k - 1], -k) for k in range(1, n)]
    for piece in back:
        own = own + piece.astype(f32)
    own = own.astype(bf16).reshape(2 * chips, capacity, columns)
    places = jnp.where(picks, weights[:, None, :], jnp.zeros((), bf16))
    dense = jnp.einsum("sct,scd->std", places, own, preferred_element_type=f32)
    from_sibling = at.to_sibling(dense[chips:].astype(bf16))
    chip_sum = dense[:chips] + from_sibling.astype(f32)
    routed_total = chip_sum[0]
    for k in range(1, chips):
        routed_total = routed_total + at.along_z(chip_sum[k].astype(bf16), -k).astype(f32)

    shared_hidden = (
        jax.nn.silu(dot(normed, shared_gate_weight)) * dot(normed, shared_up_weight)
    ).astype(bf16)
    mixed = mixer_heads(
        at,
        first_batch_queries,
        first_batch_keys,
        first_batch_values,
        output_gate_preactivation,
        decay_preactivation,
        channel_decay_bias,
        added_log_decay,
        head_norm_gain,
    )
    half = tokens // 2
    sharing = mixed.shape[1] // shared_hidden.shape[1]
    folded = jnp.concatenate(
        [
            shared_hidden[i * (tokens // sharing) : (i + 1) * (tokens // sharing)]
            for i in range(sharing)
        ],
        axis=1,
    )
    both = jnp.concatenate([mixed, folded], axis=0)
    mixer_rows = mixed.shape[0]
    mixer_total = jnp.zeros((mixer_rows, columns), f32)
    shared_total = jnp.zeros((tokens, columns), f32)
    for dy in range(n):
        for dx in range(n):
            got = both if dy == 0 and dx == 0 else at.along_tp(both, dy, dx)
            source = ((at.y - dy) % n) * n + (at.x - dx) % n
            weight = lax.dynamic_slice_in_dim(
                attention_output_weight, source * got.shape[1], got.shape[1], 0
            )
            mixer_total = mixer_total + dot(got[:mixer_rows], weight)
            wide = shared_hidden.shape[1]
            part_hidden = jnp.concatenate(
                [got[mixer_rows:, i * wide : (i + 1) * wide] for i in range(sharing)], axis=0
            )
            weight = lax.dynamic_slice_in_dim(shared_down_weight, source * wide, wide, 0)
            shared_total = shared_total + dot(part_hidden, weight)
    token_mixed = mixer_total.astype(bf16)
    channel_mixed = (routed_total + shared_total).astype(bf16)
    return (token_mixed, channel_mixed)


def solution(mesh):
    placed = (
        P("ep", "tp"),
        P("ep", "tp"),
        P("ep", "tp"),
        P("ep", "tp"),
        P("ep", "tp"),
        P("tp"),
        P("tp", "ep"),
        P("tp"),
        P(None, "tp"),
        P("ep", None),
        P(),
        P("ep", None),
        P("ep", None),
        P("ep", None, "tp"),
        P("ep", None, "tp"),
        P("ep", None, "tp"),
        P(None, "tp"),
        P(None, "tp"),
        P(None, "tp"),
    )
    return jax.shard_map(
        local, mesh=mesh, in_specs=placed, out_specs=(P("ep", "tp"), P("ep", "tp")), check_vma=False
    )
```

```python
import math

import jax
import jax.numpy as jnp
from jax import lax
from jax.experimental import pallas as pl
from jax.experimental.pallas import tpu as pltpu
from jax.sharding import PartitionSpec as P


BLOCK = 64
epsilon = 1e-06
temper = 16.0
routed_scale = 2.5
highest = lax.Precision.HIGHEST
f32 = jnp.float32
bf16 = jnp.bfloat16
AXES = ("ep", "tp")


class Places:
    def __init__(self):
        self.ep, self.tp = lax.axis_size("ep"), lax.axis_size("tp")
        self.side = math.isqrt(self.tp)
        self.chips = self.ep // 2
        assert self.side * self.side == self.tp and self.chips * 2 == self.ep
        e, j = lax.axis_index("ep"), lax.axis_index("tp")
        self.e, self.j = e, j
        self.z, self.c = e // 2, e % 2
        self.y, self.x = j // self.side, j % self.side
        self.u = jnp.where(self.c == 0, self.x, self.y)
        self.v = jnp.where(self.c == 0, self.y, self.x)

    def column(self, u, v):
        n = self.side
        u, v = u % n, v % n
        return jnp.where(self.c == 0, v * n + u, u * n + v)

    def pairs(self, move):
        n = self.side
        out = []
        for e in range(self.ep):
            for j in range(self.tp):
                z, c, y, x = move(e // 2, e % 2, j // n, j % n)
                if 0 <= z < self.chips:
                    out.append((e * self.tp + j, (z * 2 + c) * self.tp + (y % n) * n + x % n))
        return out

    def send(self, value, move):
        return lax.ppermute(value, AXES, self.pairs(move))

    def along_z(self, value, k):
        return self.send(value, lambda z, c, y, x: ((z + k) % self.chips, c, y, x))

    def up_z(self, value, k):
        return self.send(value, lambda z, c, y, x: (z + k, c, y, x))

    def to_sibling(self, value):
        return self.send(value, lambda z, c, y, x: (z, 1 - c, y, x))

    def along_u(self, value, k):
        return self.send(value, lambda z, c, y, x: (z, c, y, x + k) if c == 0 else (z, c, y + k, x))

    def along_v(self, value, k):
        return self.send(value, lambda z, c, y, x: (z, c, y + k, x) if c == 0 else (z, c, y, x + k))

    def along_tp(self, value, dy, dx):
        return self.send(value, lambda z, c, y, x: (z, c, y + dy, x + dx))


def dot(a, b, precision=None):
    return jnp.dot(a, b, preferred_element_type=f32, precision=precision)


def dot_nt(a, b):
    return lax.dot_general(a, b, (((1,), (1,)), ((), ())), preferred_element_type=f32)


def dot_tn(a, b, precision=None):
    return lax.dot_general(
        a, b, (((0,), (0,)), ((), ())), preferred_element_type=f32, precision=precision
    )


def silu(value):
    return value / (1.0 + jnp.exp(-value))


def whole(count):
    return [pl.BlockSpec(memory_space=pltpu.VMEM)] * count


def scalars(*values):
    return jnp.stack([jnp.asarray(v, jnp.int32) for v in values])


def call(body, outs, operands, flops, smem=0):
    specs = [pl.BlockSpec(memory_space=pltpu.SMEM)] * smem + whole(len(operands) - smem)
    return pl.pallas_call(
        body,
        out_shape=outs,
        in_specs=specs,
        out_specs=jax.tree.map(lambda _: pl.BlockSpec(memory_space=pltpu.VMEM), outs),
        cost_estimate=pl.CostEstimate(flops=flops, transcendentals=0, bytes_accessed=0),
    )(*operands)


def local_attention(places, q, k, v, decay_pre, bias, added):
    heads, rows = added.shape
    dk, dv = q.shape[1] // heads, v.shape[1] // heads
    blocks = rows // BLOCK
    group = min(max(1, 128 // dk), heads)
    lanes = group * dk

    def body(q_ref, k_ref, v_ref, d_ref, bias_ref, added_ref, o_ref, qd_ref, pack_ref):
        spread = (
            lax.broadcasted_iota(jnp.int32, (heads, heads * dk), 1) // dk
            == lax.broadcasted_iota(jnp.int32, (heads, heads * dk), 0)
        ).astype(f32)
        logits = d_ref[...].astype(f32) + bias_ref[...]
        base = jnp.minimum(logits, 0.0) - jnp.log1p(jnp.exp(-jnp.abs(logits)))
        decay = base / temper + dot_tn(added_ref[...], spread, highest)
        row = lax.broadcasted_iota(jnp.int32, (BLOCK, BLOCK), 0)
        col = lax.broadcasted_iota(jnp.int32, (BLOCK, BLOCK), 1)
        lower = row >= col
        lower_f = lower.astype(f32)
        lane = lax.broadcasted_iota(jnp.int32, (1, lanes), 1)
        masks = [(lane // dk == g).astype(f32) for g in range(group)]
        states = [None] * heads
        lead = jnp.zeros((1, heads * dk), f32)
        for b in range(blocks):
            span = slice(b * BLOCK, (b + 1) * BLOCK)
            running = dot(lower_f, decay[span], highest)
            total = running[BLOCK - 1 : BLOCK, :]
            grow = jnp.exp(running)
            q_dec = q_ref[span, :].astype(f32) * grow
            keys = k_ref[span, :].astype(f32)
            k_up = (keys * jnp.exp(-running)).astype(bf16)
            k_end = (keys * jnp.exp(total - running)).astype(bf16)
            qd_ref[span, :] = (q_dec * jnp.exp(lead)).astype(bf16)
            shrink = jnp.exp(total)
            for h in range(heads):
                at = slice(h // group * lanes, h // group * lanes + lanes)
                q_h = (q_dec[:, at] * masks[h % group]).astype(bf16)
                v_h = v_ref[span, h * dv : (h + 1) * dv]
                scores = jnp.where(lower, dot_nt(q_h, k_up[:, at]), 0.0).astype(bf16)
                value = dot(scores, v_h)
                if b:
                    value = value + dot_nt(q_h, states[h].astype(bf16))
                o_ref[span, h * dv : (h + 1) * dv] = value
                update = dot_tn(v_h, k_end[:, at])
                states[h] = update if b == 0 else states[h] * shrink[:, at] + update
            lead = lead + total
        for h0 in range(0, heads, group):
            packed = states[h0]
            for g in range(1, group):
                packed = jnp.where(lane // dk == g, states[h0 + g], packed)
            pack_ref[0:dv, h0 * dk : h0 * dk + lanes] = packed.astype(bf16)
        pack_ref[dv : dv + 8, :] = jnp.broadcast_to(jnp.exp(lead), (8, heads * dk)).astype(bf16)

    outs = (
        jax.ShapeDtypeStruct((rows, heads * dv), f32),
        jax.ShapeDtypeStruct((rows, heads * dk), bf16),
        jax.ShapeDtypeStruct((dv + 8, heads * dk), bf16),
    )
    return call(body, outs, (q, k, v, decay_pre, bias[None, :], added), 1 << 25)


def chip_state(places, own, sibling, dv):
    def body(s_ref, own_ref, sib_ref, out_ref):
        first = s_ref[0] == 0
        own, sib = own_ref[...].astype(f32), sib_ref[...].astype(f32)
        early, late = jnp.where(first, own, sib), jnp.where(first, sib, own)
        decay = late[dv : dv + 1, :]
        out_ref[0:dv, :] = (early[0:dv] * decay + late[0:dv]).astype(bf16)
        out_ref[dv : dv + 8, :] = (early[dv : dv + 8] * decay).astype(bf16)

    out = jax.ShapeDtypeStruct(own.shape, bf16)
    return call(body, out, (scalars(places.c), own, sibling), 1 << 20, smem=1)


def finish_attention(places, local, qd, sibling, arrived, gate_pre, gain, heads):
    rows = local.shape[0]
    dv, dk = local.shape[1] // heads, qd.shape[1] // heads
    group = min(max(1, 128 // dk), heads)
    lanes = group * dk

    def body(s_ref, local_ref, qd_ref, sib_ref, gate_ref, gain_ref, *refs):
        out_ref = refs[-1]
        between = jnp.ones((1, heads * dk), f32)
        incoming = jnp.zeros((dv, heads * dk), f32)
        for hop, ref in enumerate(refs[:-1], 1):
            got = ref[...].astype(f32)
            inside = s_ref[0] >= hop
            incoming = incoming + jnp.where(inside, between * got[0:dv], 0.0)
            between = jnp.where(inside, between * got[dv : dv + 1], between)
        sib = sib_ref[...].astype(f32)
        incoming = jnp.where(
            s_ref[1] == 0, incoming, incoming * sib[dv : dv + 1] + sib[0:dv]
        ).astype(bf16)
        lane = lax.broadcasted_iota(jnp.int32, (1, lanes), 1)
        for h in range(heads):
            at = slice(h // group * lanes, h // group * lanes + lanes)
            vs = slice(h * dv, (h + 1) * dv)
            mask = lane // dk == h % group
            q_h = jnp.where(mask, qd_ref[:, at], jnp.zeros((), bf16))
            value = local_ref[:, vs] + dot_nt(q_h, incoming[:, at])
            mean_square = jnp.mean(value * value, axis=1, keepdims=True)
            value = value * lax.rsqrt(mean_square + epsilon) * gain_ref[:, vs]
            out_ref[:, vs] = (value * silu(gate_ref[:, vs].astype(f32))).astype(bf16)

    out = jax.ShapeDtypeStruct(local.shape, bf16)
    operands = (scalars(places.z, places.c), local, qd, sibling, gate_pre, gain[None, :], *arrived)
    return call(body, out, operands, 1 << 24, smem=1)


def prepare_rows(part, parts, rows, gain, index, scores, experts):
    tokens, width = rows.shape
    top = index.shape[1]
    piece = width // parts
    pad = -(-tokens // 128) * 128
    extra = -(-experts // 8) * 8

    def body(s_ref, rows_ref, gain_ref, index_ref, score_ref, normed_ref, packed_ref):
        value = rows_ref[...].astype(f32)
        mean_square = jnp.mean(value * value, axis=1, keepdims=True)
        normed = (value * lax.rsqrt(mean_square + epsilon) * gain_ref[...]).astype(bf16)
        normed_ref[...] = normed
        for q in range(parts):

            @pl.when(s_ref[0] == q)
            def _():
                packed_ref[0:tokens, :] = normed[:, q * piece : (q + 1) * piece]

        scores = score_ref[...]
        weights = routed_scale * scores / jnp.sum(scores, axis=0, keepdims=True)
        expert = lax.broadcasted_iota(jnp.int32, (extra, tokens), 0)
        named = jnp.zeros((extra, tokens), f32)
        weight = jnp.zeros((extra, tokens), f32)
        for k in range(top):
            hit = index_ref[k : k + 1, :] == expert
            named = jnp.where(hit, 1.0, named)
            weight = jnp.where(hit, weights[k : k + 1, :], weight)
        strict = (
            lax.broadcasted_iota(jnp.int32, (tokens, tokens), 0)
            < lax.broadcasted_iota(jnp.int32, (tokens, tokens), 1)
        ).astype(bf16)
        ranks = jnp.where(named > 0, dot(named.astype(bf16), strict), -1.0)
        packed_ref[tokens : tokens + extra, :] = jnp.full((extra, piece), -1.0, bf16)
        packed_ref[tokens : tokens + extra, 0:tokens] = ranks.astype(bf16)
        packed_ref[tokens : tokens + extra, pad : pad + tokens] = weight.astype(bf16)

    outs = (
        jax.ShapeDtypeStruct((tokens, width), bf16),
        jax.ShapeDtypeStruct((tokens + extra, piece), bf16),
    )
    operands = (scalars(part), rows, gain[None, :], index.T, scores.T)
    return call(body, outs, operands, 1 << 22, smem=1)


def group_of(sources, capacity):
    group = 1
    while group < sources and group * capacity % 16:
        group *= 2
    return group


def expert_up(places, own, far, capacity, gate_weight, up_weight):
    parts = places.side
    tokens, width = own[0][0].shape
    packed_rows, piece = own[0][1].shape
    extra = packed_rows - tokens
    pad = -(-tokens // 128) * 128
    sources = len(own) + sum(len(f) for f in far)
    slots = sources * capacity
    group = group_of(sources, capacity)
    hidden = gate_weight.shape[1]
    step = min(256, hidden)
    flat, layout = [], []
    for side, chips in zip(own, far):
        layout.append((len(flat), 0))
        flat += list(side)
        for pieces in chips:
            layout.append((len(flat), 1))
            flat += list(pieces)

    def body(s_ref, *refs):
        row_refs = refs[: len(flat)]
        gate_ref, up_ref, out_ref, info_ref, rows_ref, section_ref = refs[len(flat) :]

        @pl.when(pl.program_id(0) == 0)
        def _():
            expert = lax.broadcasted_iota(jnp.int32, (extra, 2 * pad), 0) == s_ref[1]
            if pad > tokens:
                for s in range(group):
                    rows_ref[s * pad + tokens : (s + 1) * pad, :] = jnp.zeros(
                        (pad - tokens, width), bf16
                    )
            for s0 in range(0, sources, group):
                targets = []
                for s in range(s0, s0 + group):
                    first, split = layout[s]
                    base = (s - s0) * pad
                    table_ref = row_refs[first] if split else row_refs[first + 1]
                    table = table_ref[tokens : tokens + extra, 0 : 2 * pad].astype(f32)
                    mine = jnp.sum(jnp.where(expert, table, 0.0), axis=0, keepdims=True)
                    info_ref[s : s + 1, :] = mine
                    rank = mine[:, 0:pad]
                    targets.append(jnp.where(rank >= 0, rank + (s - s0) * capacity, -1.0))
                    if split:
                        for q in range(parts):

                            @pl.when(s_ref[0] == q)
                            def _():
                                for i in range(parts):
                                    to = (q - i) % parts
                                    rows_ref[
                                        base : base + tokens, to * piece : (to + 1) * piece
                                    ] = row_refs[first + i][0:tokens, :]
                    else:
                        rows_ref[base : base + tokens, :] = row_refs[first][...]
                target = jnp.concatenate(targets, axis=1) if group > 1 else targets[0]
                slot = lax.broadcasted_iota(jnp.int32, (group * capacity, group * pad), 0)
                picks = (slot.astype(f32) == target).astype(bf16)
                section_ref[s0 * capacity : (s0 + group) * capacity, :] = dot(
                    picks, rows_ref[...]
                ).astype(bf16)

        section = section_ref[...]
        gate_value = dot(section, gate_ref[...])
        up_value = dot(section, up_ref[...])
        out_ref[...] = (silu(gate_value) * up_value).astype(bf16)

    weight_spec = pl.BlockSpec((width, step), lambda i: (0, i))
    return pl.pallas_call(
        body,
        grid=(hidden // step,),
        out_shape=(
            jax.ShapeDtypeStruct((slots, hidden), bf16),
            jax.ShapeDtypeStruct((sources, 2 * pad), f32),
        ),
        in_specs=[pl.BlockSpec(memory_space=pltpu.SMEM)]
        + whole(len(flat))
        + [weight_spec, weight_spec],
        out_specs=(
            pl.BlockSpec((slots, step), lambda i: (0, i)),
            pl.BlockSpec((sources, 2 * pad), lambda i: (0, 0)),
        ),
        scratch_shapes=[
            pltpu.VMEM((group * pad, width), bf16),
            pltpu.VMEM((slots, width), bf16),
        ],
        cost_estimate=pl.CostEstimate(
            flops=4 * slots * width * hidden, transcendentals=0, bytes_accessed=0
        ),
    )(scalars((places.x + places.y) % parts, places.e), *flat, gate_weight, up_weight)


def down(hiddens, weight, blocks, out_type):
    rows, hidden = hiddens[0].shape
    columns = weight.shape[1]
    count = len(hiddens)

    def body(blocks_ref, *refs):
        weight_ref, out_ref, sum_ref = refs[count:]
        for i in range(count):

            @pl.when(pl.program_id(0) == i)
            def _():
                product = dot(refs[i][...], weight_ref[...])
                if i:
                    product = sum_ref[...] + product
                if i < count - 1:
                    sum_ref[...] = product
                else:
                    out_ref[...] = product.astype(out_type)

    return pl.pallas_call(
        body,
        out_shape=jax.ShapeDtypeStruct((rows, columns), out_type),
        grid_spec=pltpu.PrefetchScalarGridSpec(
            num_scalar_prefetch=1,
            grid=(count,),
            in_specs=[pl.BlockSpec((rows, hidden), lambda i, b: (0, 0))] * count
            + [pl.BlockSpec((hidden, columns), lambda i, b: (b[i], 0))],
            out_specs=pl.BlockSpec((rows, columns), lambda i, b: (0, 0)),
            scratch_shapes=[pltpu.VMEM((rows, columns), f32)],
        ),
        cost_estimate=pl.CostEstimate(
            flops=2 * rows * hidden * count * columns, transcendentals=0, bytes_accessed=0
        ),
    )(blocks, *hiddens, weight)


def take_blocks(weight, blocks, count, hidden):
    columns = weight.shape[1]

    def body(blocks_ref, in_ref, out_ref):
        out_ref[...] = in_ref[...]

    return pl.pallas_call(
        body,
        out_shape=jax.ShapeDtypeStruct((count * hidden, columns), weight.dtype),
        grid_spec=pltpu.PrefetchScalarGridSpec(
            num_scalar_prefetch=1,
            grid=(count,),
            in_specs=[pl.BlockSpec((hidden, columns), lambda i, b: (b[i], 0))],
            out_specs=pl.BlockSpec((hidden, columns), lambda i, b: (i, 0)),
        ),
        cost_estimate=pl.CostEstimate(flops=1 << 20, transcendentals=0, bytes_accessed=0),
    )(blocks, weight)


def combine(own, back, info, tokens, capacity):
    slots, columns = own.shape
    sources = slots // capacity
    pad = info.shape[1] // 2
    group = group_of(sources, capacity)
    half = sources // 2

    def body(own_ref, info_ref, *refs):
        here_ref, there_ref = refs[len(back) :]
        for s0 in range(0, sources, group):
            span = slice(s0 * capacity, (s0 + group) * capacity)
            value = own_ref[span, :]
            for ref in refs[: len(back)]:
                value = value + ref[span, :].astype(f32)
            value = value.astype(bf16)
            for s in range(s0, s0 + group):
                rank = info_ref[s : s + 1, 0:pad]
                target = jnp.where(rank >= 0, rank + (s - s0) * capacity, -1.0)
                slot = lax.broadcasted_iota(jnp.int32, (group * capacity, pad), 0).astype(f32)
                places = jnp.where(slot == target, info_ref[s : s + 1, pad : 2 * pad], 0.0)
                dense = dot_tn(places.astype(bf16), value)[0:tokens]
                if s < half:
                    here_ref[s] = dense
                else:
                    there_ref[s - half] = dense.astype(bf16)

    outs = (
        jax.ShapeDtypeStruct((half, tokens, columns), f32),
        jax.ShapeDtypeStruct((half, tokens, columns), bf16),
    )
    return call(body, outs, (own, info, *back), 1 << 26)


def local(
    first_batch_queries,
    first_batch_keys,
    first_batch_values,
    output_gate_preactivation,
    decay_preactivation,
    channel_decay_bias,
    added_log_decay,
    head_norm_gain,
    attention_output_weight,
    second_batch_rows,
    expert_norm_gain,
    routed_expert_index,
    router_chosen_scores,
    expert_gate_weight,
    expert_up_weight,
    expert_down_weight,
    shared_gate_weight,
    shared_up_weight,
    shared_down_weight,
):
    at = Places()
    n, chips, experts = at.side, at.chips, at.ep
    heads = added_log_decay.shape[0]
    tokens, top_count = routed_expert_index.shape
    capacity = tokens * top_count * 3 // (2 * experts)
    gate_weight, up_weight, down_weight = (
        expert_gate_weight[0],
        expert_up_weight[0],
        expert_down_weight[0],
    )
    hidden = gate_weight.shape[1]
    columns = down_weight.shape[1]

    def held(k):
        return scalars(*[at.column(at.u - i, at.v + k) for i in range(n)])

    normed, packed = prepare_rows(
        (at.x + at.y) % n,
        n,
        second_batch_rows,
        expert_norm_gain,
        routed_expert_index,
        router_chosen_scores,
        experts,
    )
    far = [at.along_z(packed, k) for k in range(1, chips)]
    traded = [
        at.along_v(take_blocks(down_weight, held(k), n, hidden), k) for k in range(1, n)
    ]

    value_width = first_batch_values.shape[1] // heads
    o_local, q_device, own_state = local_attention(
        at,
        first_batch_queries,
        first_batch_keys,
        first_batch_values,
        decay_preactivation,
        channel_decay_bias,
        added_log_decay,
    )
    sibling_state = at.to_sibling(own_state)
    both_state = chip_state(at, own_state, sibling_state, value_width)
    arrived = [at.up_z(both_state, hop) for hop in range(1, chips)]

    far = [[a] + [at.along_u(a, i) for i in range(1, n)] for a in far]
    own_side = (normed, packed)
    other_side = (at.to_sibling(normed), at.to_sibling(packed))
    other_far = [[at.to_sibling(p) for p in pieces] for pieces in far]
    routed_hidden, info = expert_up(
        at, (own_side, other_side), (far, other_far), capacity, gate_weight, up_weight
    )
    hiddens = [routed_hidden] + [at.along_u(routed_hidden, i) for i in range(1, n)]
    steps = jnp.arange(n, dtype=jnp.int32)
    back = [
        at.along_v(down(hiddens, traded[k - 1], steps, bf16), -k) for k in range(1, n)
    ]
    own = down(hiddens, down_weight, held(0), f32)
    here, there = combine(own, back, info, tokens, capacity)
    from_sibling = at.to_sibling(there)
    chip_sum = here + from_sibling.astype(f32)
    routed_total = chip_sum[0]
    for k in range(1, chips):
        routed_total = routed_total + at.along_z(chip_sum[k].astype(bf16), -k).astype(f32)

    shared_hidden = (
        jax.nn.silu(dot(normed, shared_gate_weight)) * dot(normed, shared_up_weight)
    ).astype(bf16)
    mixed = finish_attention(
        at,
        o_local,
        q_device,
        sibling_state,
        arrived,
        output_gate_preactivation,
        head_norm_gain,
        heads,
    )
    sharing = mixed.shape[1] // shared_hidden.shape[1]
    folded = jnp.concatenate(
        [
            shared_hidden[i * (tokens // sharing) : (i + 1) * (tokens // sharing)]
            for i in range(sharing)
        ],
        axis=1,
    )
    both = jnp.concatenate([mixed, folded], axis=0)
    mixer_rows = mixed.shape[0]
    mixer_total = jnp.zeros((mixer_rows, columns), f32)
    shared_total = jnp.zeros((tokens, columns), f32)
    for dy in range(n):
        for dx in range(n):
            got = both if dy == 0 and dx == 0 else at.along_tp(both, dy, dx)
            source = ((at.y - dy) % n) * n + (at.x - dx) % n
            weight = lax.dynamic_slice_in_dim(
                attention_output_weight, source * got.shape[1], got.shape[1], 0
            )
            mixer_total = mixer_total + dot(got[:mixer_rows], weight)
            wide = shared_hidden.shape[1]
            part_hidden = jnp.concatenate(
                [got[mixer_rows:, i * wide : (i + 1) * wide] for i in range(sharing)], axis=0
            )
            weight = lax.dynamic_slice_in_dim(shared_down_weight, source * wide, wide, 0)
            shared_total = shared_total + dot(part_hidden, weight)
    token_mixed = mixer_total.astype(bf16)
    channel_mixed = (routed_total + shared_total).astype(bf16)
    return (token_mixed, channel_mixed)


def solution(mesh):
    placed = (
        P("ep", "tp"),
        P("ep", "tp"),
        P("ep", "tp"),
        P("ep", "tp"),
        P("ep", "tp"),
        P("tp"),
        P("tp", "ep"),
        P("tp"),
        P(None, "tp"),
        P("ep", None),
        P(),
        P("ep", None),
        P("ep", None),
        P("ep", None, "tp"),
        P("ep", None, "tp"),
        P("ep", None, "tp"),
        P(None, "tp"),
        P(None, "tp"),
        P(None, "tp"),
    )
    return jax.shard_map(
        local, mesh=mesh, in_specs=placed, out_specs=(P("ep", "tp"), P("ep", "tp")), check_vma=False
    )
```

```python
import math

import jax
import jax.numpy as jnp
import numpy as np
from jax import lax
from jax.experimental import pallas as pl
from jax.experimental.pallas import tpu as pltpu
from jax.sharding import PartitionSpec as P


BLOCK = 64
epsilon = 1e-06
temper = 16.0
routed_scale = 2.5
highest = lax.Precision.HIGHEST
f32 = jnp.float32
bf16 = jnp.bfloat16
AXES = ("ep", "tp")


class Places:
    def __init__(self):
        self.ep, self.tp = lax.axis_size("ep"), lax.axis_size("tp")
        self.side = math.isqrt(self.tp)
        self.chips = self.ep // 2
        assert self.side * self.side == self.tp and self.chips * 2 == self.ep

    def pairs(self, move):
        n = self.side
        out = []
        for e in range(self.ep):
            for j in range(self.tp):
                z, c, y, x = move(e // 2, e % 2, j // n, j % n)
                if 0 <= z < self.chips:
                    out.append((e * self.tp + j, (z * 2 + c) * self.tp + (y % n) * n + x % n))
        return out

    def send(self, value, move):
        return lax.ppermute(value, AXES, self.pairs(move))

    def along_z(self, value, k):
        return self.send(value, lambda z, c, y, x: ((z + k) % self.chips, c, y, x))

    def up_z(self, value, k):
        return self.send(value, lambda z, c, y, x: (z + k, c, y, x))

    def to_sibling(self, value):
        return self.send(value, lambda z, c, y, x: (z, 1 - c, y, x))

    def along_u(self, value, k):
        return self.send(value, lambda z, c, y, x: (z, c, y, x + k) if c == 0 else (z, c, y + k, x))

    def along_v(self, value, k):
        return self.send(value, lambda z, c, y, x: (z, c, y + k, x) if c == 0 else (z, c, y, x + k))

    def along_tp(self, value, dy, dx):
        return self.send(value, lambda z, c, y, x: (z, c, y + dy, x + dx))


def dot(a, b, precision=None):
    return jnp.dot(a, b, preferred_element_type=f32, precision=precision)


def dot_nt(a, b):
    return lax.dot_general(a, b, (((1,), (1,)), ((), ())), preferred_element_type=f32)


def dot_tn(a, b, precision=None):
    return lax.dot_general(
        a, b, (((0,), (0,)), ((), ())), preferred_element_type=f32, precision=precision
    )


def hold(values):
    return lax.optimization_barrier(values)


def silu(value):
    return value / (1.0 + jnp.exp(-value))


def whole(count):
    return [pl.BlockSpec(memory_space=pltpu.VMEM)] * count


def column(n, core, x, y, du, dv):
    if core == 0:
        return (y + dv) % n * n + (x + du) % n
    return (y + du) % n * n + (x + dv) % n


class Index:
    def __init__(self, places):
        n = places.side
        table = [
            [z, c, (x + y) % n, z * 2 + c]
            + [column(n, c, x, y, -i, k) for k in range(n) for i in range(n)]
            + [(y - dy) % n * n + (x - dx) % n for dy in range(n) for dx in range(n)]
            for z in range(places.chips)
            for c in range(2)
            for y in range(n)
            for x in range(n)
        ]
        here = lax.axis_index("ep") * places.tp + lax.axis_index("tp")
        self.vector = lax.dynamic_index_in_dim(
            jnp.asarray(np.array(table, np.int32)), here, 0, keepdims=False
        )
        self.z, self.c, self.part, self.e = range(4)
        self.held, self.given = 4, 4 + n
        self.tp = 4 + n * n

    def block(self, place, count=1):
        return lambda i, s: (s[place + i], 0)


def call(body, outs, operands, flops, smem=0):
    specs = [pl.BlockSpec(memory_space=pltpu.SMEM)] * smem + whole(len(operands) - smem)
    return pl.pallas_call(
        body,
        out_shape=outs,
        in_specs=specs,
        out_specs=jax.tree.map(lambda _: pl.BlockSpec(memory_space=pltpu.VMEM), outs),
        cost_estimate=pl.CostEstimate(flops=flops, transcendentals=0, bytes_accessed=0),
    )(*operands)


def local_attention(q, k, v, decay_pre, bias, added):
    heads, rows = added.shape
    dk, dv = q.shape[1] // heads, v.shape[1] // heads
    blocks = rows // BLOCK
    group = min(max(1, 128 // dk), heads)
    lanes = group * dk

    def body(q_ref, k_ref, v_ref, d_ref, bias_ref, added_ref, o_ref, qd_ref, pack_ref):
        spread = (
            lax.broadcasted_iota(jnp.int32, (heads, heads * dk), 1) // dk
            == lax.broadcasted_iota(jnp.int32, (heads, heads * dk), 0)
        ).astype(f32)
        logits = d_ref[...].astype(f32) + bias_ref[...]
        base = jnp.minimum(logits, 0.0) - jnp.log1p(jnp.exp(-jnp.abs(logits)))
        decay = base / temper + dot_tn(added_ref[...], spread, highest)
        row = lax.broadcasted_iota(jnp.int32, (BLOCK, BLOCK), 0)
        col = lax.broadcasted_iota(jnp.int32, (BLOCK, BLOCK), 1)
        lower = row >= col
        lower_f = lower.astype(f32)
        lane = lax.broadcasted_iota(jnp.int32, (1, lanes), 1)
        masks = [(lane // dk == g).astype(f32) for g in range(group)]
        states = [None] * heads
        lead = jnp.zeros((1, heads * dk), f32)
        for b in range(blocks):
            span = slice(b * BLOCK, (b + 1) * BLOCK)
            running = dot(lower_f, decay[span], highest)
            total = running[BLOCK - 1 : BLOCK, :]
            grow = jnp.exp(running)
            q_dec = q_ref[span, :].astype(f32) * grow
            keys = k_ref[span, :].astype(f32)
            k_up = (keys * jnp.exp(-running)).astype(bf16)
            k_end = (keys * jnp.exp(total - running)).astype(bf16)
            qd_ref[span, :] = (q_dec * jnp.exp(lead)).astype(bf16)
            shrink = jnp.exp(total)
            for h in range(heads):
                at = slice(h // group * lanes, h // group * lanes + lanes)
                q_h = (q_dec[:, at] * masks[h % group]).astype(bf16)
                v_h = v_ref[span, h * dv : (h + 1) * dv]
                scores = jnp.where(lower, dot_nt(q_h, k_up[:, at]), 0.0).astype(bf16)
                value = dot(scores, v_h)
                if b:
                    value = value + dot_nt(q_h, states[h].astype(bf16))
                o_ref[span, h * dv : (h + 1) * dv] = value
                update = dot_tn(v_h, k_end[:, at])
                states[h] = update if b == 0 else states[h] * shrink[:, at] + update
            lead = lead + total
        for h0 in range(0, heads, group):
            packed = states[h0]
            for g in range(1, group):
                packed = jnp.where(lane // dk == g, states[h0 + g], packed)
            pack_ref[0:dv, h0 * dk : h0 * dk + lanes] = packed.astype(bf16)
        pack_ref[dv : dv + 8, :] = jnp.broadcast_to(jnp.exp(lead), (8, heads * dk)).astype(bf16)

    outs = (
        jax.ShapeDtypeStruct((rows, heads * dv), f32),
        jax.ShapeDtypeStruct((rows, heads * dk), bf16),
        jax.ShapeDtypeStruct((dv + 8, heads * dk), bf16),
    )
    return call(body, outs, (q, k, v, decay_pre, bias[None, :], added), 1 << 25)


def finish_attention(
    index, local, qd, states, gate_pre, gain, heads, normed, shared_gate, shared_up
):
    rows = local.shape[0]
    dv, dk = local.shape[1] // heads, qd.shape[1] // heads
    group = min(max(1, 128 // dk), heads)
    lanes = group * dk
    tokens, hidden = normed.shape[0], shared_gate.shape[1]
    sharing = local.shape[1] // hidden
    part = tokens // sharing

    def body(s_ref, local_ref, qd_ref, gate_ref, gain_ref, normed_ref, sg_ref, su_ref, *refs):
        out_ref = refs[-1]
        first = s_ref[index.c] == 0
        between = jnp.ones((1, heads * dk), f32)
        incoming = jnp.zeros((dv, heads * dk), f32)
        sib = refs[0][...].astype(f32)
        for hop in range(1, (len(refs) - 2) // 2 + 1):
            mine, other = refs[2 * hop - 1][...].astype(f32), refs[2 * hop][...].astype(f32)
            inside = s_ref[index.z] >= hop
            early, late = jnp.where(first, mine, other), jnp.where(first, other, mine)
            decay = late[dv : dv + 1]
            got = early[0:dv] * decay + late[0:dv]
            incoming = incoming + jnp.where(inside, between * got, 0.0)
            between = jnp.where(inside, between * (early[dv : dv + 1] * decay), between)
        incoming = jnp.where(first, incoming, incoming * sib[dv : dv + 1] + sib[0:dv]).astype(bf16)
        lane = lax.broadcasted_iota(jnp.int32, (1, lanes), 1)
        for h in range(heads):
            at = slice(h // group * lanes, h // group * lanes + lanes)
            vs = slice(h * dv, (h + 1) * dv)
            mask = lane // dk == h % group
            q_h = jnp.where(mask, qd_ref[:, at], jnp.zeros((), bf16))
            value = local_ref[:, vs] + dot_nt(q_h, incoming[:, at])
            mean_square = jnp.mean(value * value, axis=1, keepdims=True)
            value = value * lax.rsqrt(mean_square + epsilon) * gain_ref[:, vs]
            out_ref[0:rows, vs] = (value * silu(gate_ref[:, vs].astype(f32))).astype(bf16)
        features = normed_ref[...]
        shared = (silu(dot(features, sg_ref[...])) * dot(features, su_ref[...])).astype(bf16)
        for i in range(sharing):
            out_ref[rows : rows + part, i * hidden : (i + 1) * hidden] = shared[
                i * part : (i + 1) * part
            ]

    out = jax.ShapeDtypeStruct((rows + part, local.shape[1]), bf16)
    operands = (index.vector, local, qd, gate_pre, gain[None, :], normed, shared_gate, shared_up)
    return call(body, out, operands + tuple(states), 1 << 27, smem=1)


def project(index, gathered, attention_weight, shared_weight, tokens):
    count = len(gathered)
    folded, width = gathered[0].shape
    hidden, columns = shared_weight.shape[0] // count, shared_weight.shape[1]
    sharing = width // hidden
    part = tokens // sharing
    rows = folded - part

    def body(s_ref, *refs):
        weight_ref, shared_ref, mixed_ref, out_ref, sum_ref = refs[count:]
        for i in range(count):

            @pl.when(pl.program_id(0) == i)
            def _():
                ref = refs[i]
                mixed = dot(ref[0:rows, :], weight_ref[...])
                units = jnp.concatenate(
                    [ref[rows:, q * hidden : (q + 1) * hidden] for q in range(sharing)], axis=0
                )
                shared = dot(units, shared_ref[...])
                if i:
                    mixed, shared = mixed + sum_ref[...], shared + out_ref[...]
                if i < count - 1:
                    sum_ref[...] = mixed
                else:
                    mixed_ref[...] = mixed.astype(bf16)
                out_ref[...] = shared

    fixed = lambda i, s: (0, 0)
    return pl.pallas_call(
        body,
        out_shape=(
            jax.ShapeDtypeStruct((rows, columns), bf16),
            jax.ShapeDtypeStruct((tokens, columns), f32),
        ),
        grid_spec=pltpu.PrefetchScalarGridSpec(
            num_scalar_prefetch=1,
            grid=(count,),
            in_specs=[pl.BlockSpec((folded, width), fixed)] * count
            + [
                pl.BlockSpec((width, columns), index.block(index.tp)),
                pl.BlockSpec((hidden, columns), index.block(index.tp)),
            ],
            out_specs=(pl.BlockSpec((rows, columns), fixed), pl.BlockSpec((tokens, columns), fixed)),
            scratch_shapes=[pltpu.VMEM((rows, columns), f32)],
        ),
        cost_estimate=pl.CostEstimate(
            flops=2 * folded * width * columns * count, transcendentals=0, bytes_accessed=0
        ),
    )(index.vector, *gathered, attention_weight, shared_weight)


def prepare_rows(places, parts, rows, gain, index, scores, experts):
    tokens, width = rows.shape
    top = index.shape[1]
    piece = width // parts
    pad = -(-tokens // 128) * 128
    extra = -(-experts // 8) * 8

    def body(s_ref, rows_ref, gain_ref, index_ref, score_ref, normed_ref, packed_ref):
        value = rows_ref[...].astype(f32)
        mean_square = jnp.mean(value * value, axis=1, keepdims=True)
        normed = (value * lax.rsqrt(mean_square + epsilon) * gain_ref[...]).astype(bf16)
        normed_ref[...] = normed
        for q in range(parts):

            @pl.when(s_ref[places.part] == q)
            def _():
                packed_ref[0:tokens, :] = normed[:, q * piece : (q + 1) * piece]

        scores = score_ref[...]
        weights = routed_scale * scores / jnp.sum(scores, axis=0, keepdims=True)
        expert = lax.broadcasted_iota(jnp.int32, (extra, tokens), 0)
        named = jnp.zeros((extra, tokens), f32)
        weight = jnp.zeros((extra, tokens), f32)
        for k in range(top):
            hit = index_ref[k : k + 1, :] == expert
            named = jnp.where(hit, 1.0, named)
            weight = jnp.where(hit, weights[k : k + 1, :], weight)
        strict = (
            lax.broadcasted_iota(jnp.int32, (tokens, tokens), 0)
            < lax.broadcasted_iota(jnp.int32, (tokens, tokens), 1)
        ).astype(bf16)
        ranks = jnp.where(named > 0, dot(named.astype(bf16), strict), -1.0)
        packed_ref[tokens : tokens + extra, :] = jnp.full((extra, piece), -1.0, bf16)
        packed_ref[tokens : tokens + extra, 0:tokens] = ranks.astype(bf16)
        packed_ref[tokens : tokens + extra, pad : pad + tokens] = weight.astype(bf16)

    outs = (
        jax.ShapeDtypeStruct((tokens, width), bf16),
        jax.ShapeDtypeStruct((tokens + extra, piece), bf16),
    )
    operands = (places.vector, rows, gain[None, :], index.T, scores.T)
    return call(body, outs, operands, 1 << 22, smem=1)


def group_of(sources, capacity):
    group = 1
    while group < sources and group * capacity % 16:
        group *= 2
    return group


def expert_up(index, own, far, capacity, gate_weight, up_weight):
    parts = len(far[0])
    tokens, width = own[0].shape
    packed_rows, piece = own[1].shape
    extra = packed_rows - tokens
    pad = -(-tokens // 128) * 128
    sources = 1 + len(far)
    slots = sources * capacity
    group = group_of(sources, capacity)
    hidden = gate_weight.shape[1]
    step = min(256, hidden)
    flat = list(own) + [p for pieces in far for p in pieces]

    def body(s_ref, *refs):
        row_refs = refs[: len(flat)]
        gate_ref, up_ref, out_ref, info_ref, rows_ref, section_ref = refs[len(flat) :]

        @pl.when(pl.program_id(0) == 0)
        def _():
            expert = lax.broadcasted_iota(jnp.int32, (extra, 2 * pad), 0) == s_ref[index.e]
            if pad > tokens:
                for s in range(sources):
                    rows_ref[s * pad + tokens : (s + 1) * pad, :] = jnp.zeros(
                        (pad - tokens, width), bf16
                    )
            rows_ref[0:tokens, :] = row_refs[0][...]
            for q in range(parts):

                @pl.when(s_ref[index.part] == q)
                def _():
                    for s in range(1, sources):
                        for i in range(parts):
                            to = (q - i) % parts
                            rows_ref[
                                s * pad : s * pad + tokens, to * piece : (to + 1) * piece
                            ] = row_refs[2 + (s - 1) * parts + i][0:tokens, :]

            for s0 in range(0, sources, group):
                targets = []
                for s in range(s0, s0 + group):
                    table_ref = row_refs[2 + (s - 1) * parts if s else 1]
                    table = table_ref[tokens : tokens + extra, 0 : 2 * pad].astype(f32)
                    mine = jnp.sum(jnp.where(expert, table, 0.0), axis=0, keepdims=True)
                    info_ref[s : s + 1, :] = mine
                    rank = mine[:, 0:pad]
                    targets.append(jnp.where(rank >= 0, rank + (s - s0) * capacity, -1.0))
                target = jnp.concatenate(targets, axis=1) if group > 1 else targets[0]
                slot = lax.broadcasted_iota(jnp.int32, (group * capacity, group * pad), 0)
                picks = (slot.astype(f32) == target).astype(bf16)
                section_ref[s0 * capacity : (s0 + group) * capacity, :] = dot(
                    picks, rows_ref[s0 * pad : (s0 + group) * pad, :]
                ).astype(bf16)

        section = section_ref[...]
        gate_value = dot(section, gate_ref[...])
        up_value = dot(section, up_ref[...])
        out_ref[...] = (silu(gate_value) * up_value).astype(bf16)

    weight_spec = pl.BlockSpec((width, step), lambda i: (0, i))
    return pl.pallas_call(
        body,
        grid=(hidden // step,),
        out_shape=(
            jax.ShapeDtypeStruct((slots, hidden), bf16),
            jax.ShapeDtypeStruct((sources, 2 * pad), f32),
        ),
        in_specs=[pl.BlockSpec(memory_space=pltpu.SMEM)]
        + whole(len(flat))
        + [weight_spec, weight_spec],
        out_specs=(
            pl.BlockSpec((slots, step), lambda i: (0, i)),
            pl.BlockSpec((sources, 2 * pad), lambda i: (0, 0)),
        ),
        scratch_shapes=[
            pltpu.VMEM((sources * pad, width), bf16),
            pltpu.VMEM((slots, width), bf16),
        ],
        cost_estimate=pl.CostEstimate(
            flops=4 * slots * width * hidden, transcendentals=0, bytes_accessed=0
        ),
    )(index.vector, *flat, gate_weight, up_weight)


def take_block(index, weight, place, hidden):
    columns = weight.shape[1]

    def body(s_ref, in_ref, out_ref):
        out_ref[...] = in_ref[...]

    return pl.pallas_call(
        body,
        out_shape=jax.ShapeDtypeStruct((hidden, columns), weight.dtype),
        grid_spec=pltpu.PrefetchScalarGridSpec(
            num_scalar_prefetch=1,
            grid=(4,),
            in_specs=[pl.BlockSpec((hidden // 4, columns), lambda i, s: (s[place] * 4 + i, 0))],
            out_specs=pl.BlockSpec((hidden // 4, columns), lambda i, s: (i, 0)),
        ),
        cost_estimate=pl.CostEstimate(flops=1 << 20, transcendentals=0, bytes_accessed=0),
    )(index.vector, weight)


def down_first(index, hiddens, weight, traded):
    hidden, columns = hiddens[0].shape[1], weight.shape[1]
    chunks, partners = len(hiddens), len(traded)
    fixed = lambda i, s: (0, 0)

    def body(s_ref, *refs):
        weights = refs[chunks : chunks + 1 + partners]
        outs = refs[chunks + 1 + partners :]
        for w in range(1 + partners):
            for h in range(chunks):
                outs[w * chunks + h][...] = dot(refs[h][...], weights[w][...])

    outs = pl.pallas_call(
        body,
        out_shape=[
            jax.ShapeDtypeStruct((h.shape[0], columns), f32)
            for _ in range(1 + partners)
            for h in hiddens
        ],
        grid_spec=pltpu.PrefetchScalarGridSpec(
            num_scalar_prefetch=1,
            grid=(1,),
            in_specs=[pl.BlockSpec(h.shape, fixed) for h in hiddens]
            + [pl.BlockSpec((hidden, columns), index.block(index.held))]
            + [pl.BlockSpec((hidden, columns), fixed)] * partners,
            out_specs=[
                pl.BlockSpec((h.shape[0], columns), fixed)
                for _ in range(1 + partners)
                for h in hiddens
            ],
        ),
        cost_estimate=pl.CostEstimate(
            flops=2 * sum(h.shape[0] for h in hiddens) * hidden * columns * (1 + partners),
            transcendentals=0,
            bytes_accessed=0,
        ),
    )(index.vector, *hiddens, weight, *traded)
    return [outs[w * chunks : (w + 1) * chunks] for w in range(1 + partners)]


def down_partner(first, hiddens, weights):
    count = len(hiddens)

    def body(first_ref, *refs):
        total = first_ref[...]
        for i in range(count):
            total = total + dot(refs[i][...], refs[count + i][...])
        refs[-1][...] = total.astype(bf16)

    out = jax.ShapeDtypeStruct(first.shape, bf16)
    flops = 2 * first.size * hiddens[0].shape[1] * count
    return call(body, out, (first, *hiddens, *weights), flops)


def down_own(index, firsts, gathered, weight):
    count, chunks = len(gathered), len(firsts)
    hidden, columns = gathered[0][0].shape[1], weight.shape[1]
    fixed = lambda i, s: (0, 0)

    def body(s_ref, *refs):
        hidden_refs = refs[chunks : chunks + count * chunks]
        weight_ref = refs[chunks + count * chunks]
        outs = refs[chunks + count * chunks + 1 :]
        for i in range(count):

            @pl.when(pl.program_id(0) == i)
            def _():
                for h in range(chunks):
                    before = outs[h][...] if i else refs[h][...]
                    outs[h][...] = before + dot(hidden_refs[i * chunks + h][...], weight_ref[...])

    flat = [h for pieces in gathered for h in pieces]
    return pl.pallas_call(
        body,
        out_shape=[jax.ShapeDtypeStruct(f.shape, f32) for f in firsts],
        grid_spec=pltpu.PrefetchScalarGridSpec(
            num_scalar_prefetch=1,
            grid=(count,),
            in_specs=[pl.BlockSpec(f.shape, fixed) for f in firsts]
            + [pl.BlockSpec(h.shape, fixed) for h in flat]
            + [pl.BlockSpec((hidden, columns), index.block(index.held + 1))],
            out_specs=[pl.BlockSpec(f.shape, fixed) for f in firsts],
        ),
        cost_estimate=pl.CostEstimate(
            flops=2 * sum(h.shape[0] for h in flat) * hidden * columns,
            transcendentals=0,
            bytes_accessed=0,
        ),
    )(index.vector, *firsts, *flat, weight)


def combine(own, back, info, tokens, capacity, out_type):
    slots, columns = own.shape
    sources = slots // capacity
    pad = info.shape[1] // 2
    group = group_of(sources, capacity)

    def body(own_ref, info_ref, *refs):
        out_ref = refs[-1]
        for s0 in range(0, sources, group):
            span = slice(s0 * capacity, (s0 + group) * capacity)
            value = own_ref[span, :]
            for ref in refs[:-1]:
                value = value + ref[span, :].astype(f32)
            value = value.astype(bf16)
            for s in range(s0, s0 + group):
                rank = info_ref[s : s + 1, 0:pad]
                target = jnp.where(rank >= 0, rank + (s - s0) * capacity, -1.0)
                slot = lax.broadcasted_iota(jnp.int32, (group * capacity, pad), 0).astype(f32)
                places = jnp.where(slot == target, info_ref[s : s + 1, pad : 2 * pad], 0.0)
                out_ref[s] = dot_tn(places.astype(bf16), value)[0:tokens].astype(out_type)

    out = jax.ShapeDtypeStruct((sources, tokens, columns), out_type)
    return call(body, out, (own, info, *back), 1 << 26)


def local(
    first_batch_queries,
    first_batch_keys,
    first_batch_values,
    output_gate_preactivation,
    decay_preactivation,
    channel_decay_bias,
    added_log_decay,
    head_norm_gain,
    attention_output_weight,
    second_batch_rows,
    expert_norm_gain,
    routed_expert_index,
    router_chosen_scores,
    expert_gate_weight,
    expert_up_weight,
    expert_down_weight,
    shared_gate_weight,
    shared_up_weight,
    shared_down_weight,
):
    at = Places()
    index = Index(at)
    n, chips, experts = at.side, at.chips, at.ep
    heads = added_log_decay.shape[0]
    tokens, top_count = routed_expert_index.shape
    capacity = tokens * top_count * 3 // (2 * experts)
    gate_weight, up_weight, down_weight = (
        expert_gate_weight[0],
        expert_up_weight[0],
        expert_down_weight[0],
    )
    hidden = gate_weight.shape[1]

    def down_block(k, i):
        return take_block(index, down_weight, index.given + (k - 1) * n + i, hidden)

    normed, packed = prepare_rows(
        index,
        n,
        second_batch_rows,
        expert_norm_gain,
        routed_expert_index,
        router_chosen_scores,
        experts,
    )
    far = [at.along_z(packed, k) for k in range(1, chips)]
    early = [down_block(k, 0) for k in range(1, n)]
    o_local, q_device, own_state = local_attention(
        first_batch_queries,
        first_batch_keys,
        first_batch_values,
        decay_preactivation,
        channel_decay_bias,
        added_log_decay,
    )
    far, own_state, early = hold((far, own_state, early))
    traded = [[at.along_v(early[k - 1], k)] for k in range(1, n)]
    arrived = [at.up_z(own_state, hop) for hop in range(1, chips)]
    far = [[a] + [at.along_u(a, i) for i in range(1, n)] for a in far]
    late = [[down_block(k, i) for i in range(1, n)] for k in range(1, n)]
    far, arrived, late = hold((far, arrived, late))
    states = [at.to_sibling(own_state)]
    for state in arrived:
        states += [state, at.to_sibling(state)]
    for k in range(1, n):
        traded[k - 1] += [at.along_v(block, k) for block in late[k - 1]]
    ups = [expert_up(index, (normed, packed), far, capacity, gate_weight, up_weight)]
    other = (
        (at.to_sibling(normed), at.to_sibling(packed)),
        [[at.to_sibling(p) for p in pieces] for pieces in far],
    )
    gathered_first = [at.along_u(ups[0][0], i) for i in range(1, n)]
    _, other = hold((ups[0][0], other))
    ups.append(expert_up(index, *other, capacity, gate_weight, up_weight))
    hiddens = [up[0] for up in ups]
    gathered_second = [at.along_u(hiddens[1], i) for i in range(1, n)]
    both = finish_attention(
        index,
        o_local,
        q_device,
        states,
        output_gate_preactivation,
        head_norm_gain,
        heads,
        normed,
        shared_gate_weight,
        shared_up_weight,
    )
    firsts = down_first(index, hiddens, down_weight, [t[0] for t in traded])

    def partials(chunk, gathered):
        return [
            down_partner(firsts[k][chunk], gathered, traded[k - 1][1:]) for k in range(1, n)
        ]

    partial = partials(0, gathered_first)
    back = [[at.along_v(partial[k - 1], -k) for k in range(1, n)]]
    gathered_second, both, _ = hold((gathered_second, both, partial))
    partial = partials(1, gathered_second)
    back.append([at.along_v(partial[k - 1], -k) for k in range(1, n)])
    gathered = [list(pair) for pair in zip(gathered_first, gathered_second)]
    owns = down_own(index, firsts[0], gathered, down_weight)
    here, there = [
        combine(owns[chunk], back[chunk], ups[chunk][1], tokens, capacity, (f32, bf16)[chunk])
        for chunk in range(2)
    ]
    there, to_send = hold((there, both))
    from_sibling = at.to_sibling(there)
    chip_sum = here + from_sibling.astype(f32)
    routed_total = chip_sum[0]
    for k in range(1, chips):
        routed_total = routed_total + at.along_z(chip_sum[k].astype(bf16), -k).astype(f32)

    mixed = [
        both if dy == 0 and dx == 0 else at.along_tp(to_send, dy, dx)
        for dy in range(n)
        for dx in range(n)
    ]
    token_mixed, shared_total = project(
        index, mixed, attention_output_weight, shared_down_weight, tokens
    )
    channel_mixed = (routed_total + shared_total).astype(bf16)
    return (token_mixed, channel_mixed)


def solution(mesh):
    placed = (
        P("ep", "tp"),
        P("ep", "tp"),
        P("ep", "tp"),
        P("ep", "tp"),
        P("ep", "tp"),
        P("tp"),
        P("tp", "ep"),
        P("tp"),
        P(None, "tp"),
        P("ep", None),
        P(),
        P("ep", None),
        P("ep", None),
        P("ep", None, "tp"),
        P("ep", None, "tp"),
        P("ep", None, "tp"),
        P(None, "tp"),
        P(None, "tp"),
        P(None, "tp"),
    )

    return jax.shard_map(
        local, mesh=mesh, in_specs=placed, out_specs=(P("ep", "tp"), P("ep", "tp")), check_vma=False
    )
```

```python
import math

import jax
import jax.numpy as jnp
import numpy as np
from jax import lax
from jax.experimental import pallas as pl
from jax.experimental.pallas import tpu as pltpu
from jax.sharding import PartitionSpec as P


BLOCK = 64
epsilon = 1e-06
temper = 16.0
routed_scale = 2.5
highest = lax.Precision.HIGHEST
f32 = jnp.float32
bf16 = jnp.bfloat16
AXES = ("ep", "tp")


class Places:
    def __init__(self):
        self.ep, self.tp = lax.axis_size("ep"), lax.axis_size("tp")
        self.side = math.isqrt(self.tp)
        self.chips = self.ep // 2
        assert self.side * self.side == self.tp and self.chips * 2 == self.ep

    def pairs(self, move):
        n = self.side
        out = []
        for e in range(self.ep):
            for j in range(self.tp):
                z, c, y, x = move(e // 2, e % 2, j // n, j % n)
                if 0 <= z < self.chips:
                    out.append((e * self.tp + j, (z * 2 + c) * self.tp + (y % n) * n + x % n))
        return out

    def send(self, value, move):
        return lax.ppermute(value, AXES, self.pairs(move))

    def along_z(self, value, k):
        return self.send(value, lambda z, c, y, x: ((z + k) % self.chips, c, y, x))

    def up_z(self, value, k):
        return self.send(value, lambda z, c, y, x: (z + k, c, y, x))

    def to_sibling(self, value):
        return self.send(value, lambda z, c, y, x: (z, 1 - c, y, x))

    def along_u(self, value, k):
        return self.send(value, lambda z, c, y, x: (z, c, y, x + k) if c == 0 else (z, c, y + k, x))

    def along_v(self, value, k):
        return self.send(value, lambda z, c, y, x: (z, c, y + k, x) if c == 0 else (z, c, y, x + k))

    def along_tp(self, value, dy, dx):
        return self.send(value, lambda z, c, y, x: (z, c, y + dy, x + dx))


def dot(a, b, precision=None):
    return jnp.dot(a, b, preferred_element_type=f32, precision=precision)


def dot_nt(a, b):
    return lax.dot_general(a, b, (((1,), (1,)), ((), ())), preferred_element_type=f32)


def dot_tn(a, b, precision=None):
    return lax.dot_general(
        a, b, (((0,), (0,)), ((), ())), preferred_element_type=f32, precision=precision
    )


def hold(values):
    return lax.optimization_barrier(values)


def silu(value):
    return value / (1.0 + jnp.exp(-value))


def column(n, core, x, y, du, dv):
    if core == 0:
        return (y + dv) % n * n + (x + du) % n
    return (y + du) % n * n + (x + dv) % n


class Index:
    def __init__(self, places):
        n = places.side
        table = [
            [z, c, (x + y) % n, z * 2 + c]
            + [column(n, c, x, y, -i, k) for k in range(n) for i in range(n)]
            + [(y - dy) % n * n + (x - dx) % n for dy in range(n) for dx in range(n)]
            for z in range(places.chips)
            for c in range(2)
            for y in range(n)
            for x in range(n)
        ]
        here = lax.axis_index("ep") * places.tp + lax.axis_index("tp")
        self.vector = lax.dynamic_index_in_dim(
            jnp.asarray(np.array(table, np.int32)), here, 0, keepdims=False
        )
        self.z, self.c, self.part, self.e = range(4)
        self.held, self.given = 4, 4 + n
        self.tp = 4 + n * n

    def rows(self, s_ref, place, ref, size):
        start = pl.multiple_of(s_ref[place] * size, size)
        return ref[pl.ds(start, size), :]


def call(body, outs, operands, flops, smem=0, scratch=()):
    specs = [pl.BlockSpec(memory_space=pltpu.SMEM)] * smem
    specs += [pl.BlockSpec(memory_space=pltpu.VMEM)] * (len(operands) - smem)
    given = list(operands[:smem])
    given += [pltpu.with_memory_space_constraint(v, pltpu.VMEM) for v in operands[smem:]]
    return pl.pallas_call(
        body,
        out_shape=jax.tree.map(lambda o: pltpu.VMEM(o.shape, o.dtype), outs),
        in_specs=specs,
        out_specs=jax.tree.map(lambda _: pl.BlockSpec(memory_space=pltpu.VMEM), outs),
        scratch_shapes=list(scratch),
        compiler_params=pltpu.CompilerParams(vmem_limit_bytes=12 << 20),
        cost_estimate=pl.CostEstimate(flops=flops, transcendentals=0, bytes_accessed=0),
    )(*given)


def local_attention(q, k, v, decay_pre, bias, added):
    heads, rows = added.shape
    dk, dv = q.shape[1] // heads, v.shape[1] // heads
    blocks = rows // BLOCK
    group = min(max(1, 128 // dk), heads)
    lanes = group * dk

    def body(q_ref, k_ref, v_ref, d_ref, bias_ref, added_ref, o_ref, qd_ref, pack_ref):
        spread = (
            lax.broadcasted_iota(jnp.int32, (heads, heads * dk), 1) // dk
            == lax.broadcasted_iota(jnp.int32, (heads, heads * dk), 0)
        ).astype(f32)
        logits = d_ref[...].astype(f32) + bias_ref[...]
        base = jnp.minimum(logits, 0.0) - jnp.log1p(jnp.exp(-jnp.abs(logits)))
        decay = base / temper + dot_tn(added_ref[...], spread, highest)
        row = lax.broadcasted_iota(jnp.int32, (BLOCK, BLOCK), 0)
        col = lax.broadcasted_iota(jnp.int32, (BLOCK, BLOCK), 1)
        lower = row >= col
        lower_f = lower.astype(f32)
        lane = lax.broadcasted_iota(jnp.int32, (1, lanes), 1)
        masks = [(lane // dk == g).astype(f32) for g in range(group)]
        states = [None] * heads
        lead = jnp.zeros((1, heads * dk), f32)
        for b in range(blocks):
            span = slice(b * BLOCK, (b + 1) * BLOCK)
            running = dot(lower_f, decay[span], highest)
            total = running[BLOCK - 1 : BLOCK, :]
            grow = jnp.exp(running)
            q_dec = q_ref[span, :].astype(f32) * grow
            keys = k_ref[span, :].astype(f32)
            k_up = (keys * jnp.exp(-running)).astype(bf16)
            k_end = (keys * jnp.exp(total - running)).astype(bf16)
            qd_ref[span, :] = (q_dec * jnp.exp(lead)).astype(bf16)
            shrink = jnp.exp(total)
            for h in range(heads):
                at = slice(h // group * lanes, h // group * lanes + lanes)
                q_h = (q_dec[:, at] * masks[h % group]).astype(bf16)
                v_h = v_ref[span, h * dv : (h + 1) * dv]
                scores = jnp.where(lower, dot_nt(q_h, k_up[:, at]), 0.0).astype(bf16)
                value = dot(scores, v_h)
                if b:
                    value = value + dot_nt(q_h, states[h].astype(bf16))
                o_ref[span, h * dv : (h + 1) * dv] = value
                update = dot_tn(v_h, k_end[:, at])
                states[h] = update if b == 0 else states[h] * shrink[:, at] + update
            lead = lead + total
        for h0 in range(0, heads, group):
            packed = states[h0]
            for g in range(1, group):
                packed = jnp.where(lane // dk == g, states[h0 + g], packed)
            pack_ref[0:dv, h0 * dk : h0 * dk + lanes] = packed.astype(bf16)
        pack_ref[dv : dv + 8, :] = jnp.broadcast_to(jnp.exp(lead), (8, heads * dk)).astype(bf16)

    outs = (
        jax.ShapeDtypeStruct((rows, heads * dv), f32),
        jax.ShapeDtypeStruct((rows, heads * dk), bf16),
        jax.ShapeDtypeStruct((dv + 8, heads * dk), bf16),
    )
    return call(body, outs, (q, k, v, decay_pre, bias[None, :], added), 1 << 25)


def finish_attention(
    index, local, qd, states, gate_pre, gain, heads, normed, shared_gate, shared_up
):
    rows = local.shape[0]
    dv, dk = local.shape[1] // heads, qd.shape[1] // heads
    group = min(max(1, 128 // dk), heads)
    lanes = group * dk
    tokens, hidden = normed.shape[0], shared_gate.shape[1]
    sharing = local.shape[1] // hidden
    part = tokens // sharing

    def body(s_ref, local_ref, qd_ref, gate_ref, gain_ref, normed_ref, sg_ref, su_ref, *refs):
        out_ref = refs[-1]
        first = s_ref[index.c] == 0
        between = jnp.ones((1, heads * dk), f32)
        incoming = jnp.zeros((dv, heads * dk), f32)
        sib = refs[0][...].astype(f32)
        for hop in range(1, (len(refs) - 2) // 2 + 1):
            mine, other = refs[2 * hop - 1][...].astype(f32), refs[2 * hop][...].astype(f32)
            inside = s_ref[index.z] >= hop
            early, late = jnp.where(first, mine, other), jnp.where(first, other, mine)
            decay = late[dv : dv + 1]
            got = early[0:dv] * decay + late[0:dv]
            incoming = incoming + jnp.where(inside, between * got, 0.0)
            between = jnp.where(inside, between * (early[dv : dv + 1] * decay), between)
        incoming = jnp.where(first, incoming, incoming * sib[dv : dv + 1] + sib[0:dv]).astype(bf16)
        lane = lax.broadcasted_iota(jnp.int32, (1, lanes), 1)
        for h in range(heads):
            at = slice(h // group * lanes, h // group * lanes + lanes)
            vs = slice(h * dv, (h + 1) * dv)
            mask = lane // dk == h % group
            q_h = jnp.where(mask, qd_ref[:, at], jnp.zeros((), bf16))
            value = local_ref[:, vs] + dot_nt(q_h, incoming[:, at])
            mean_square = jnp.mean(value * value, axis=1, keepdims=True)
            value = value * lax.rsqrt(mean_square + epsilon) * gain_ref[:, vs]
            out_ref[0:rows, vs] = (value * silu(gate_ref[:, vs].astype(f32))).astype(bf16)
        features = normed_ref[...]
        shared = (silu(dot(features, sg_ref[...])) * dot(features, su_ref[...])).astype(bf16)
        for i in range(sharing):
            out_ref[rows : rows + part, i * hidden : (i + 1) * hidden] = shared[
                i * part : (i + 1) * part
            ]

    out = jax.ShapeDtypeStruct((rows + part, local.shape[1]), bf16)
    operands = (index.vector, local, qd, gate_pre, gain[None, :], normed, shared_gate, shared_up)
    return call(body, out, operands + tuple(states), 1 << 27, smem=1)


def project(index, gathered, attention_weight, shared_weight, tokens):
    count = len(gathered)
    folded, width = gathered[0].shape
    hidden, columns = shared_weight.shape[0] // count, shared_weight.shape[1]
    sharing = width // hidden
    part = tokens // sharing
    rows = folded - part

    def body(s_ref, *refs):
        weight_ref, shared_ref, mixed_ref, out_ref = refs[count:]
        mixed = shared = 0.0
        for i in range(count):
            ref = refs[i]
            mixed = mixed + dot(ref[0:rows, :], index.rows(s_ref, index.tp + i, weight_ref, width))
            units = jnp.concatenate(
                [ref[rows:, q * hidden : (q + 1) * hidden] for q in range(sharing)], axis=0
            )
            shared = shared + dot(units, index.rows(s_ref, index.tp + i, shared_ref, hidden))
        mixed_ref[...] = mixed.astype(bf16)
        out_ref[...] = shared

    outs = (
        jax.ShapeDtypeStruct((rows, columns), bf16),
        jax.ShapeDtypeStruct((tokens, columns), f32),
    )
    operands = (index.vector, *gathered, attention_weight, shared_weight)
    return call(body, outs, operands, 2 * folded * width * columns * count, smem=1)


def prepare_rows(places, parts, rows, gain, index, scores, experts):
    tokens, width = rows.shape
    top = index.shape[1]
    piece = width // parts
    pad = -(-tokens // 128) * 128
    extra = -(-experts // 8) * 8

    def body(s_ref, rows_ref, gain_ref, index_ref, score_ref, normed_ref, packed_ref):
        value = rows_ref[...].astype(f32)
        mean_square = jnp.mean(value * value, axis=1, keepdims=True)
        normed = (value * lax.rsqrt(mean_square + epsilon) * gain_ref[...]).astype(bf16)
        normed_ref[...] = normed
        for q in range(parts):

            @pl.when(s_ref[places.part] == q)
            def _():
                packed_ref[0:tokens, :] = normed[:, q * piece : (q + 1) * piece]

        scores = score_ref[...]
        weights = routed_scale * scores / jnp.sum(scores, axis=0, keepdims=True)
        expert = lax.broadcasted_iota(jnp.int32, (extra, tokens), 0)
        named = jnp.zeros((extra, tokens), f32)
        weight = jnp.zeros((extra, tokens), f32)
        for k in range(top):
            hit = index_ref[k : k + 1, :] == expert
            named = jnp.where(hit, 1.0, named)
            weight = jnp.where(hit, weights[k : k + 1, :], weight)
        strict = (
            lax.broadcasted_iota(jnp.int32, (tokens, tokens), 0)
            < lax.broadcasted_iota(jnp.int32, (tokens, tokens), 1)
        ).astype(bf16)
        ranks = jnp.where(named > 0, dot(named.astype(bf16), strict), -1.0)
        packed_ref[tokens : tokens + extra, :] = jnp.full((extra, piece), -1.0, bf16)
        packed_ref[tokens : tokens + extra, 0:tokens] = ranks.astype(bf16)
        packed_ref[tokens : tokens + extra, pad : pad + tokens] = weight.astype(bf16)

    outs = (
        jax.ShapeDtypeStruct((tokens, width), bf16),
        jax.ShapeDtypeStruct((tokens + extra, piece), bf16),
    )
    operands = (places.vector, rows, gain[None, :], index.T, scores.T)
    return call(body, outs, operands, 1 << 22, smem=1)


def group_of(sources, capacity):
    group = 1
    while group < sources and group * capacity % 16:
        group *= 2
    return group


def expert_up(index, own, far, capacity, gate_weight, up_weight):
    parts = len(far[0])
    tokens, width = own[0].shape
    packed_rows, piece = own[1].shape
    extra = packed_rows - tokens
    pad = -(-tokens // 128) * 128
    sources = 1 + len(far)
    slots = sources * capacity
    group = group_of(sources, capacity)
    hidden = gate_weight.shape[1]
    step = min(256, hidden)
    flat = list(own) + [p for pieces in far for p in pieces]

    def body(s_ref, *refs):
        row_refs = refs[: len(flat)]
        gate_ref, up_ref, out_ref, info_ref, rows_ref, section_ref = refs[len(flat) :]
        expert = lax.broadcasted_iota(jnp.int32, (extra, 2 * pad), 0) == s_ref[index.e]
        if pad > tokens:
            for s in range(sources):
                rows_ref[s * pad + tokens : (s + 1) * pad, :] = jnp.zeros((pad - tokens, width), bf16)
        rows_ref[0:tokens, :] = row_refs[0][...]
        for q in range(parts):

            @pl.when(s_ref[index.part] == q)
            def _():
                for s in range(1, sources):
                    for i in range(parts):
                        to = (q - i) % parts
                        rows_ref[s * pad : s * pad + tokens, to * piece : (to + 1) * piece] = (
                            row_refs[2 + (s - 1) * parts + i][0:tokens, :]
                        )

        for s0 in range(0, sources, group):
            targets = []
            for s in range(s0, s0 + group):
                table_ref = row_refs[2 + (s - 1) * parts if s else 1]
                table = table_ref[tokens : tokens + extra, 0 : 2 * pad].astype(f32)
                mine = jnp.sum(jnp.where(expert, table, 0.0), axis=0, keepdims=True)
                info_ref[s : s + 1, :] = mine
                rank = mine[:, 0:pad]
                targets.append(jnp.where(rank >= 0, rank + (s - s0) * capacity, -1.0))
            target = jnp.concatenate(targets, axis=1) if group > 1 else targets[0]
            slot = lax.broadcasted_iota(jnp.int32, (group * capacity, group * pad), 0)
            picks = (slot.astype(f32) == target).astype(bf16)
            section_ref[s0 * capacity : (s0 + group) * capacity, :] = dot(
                picks, rows_ref[s0 * pad : (s0 + group) * pad, :]
            ).astype(bf16)
        for h in range(0, hidden, step):
            section = section_ref[...]
            gate_value = dot(section, gate_ref[:, h : h + step])
            up_value = dot(section, up_ref[:, h : h + step])
            out_ref[:, h : h + step] = (silu(gate_value) * up_value).astype(bf16)

    outs = (
        jax.ShapeDtypeStruct((slots, hidden), bf16),
        jax.ShapeDtypeStruct((sources, 2 * pad), f32),
    )
    scratch = (pltpu.VMEM((sources * pad, width), bf16), pltpu.VMEM((slots, width), bf16))
    operands = (index.vector, *flat, gate_weight, up_weight)
    return call(body, outs, operands, 4 * slots * width * hidden, smem=1, scratch=scratch)


def take_block(index, weight, place, hidden):
    def body(s_ref, in_ref, out_ref):
        out_ref[...] = index.rows(s_ref, place, in_ref, hidden)

    out = jax.ShapeDtypeStruct((hidden, weight.shape[1]), weight.dtype)
    return call(body, out, (index.vector, weight), 1 << 20, smem=1)


def down_first(index, hiddens, weight, traded):
    hidden, columns = hiddens[0].shape[1], weight.shape[1]
    chunks, partners = len(hiddens), len(traded)

    def body(s_ref, *refs):
        outs = refs[chunks + 1 + partners :]
        weights = [index.rows(s_ref, index.held, refs[chunks], hidden)]
        weights += [ref[...] for ref in refs[chunks + 1 : chunks + 1 + partners]]
        for w, weight in enumerate(weights):
            for h in range(chunks):
                outs[w * chunks + h][...] = dot(refs[h][...], weight)

    shapes = [
        jax.ShapeDtypeStruct((h.shape[0], columns), f32) for _ in range(1 + partners) for h in hiddens
    ]
    flops = 2 * sum(h.shape[0] for h in hiddens) * hidden * columns * (1 + partners)
    outs = call(body, shapes, (index.vector, *hiddens, weight, *traded), flops, smem=1)
    return [outs[w * chunks : (w + 1) * chunks] for w in range(1 + partners)]


def down_partner(first, hiddens, weights):
    count = len(hiddens)

    def body(first_ref, *refs):
        total = first_ref[...]
        for i in range(count):
            total = total + dot(refs[i][...], refs[count + i][...])
        refs[-1][...] = total.astype(bf16)

    out = jax.ShapeDtypeStruct(first.shape, bf16)
    flops = 2 * first.size * hiddens[0].shape[1] * count
    return call(body, out, (first, *hiddens, *weights), flops)


def down_own(index, firsts, gathered, weight):
    count, chunks = len(gathered), len(firsts)
    hidden, columns = gathered[0][0].shape[1], weight.shape[1]

    def body(s_ref, *refs):
        hidden_refs = refs[chunks : chunks + count * chunks]
        weight_ref = refs[chunks + count * chunks]
        outs = refs[chunks + count * chunks + 1 :]
        for h in range(chunks):
            total = refs[h][...]
            for i in range(count):
                rows = index.rows(s_ref, index.held + 1 + i, weight_ref, hidden)
                total = total + dot(hidden_refs[i * chunks + h][...], rows)
            outs[h][...] = total

    flat = [h for pieces in gathered for h in pieces]
    outs = [jax.ShapeDtypeStruct(f.shape, f32) for f in firsts]
    flops = 2 * sum(h.shape[0] for h in flat) * hidden * columns
    return call(body, outs, (index.vector, *firsts, *flat, weight), flops, smem=1)


def combine(own, back, info, tokens, capacity, out_type):
    slots, columns = own.shape
    sources = slots // capacity
    pad = info.shape[1] // 2
    group = group_of(sources, capacity)

    def body(own_ref, info_ref, *refs):
        out_ref = refs[-1]
        for s0 in range(0, sources, group):
            span = slice(s0 * capacity, (s0 + group) * capacity)
            value = own_ref[span, :]
            for ref in refs[:-1]:
                value = value + ref[span, :].astype(f32)
            value = value.astype(bf16)
            for s in range(s0, s0 + group):
                rank = info_ref[s : s + 1, 0:pad]
                target = jnp.where(rank >= 0, rank + (s - s0) * capacity, -1.0)
                slot = lax.broadcasted_iota(jnp.int32, (group * capacity, pad), 0).astype(f32)
                places = jnp.where(slot == target, info_ref[s : s + 1, pad : 2 * pad], 0.0)
                out_ref[s] = dot_tn(places.astype(bf16), value)[0:tokens].astype(out_type)

    out = jax.ShapeDtypeStruct((sources, tokens, columns), out_type)
    return call(body, out, (own, info, *back), 1 << 26)


def local(
    first_batch_queries,
    first_batch_keys,
    first_batch_values,
    output_gate_preactivation,
    decay_preactivation,
    channel_decay_bias,
    added_log_decay,
    head_norm_gain,
    attention_output_weight,
    second_batch_rows,
    expert_norm_gain,
    routed_expert_index,
    router_chosen_scores,
    expert_gate_weight,
    expert_up_weight,
    expert_down_weight,
    shared_gate_weight,
    shared_up_weight,
    shared_down_weight,
):
    at = Places()
    index = Index(at)
    n, chips, experts = at.side, at.chips, at.ep
    heads = added_log_decay.shape[0]
    tokens, top_count = routed_expert_index.shape
    capacity = tokens * top_count * 3 // (2 * experts)
    gate_weight, up_weight, down_weight = (
        expert_gate_weight[0],
        expert_up_weight[0],
        expert_down_weight[0],
    )
    hidden = gate_weight.shape[1]

    def down_block(k, i):
        return take_block(index, down_weight, index.given + (k - 1) * n + i, hidden)

    normed, packed = prepare_rows(
        index,
        n,
        second_batch_rows,
        expert_norm_gain,
        routed_expert_index,
        router_chosen_scores,
        experts,
    )
    far = [at.along_z(packed, k) for k in range(1, chips)]
    early = [down_block(k, 0) for k in range(1, n)]
    o_local, q_device, own_state = local_attention(
        first_batch_queries,
        first_batch_keys,
        first_batch_values,
        decay_preactivation,
        channel_decay_bias,
        added_log_decay,
    )
    far, own_state, early = hold((far, own_state, early))
    traded = [[at.along_v(early[k - 1], k)] for k in range(1, n)]
    arrived = [at.up_z(own_state, hop) for hop in range(1, chips)]
    far = [[a] + [at.along_u(a, i) for i in range(1, n)] for a in far]
    late = [[down_block(k, i) for i in range(1, n)] for k in range(1, n)]
    far, arrived, late = hold((far, arrived, late))
    states = [at.to_sibling(own_state)]
    for state in arrived:
        states += [state, at.to_sibling(state)]
    for k in range(1, n):
        traded[k - 1] += [at.along_v(block, k) for block in late[k - 1]]
    ups = [expert_up(index, (normed, packed), far, capacity, gate_weight, up_weight)]
    other = (
        (at.to_sibling(normed), at.to_sibling(packed)),
        [[at.to_sibling(p) for p in pieces] for pieces in far],
    )
    gathered_first = [at.along_u(ups[0][0], i) for i in range(1, n)]
    _, other = hold((ups[0][0], other))
    ups.append(expert_up(index, *other, capacity, gate_weight, up_weight))
    hiddens = [up[0] for up in ups]
    gathered_second = [at.along_u(hiddens[1], i) for i in range(1, n)]
    both = finish_attention(
        index,
        o_local,
        q_device,
        states,
        output_gate_preactivation,
        head_norm_gain,
        heads,
        normed,
        shared_gate_weight,
        shared_up_weight,
    )
    firsts = down_first(index, hiddens, down_weight, [t[0] for t in traded])

    def partials(chunk, gathered):
        return [
            down_partner(firsts[k][chunk], gathered, traded[k - 1][1:]) for k in range(1, n)
        ]

    partial = partials(0, gathered_first)
    back = [[at.along_v(partial[k - 1], -k) for k in range(1, n)]]
    gathered_second, both, _ = hold((gathered_second, both, partial))
    partial = partials(1, gathered_second)
    back.append([at.along_v(partial[k - 1], -k) for k in range(1, n)])
    gathered = [list(pair) for pair in zip(gathered_first, gathered_second)]
    owns = down_own(index, firsts[0], gathered, down_weight)
    here, there = [
        combine(owns[chunk], back[chunk], ups[chunk][1], tokens, capacity, (f32, bf16)[chunk])
        for chunk in range(2)
    ]
    there, to_send = hold((there, both))
    from_sibling = at.to_sibling(there)
    chip_sum = here + from_sibling.astype(f32)
    routed_total = chip_sum[0]
    for k in range(1, chips):
        routed_total = routed_total + at.along_z(chip_sum[k].astype(bf16), -k).astype(f32)

    mixed = [
        both if dy == 0 and dx == 0 else at.along_tp(to_send, dy, dx)
        for dy in range(n)
        for dx in range(n)
    ]
    token_mixed, shared_total = project(
        index, mixed, attention_output_weight, shared_down_weight, tokens
    )
    channel_mixed = (routed_total + shared_total).astype(bf16)
    return (token_mixed, channel_mixed)


def solution(mesh):
    placed = (
        P("ep", "tp"),
        P("ep", "tp"),
        P("ep", "tp"),
        P("ep", "tp"),
        P("ep", "tp"),
        P("tp"),
        P("tp", "ep"),
        P("tp"),
        P(None, "tp"),
        P("ep", None),
        P(),
        P("ep", None),
        P("ep", None),
        P("ep", None, "tp"),
        P("ep", None, "tp"),
        P("ep", None, "tp"),
        P(None, "tp"),
        P(None, "tp"),
        P(None, "tp"),
    )

    return jax.shard_map(
        local, mesh=mesh, in_specs=placed, out_specs=(P("ep", "tp"), P("ep", "tp")), check_vma=False
    )
```

```python
import math

import jax
import jax.numpy as jnp
from jax import lax
from jax.experimental import pallas as pl
from jax.experimental.pallas import tpu as pltpu
from jax.sharding import PartitionSpec as P


BLOCK = 64
epsilon = 1e-06
temper = 16.0
routed_scale = 2.5
highest = lax.Precision.HIGHEST
f32 = jnp.float32
bf16 = jnp.bfloat16
AXES = ("ep", "tp")


class Places:
    def __init__(self):
        self.ep, self.tp = lax.axis_size("ep"), lax.axis_size("tp")
        self.side = math.isqrt(self.tp)
        self.chips = self.ep // 2
        assert self.side * self.side == self.tp and self.chips * 2 == self.ep

    def pairs(self, move):
        n = self.side
        out = []
        for e in range(self.ep):
            for j in range(self.tp):
                z, c, y, x = move(e // 2, e % 2, j // n, j % n)
                if 0 <= z < self.chips:
                    out.append((e * self.tp + j, (z * 2 + c) * self.tp + (y % n) * n + x % n))
        return out

    def send(self, value, move):
        return lax.ppermute(value, AXES, self.pairs(move))

    def along_z(self, value, k):
        return self.send(value, lambda z, c, y, x: ((z + k) % self.chips, c, y, x))

    def up_z(self, value, k):
        return self.send(value, lambda z, c, y, x: (z + k, c, y, x))

    def to_sibling(self, value):
        return self.send(value, lambda z, c, y, x: (z, 1 - c, y, x))

    def along_u(self, value, k):
        return self.send(value, lambda z, c, y, x: (z, c, y, x + k) if c == 0 else (z, c, y + k, x))

    def along_v(self, value, k):
        return self.send(value, lambda z, c, y, x: (z, c, y + k, x) if c == 0 else (z, c, y, x + k))

    def along_tp(self, value, dy, dx):
        return self.send(value, lambda z, c, y, x: (z, c, y + dy, x + dx))


def dot(a, b, precision=None):
    return jnp.dot(a, b, preferred_element_type=f32, precision=precision)


def dot_nt(a, b):
    return lax.dot_general(a, b, (((1,), (1,)), ((), ())), preferred_element_type=f32)


def dot_tn(a, b, precision=None):
    return lax.dot_general(
        a, b, (((0,), (0,)), ((), ())), preferred_element_type=f32, precision=precision
    )


def hold(values):
    return lax.optimization_barrier(values)


def silu(value):
    return value / (1.0 + jnp.exp(-value))


class Here:
    def __init__(self, places):
        n = self.side = places.side
        self.e = lax.axis_index("ep")
        j = lax.axis_index("tp")
        self.z, self.c = lax.div(self.e, 2), lax.rem(self.e, 2)
        self.y, self.x = lax.div(j, n), lax.rem(j, n)
        self.part = lax.rem(self.x + self.y, n)

    def along(self, dy, dx):
        n = self.side
        return lax.rem(self.y + dy % n, n) * n + lax.rem(self.x + dx % n, n)

    def column(self, du, dv):
        return jnp.where(self.c == 0, self.along(dv, du), self.along(du, dv))


def rows_of(ref, block, size):
    return ref[pl.ds(pl.multiple_of(block * size, size), size), :]


def call(body, outs, operands, flops, scratch=(), far=0):
    given = list(operands[:far])
    given += [pltpu.with_memory_space_constraint(v, pltpu.VMEM) for v in operands[far:]]
    return pl.pallas_call(
        body,
        out_shape=jax.tree.map(lambda o: pltpu.VMEM(o.shape, o.dtype), outs),
        in_specs=[pl.BlockSpec(memory_space=pltpu.HBM)] * far
        + [pl.BlockSpec(memory_space=pltpu.VMEM)] * (len(operands) - far),
        out_specs=jax.tree.map(lambda _: pl.BlockSpec(memory_space=pltpu.VMEM), outs),
        scratch_shapes=list(scratch),
        compiler_params=pltpu.CompilerParams(vmem_limit_bytes=12 << 20),
        cost_estimate=pl.CostEstimate(flops=flops, transcendentals=0, bytes_accessed=0),
    )(*given)


def local_attention(q, k, v, decay_pre, bias, added):
    heads, rows = added.shape
    dk, dv = q.shape[1] // heads, v.shape[1] // heads
    blocks = rows // BLOCK
    group = min(max(1, 128 // dk), heads)
    lanes = group * dk

    def body(q_ref, k_ref, v_ref, d_ref, bias_ref, added_ref, o_ref, qd_ref, pack_ref):
        spread = (
            lax.broadcasted_iota(jnp.int32, (heads, heads * dk), 1) // dk
            == lax.broadcasted_iota(jnp.int32, (heads, heads * dk), 0)
        ).astype(f32)
        logits = d_ref[...].astype(f32) + bias_ref[...]
        base = jnp.minimum(logits, 0.0) - jnp.log1p(jnp.exp(-jnp.abs(logits)))
        decay = base / temper + dot_tn(added_ref[...], spread, highest)
        row = lax.broadcasted_iota(jnp.int32, (BLOCK, BLOCK), 0)
        col = lax.broadcasted_iota(jnp.int32, (BLOCK, BLOCK), 1)
        lower = row >= col
        lower_f = lower.astype(f32)
        lane = lax.broadcasted_iota(jnp.int32, (1, lanes), 1)
        masks = [(lane // dk == g).astype(f32) for g in range(group)]
        states = [None] * heads
        lead = jnp.zeros((1, heads * dk), f32)
        for b in range(blocks):
            span = slice(b * BLOCK, (b + 1) * BLOCK)
            running = dot(lower_f, decay[span], highest)
            total = running[BLOCK - 1 : BLOCK, :]
            grow = jnp.exp(running)
            q_dec = q_ref[span, :].astype(f32) * grow
            keys = k_ref[span, :].astype(f32)
            k_up = (keys * jnp.exp(-running)).astype(bf16)
            k_end = (keys * jnp.exp(total - running)).astype(bf16)
            qd_ref[span, :] = (q_dec * jnp.exp(lead)).astype(bf16)
            shrink = jnp.exp(total)
            for h in range(heads):
                at = slice(h // group * lanes, h // group * lanes + lanes)
                q_h = (q_dec[:, at] * masks[h % group]).astype(bf16)
                v_h = v_ref[span, h * dv : (h + 1) * dv]
                scores = jnp.where(lower, dot_nt(q_h, k_up[:, at]), 0.0).astype(bf16)
                value = dot(scores, v_h)
                if b:
                    value = value + dot_nt(q_h, states[h].astype(bf16))
                o_ref[span, h * dv : (h + 1) * dv] = value
                update = dot_tn(v_h, k_end[:, at])
                states[h] = update if b == 0 else states[h] * shrink[:, at] + update
            lead = lead + total
        for h0 in range(0, heads, group):
            packed = states[h0]
            for g in range(1, group):
                packed = jnp.where(lane // dk == g, states[h0 + g], packed)
            pack_ref[0:dv, h0 * dk : h0 * dk + lanes] = packed.astype(bf16)
        pack_ref[dv : dv + 8, :] = jnp.broadcast_to(jnp.exp(lead), (8, heads * dk)).astype(bf16)

    outs = (
        jax.ShapeDtypeStruct((rows, heads * dv), f32),
        jax.ShapeDtypeStruct((rows, heads * dk), bf16),
        jax.ShapeDtypeStruct((dv + 8, heads * dk), bf16),
    )
    return call(body, outs, (q, k, v, decay_pre, bias[None, :], added), 1 << 25)


def finish_attention(
    places, local, qd, states, gate_pre, gain, heads, normed, shared_gate, shared_up
):
    rows = local.shape[0]
    dv, dk = local.shape[1] // heads, qd.shape[1] // heads
    group = min(max(1, 128 // dk), heads)
    lanes = group * dk
    tokens, hidden = normed.shape[0], shared_gate.shape[1]
    sharing = local.shape[1] // hidden
    part = tokens // sharing

    def body(local_ref, qd_ref, gate_ref, gain_ref, normed_ref, sg_ref, su_ref, *refs):
        out_ref = refs[-1]
        here = Here(places)
        first = here.c == 0
        between = jnp.ones((1, heads * dk), f32)
        incoming = jnp.zeros((dv, heads * dk), f32)
        sib = refs[0][...].astype(f32)
        for hop in range(1, (len(refs) - 2) // 2 + 1):
            mine, other = refs[2 * hop - 1][...].astype(f32), refs[2 * hop][...].astype(f32)
            inside = here.z >= hop
            early, late = jnp.where(first, mine, other), jnp.where(first, other, mine)
            decay = late[dv : dv + 1]
            got = early[0:dv] * decay + late[0:dv]
            incoming = incoming + jnp.where(inside, between * got, 0.0)
            between = jnp.where(inside, between * (early[dv : dv + 1] * decay), between)
        incoming = jnp.where(first, incoming, incoming * sib[dv : dv + 1] + sib[0:dv]).astype(bf16)
        lane = lax.broadcasted_iota(jnp.int32, (1, lanes), 1)
        for h in range(heads):
            at = slice(h // group * lanes, h // group * lanes + lanes)
            vs = slice(h * dv, (h + 1) * dv)
            mask = lane // dk == h % group
            q_h = jnp.where(mask, qd_ref[:, at], jnp.zeros((), bf16))
            value = local_ref[:, vs] + dot_nt(q_h, incoming[:, at])
            mean_square = jnp.mean(value * value, axis=1, keepdims=True)
            value = value * lax.rsqrt(mean_square + epsilon) * gain_ref[:, vs]
            out_ref[0:rows, vs] = (value * silu(gate_ref[:, vs].astype(f32))).astype(bf16)
        features = normed_ref[...]
        shared = (silu(dot(features, sg_ref[...])) * dot(features, su_ref[...])).astype(bf16)
        for i in range(sharing):
            out_ref[rows : rows + part, i * hidden : (i + 1) * hidden] = shared[
                i * part : (i + 1) * part
            ]

    out = jax.ShapeDtypeStruct((rows + part, local.shape[1]), bf16)
    operands = (local, qd, gate_pre, gain[None, :], normed, shared_gate, shared_up)
    return call(body, out, operands + tuple(states), 1 << 27)


def project(places, gathered, attention_weight, shared_weight, tokens):
    count = len(gathered)
    folded, width = gathered[0].shape
    hidden, columns = shared_weight.shape[0] // count, shared_weight.shape[1]
    sharing = width // hidden
    part = tokens // sharing
    rows = folded - part

    def body(*refs):
        weight_ref, shared_ref, mixed_ref, out_ref = refs[count:]
        mixed = shared = 0.0
        here = Here(places)
        for i in range(count):
            ref = refs[i]
            block = here.along(-(i // here.side), -(i % here.side))
            mixed = mixed + dot(ref[0:rows, :], rows_of(weight_ref, block, width))
            units = jnp.concatenate(
                [ref[rows:, q * hidden : (q + 1) * hidden] for q in range(sharing)], axis=0
            )
            shared = shared + dot(units, rows_of(shared_ref, block, hidden))
        mixed_ref[...] = mixed.astype(bf16)
        out_ref[...] = shared

    outs = (
        jax.ShapeDtypeStruct((rows, columns), bf16),
        jax.ShapeDtypeStruct((tokens, columns), f32),
    )
    operands = (*gathered, attention_weight, shared_weight)
    return call(body, outs, operands, 2 * folded * width * columns * count)


def prepare_rows(places, parts, rows, gain, index, scores, experts):
    tokens, width = rows.shape
    top = index.shape[1]
    piece = width // parts
    pad = -(-tokens // 128) * 128
    extra = -(-experts // 8) * 8

    def body(rows_hbm, gain_hbm, index_hbm, score_hbm, normed_ref, packed_ref, *scratch):
        rows_ref, gain_ref, index_ref, score_ref, done = scratch
        copies = [
            pltpu.make_async_copy(source, target, done.at[i])
            for i, (source, target) in enumerate(
                zip((rows_hbm, gain_hbm, index_hbm, score_hbm), scratch[:4])
            )
        ]
        for copy in copies:
            copy.start()
        for copy in copies:
            copy.wait()
        here = Here(places)
        value = rows_ref[...].astype(f32)
        mean_square = jnp.mean(value * value, axis=1, keepdims=True)
        normed = (value * lax.rsqrt(mean_square + epsilon) * gain_ref[...]).astype(bf16)
        normed_ref[...] = normed
        for q in range(parts):

            @pl.when(here.part == q)
            def _():
                packed_ref[0:tokens, :] = normed[:, q * piece : (q + 1) * piece]

        scores = score_ref[...]
        weights = routed_scale * scores / jnp.sum(scores, axis=0, keepdims=True)
        expert = lax.broadcasted_iota(jnp.int32, (extra, tokens), 0)
        named = jnp.zeros((extra, tokens), f32)
        weight = jnp.zeros((extra, tokens), f32)
        for k in range(top):
            hit = index_ref[k : k + 1, :] == expert
            named = jnp.where(hit, 1.0, named)
            weight = jnp.where(hit, weights[k : k + 1, :], weight)
        strict = (
            lax.broadcasted_iota(jnp.int32, (tokens, tokens), 0)
            < lax.broadcasted_iota(jnp.int32, (tokens, tokens), 1)
        ).astype(bf16)
        ranks = jnp.where(named > 0, dot(named.astype(bf16), strict), -1.0)
        packed_ref[tokens : tokens + extra, :] = jnp.full((extra, piece), -1.0, bf16)
        packed_ref[tokens : tokens + extra, 0:tokens] = ranks.astype(bf16)
        packed_ref[tokens : tokens + extra, pad : pad + tokens] = weight.astype(bf16)

    outs = (
        jax.ShapeDtypeStruct((tokens, width), bf16),
        jax.ShapeDtypeStruct((tokens + extra, piece), bf16),
    )
    operands = (rows, gain[None, :], index.T, scores.T)
    scratch = [pltpu.VMEM(v.shape, v.dtype) for v in operands]
    scratch.append(pltpu.SemaphoreType.DMA((4,)))
    return call(body, outs, operands, 1 << 22, scratch=scratch, far=4)


def group_of(sources, capacity):
    group = 1
    while group < sources and group * capacity % 16:
        group *= 2
    return group


def expert_up(places, own, far, capacity, gate_weight, up_weight):
    parts = len(far[0])
    tokens, width = own[0].shape
    packed_rows, piece = own[1].shape
    extra = packed_rows - tokens
    pad = -(-tokens // 128) * 128
    sources = 1 + len(far)
    slots = sources * capacity
    group = group_of(sources, capacity)
    hidden = gate_weight.shape[1]
    step = min(256, hidden)
    flat = list(own) + [p for pieces in far for p in pieces]

    def body(*refs):
        row_refs = refs[: len(flat)]
        gate_ref, up_ref, out_ref, info_ref, rows_ref, section_ref = refs[len(flat) :]
        here = Here(places)
        expert = lax.broadcasted_iota(jnp.int32, (extra, 2 * pad), 0) == here.e
        if pad > tokens:
            for s in range(sources):
                rows_ref[s * pad + tokens : (s + 1) * pad, :] = jnp.zeros((pad - tokens, width), bf16)
        rows_ref[0:tokens, :] = row_refs[0][...]
        for q in range(parts):

            @pl.when(here.part == q)
            def _():
                for s in range(1, sources):
                    for i in range(parts):
                        to = (q - i) % parts
                        rows_ref[s * pad : s * pad + tokens, to * piece : (to + 1) * piece] = (
                            row_refs[2 + (s - 1) * parts + i][0:tokens, :]
                        )

        for s0 in range(0, sources, group):
            targets = []
            for s in range(s0, s0 + group):
                table_ref = row_refs[2 + (s - 1) * parts if s else 1]
                table = table_ref[tokens : tokens + extra, 0 : 2 * pad].astype(f32)
                mine = jnp.sum(jnp.where(expert, table, 0.0), axis=0, keepdims=True)
                info_ref[s : s + 1, :] = mine
                rank = mine[:, 0:pad]
                targets.append(jnp.where(rank >= 0, rank + (s - s0) * capacity, -1.0))
            target = jnp.concatenate(targets, axis=1) if group > 1 else targets[0]
            slot = lax.broadcasted_iota(jnp.int32, (group * capacity, group * pad), 0)
            picks = (slot.astype(f32) == target).astype(bf16)
            section_ref[s0 * capacity : (s0 + group) * capacity, :] = dot(
                picks, rows_ref[s0 * pad : (s0 + group) * pad, :]
            ).astype(bf16)
        for h in range(0, hidden, step):
            section = section_ref[...]
            gate_value = dot(section, gate_ref[:, h : h + step])
            up_value = dot(section, up_ref[:, h : h + step])
            out_ref[:, h : h + step] = (silu(gate_value) * up_value).astype(bf16)

    outs = (
        jax.ShapeDtypeStruct((slots, hidden), bf16),
        jax.ShapeDtypeStruct((sources, 2 * pad), f32),
    )
    scratch = (pltpu.VMEM((sources * pad, width), bf16), pltpu.VMEM((slots, width), bf16))
    operands = (*flat, gate_weight, up_weight)
    return call(body, outs, operands, 4 * slots * width * hidden, scratch=scratch)


def take_block(places, weight, du, dv, hidden):
    def body(in_ref, out_ref, done):
        start = pl.multiple_of(Here(places).column(du, dv) * hidden, hidden)
        copy = pltpu.make_async_copy(in_ref.at[pl.ds(start, hidden), :], out_ref, done)
        copy.start()
        copy.wait()

    out = jax.ShapeDtypeStruct((hidden, weight.shape[1]), weight.dtype)
    return call(body, out, (weight,), 1 << 20, scratch=(pltpu.SemaphoreType.DMA,), far=1)


def down_first(places, hiddens, weight, traded):
    hidden, columns = hiddens[0].shape[1], weight.shape[1]
    chunks, partners = len(hiddens), len(traded)

    def body(*refs):
        outs = refs[chunks + 1 + partners :]
        weights = [rows_of(refs[chunks], Here(places).column(0, 0), hidden)]
        weights += [ref[...] for ref in refs[chunks + 1 : chunks + 1 + partners]]
        for w, weight in enumerate(weights):
            for h in range(chunks):
                outs[w * chunks + h][...] = dot(refs[h][...], weight)

    shapes = [
        jax.ShapeDtypeStruct((h.shape[0], columns), f32) for _ in range(1 + partners) for h in hiddens
    ]
    flops = 2 * sum(h.shape[0] for h in hiddens) * hidden * columns * (1 + partners)
    outs = call(body, shapes, (*hiddens, weight, *traded), flops)
    return [outs[w * chunks : (w + 1) * chunks] for w in range(1 + partners)]


def down_partner(first, hiddens, weights):
    count = len(hiddens)

    def body(first_ref, *refs):
        total = first_ref[...]
        for i in range(count):
            total = total + dot(refs[i][...], refs[count + i][...])
        refs[-1][...] = total.astype(bf16)

    out = jax.ShapeDtypeStruct(first.shape, bf16)
    flops = 2 * first.size * hiddens[0].shape[1] * count
    return call(body, out, (first, *hiddens, *weights), flops)


def down_own(places, firsts, gathered, weight):
    count, chunks = len(gathered), len(firsts)
    hidden, columns = gathered[0][0].shape[1], weight.shape[1]

    def body(*refs):
        hidden_refs = refs[chunks : chunks + count * chunks]
        weight_ref = refs[chunks + count * chunks]
        outs = refs[chunks + count * chunks + 1 :]
        here = Here(places)
        for h in range(chunks):
            total = refs[h][...]
            for i in range(count):
                rows = rows_of(weight_ref, here.column(-1 - i, 0), hidden)
                total = total + dot(hidden_refs[i * chunks + h][...], rows)
            outs[h][...] = total

    flat = [h for pieces in gathered for h in pieces]
    outs = [jax.ShapeDtypeStruct(f.shape, f32) for f in firsts]
    flops = 2 * sum(h.shape[0] for h in flat) * hidden * columns
    return call(body, outs, (*firsts, *flat, weight), flops)


def combine(own, back, info, tokens, capacity, out_type):
    slots, columns = own.shape
    sources = slots // capacity
    pad = info.shape[1] // 2
    group = group_of(sources, capacity)

    def body(own_ref, info_ref, *refs):
        out_ref = refs[-1]
        for s0 in range(0, sources, group):
            span = slice(s0 * capacity, (s0 + group) * capacity)
            value = own_ref[span, :]
            for ref in refs[:-1]:
                value = value + ref[span, :].astype(f32)
            value = value.astype(bf16)
            for s in range(s0, s0 + group):
                rank = info_ref[s : s + 1, 0:pad]
                target = jnp.where(rank >= 0, rank + (s - s0) * capacity, -1.0)
                slot = lax.broadcasted_iota(jnp.int32, (group * capacity, pad), 0).astype(f32)
                places = jnp.where(slot == target, info_ref[s : s + 1, pad : 2 * pad], 0.0)
                out_ref[s] = dot_tn(places.astype(bf16), value)[0:tokens].astype(out_type)

    out = jax.ShapeDtypeStruct((sources, tokens, columns), out_type)
    return call(body, out, (own, info, *back), 1 << 26)


def local(
    first_batch_queries,
    first_batch_keys,
    first_batch_values,
    output_gate_preactivation,
    decay_preactivation,
    channel_decay_bias,
    added_log_decay,
    head_norm_gain,
    attention_output_weight,
    second_batch_rows,
    expert_norm_gain,
    routed_expert_index,
    router_chosen_scores,
    expert_gate_weight,
    expert_up_weight,
    expert_down_weight,
    shared_gate_weight,
    shared_up_weight,
    shared_down_weight,
):
    at = Places()
    n, chips, experts = at.side, at.chips, at.ep
    heads = added_log_decay.shape[0]
    tokens, top_count = routed_expert_index.shape
    capacity = tokens * top_count * 3 // (2 * experts)
    gate_weight, up_weight, down_weight = (
        expert_gate_weight[0],
        expert_up_weight[0],
        expert_down_weight[0],
    )
    hidden = gate_weight.shape[1]

    def trade(k, i):
        return at.along_v(take_block(at, down_weight, -i, k, hidden), k)

    normed, packed = prepare_rows(
        at,
        n,
        second_batch_rows,
        expert_norm_gain,
        routed_expert_index,
        router_chosen_scores,
        experts,
    )
    middle = chips // 2
    far = {middle: at.along_z(packed, middle)}
    traded = [[trade(k, 0)] for k in range(1, n)]
    far |= {k: at.along_z(packed, k) for k in range(1, chips) if k != middle}
    for k in range(1, n):
        traded[k - 1] += [trade(k, i) for i in range(1, n)]
    o_local, q_device, own_state = local_attention(
        first_batch_queries,
        first_batch_keys,
        first_batch_values,
        decay_preactivation,
        channel_decay_bias,
        added_log_decay,
    )
    arrived = [at.along_z(own_state, hop) for hop in range(1, chips)]
    states = [at.to_sibling(own_state)]
    for state in arrived:
        states += [state, at.to_sibling(state)]
    parts = [far[k] for k in range(1, chips)]
    far = [[a] + [at.along_u(a, i) for i in range(1, n)] for a in parts]
    other = ((at.to_sibling(normed), at.to_sibling(packed)), [[at.to_sibling(a)] for a in parts])
    for pieces, others in zip(far, other[1]):
        others += [at.to_sibling(p) for p in pieces[1:]]
    ups = [expert_up(at, (normed, packed), far, capacity, gate_weight, up_weight)]
    gathered_first = [at.along_u(ups[0][0], i) for i in range(1, n)]
    _, other = hold((ups[0][0], other))
    ups.append(expert_up(at, *other, capacity, gate_weight, up_weight))
    hiddens = [up[0] for up in ups]
    gathered_second = [at.along_u(hiddens[1], i) for i in range(1, n)]
    both = finish_attention(
        at,
        o_local,
        q_device,
        states,
        output_gate_preactivation,
        head_norm_gain,
        heads,
        normed,
        shared_gate_weight,
        shared_up_weight,
    )
    firsts = down_first(at, hiddens, down_weight, [t[0] for t in traded])

    def partials(chunk, gathered):
        return [
            down_partner(firsts[k][chunk], gathered, traded[k - 1][1:]) for k in range(1, n)
        ]

    partial = partials(0, gathered_first)
    back = [[at.along_v(partial[k - 1], -k) for k in range(1, n)]]
    gathered_second, both, _ = hold((gathered_second, both, partial))
    partial = partials(1, gathered_second)
    back.append([at.along_v(partial[k - 1], -k) for k in range(1, n)])
    gathered = [list(pair) for pair in zip(gathered_first, gathered_second)]
    owns = down_own(at, firsts[0], gathered, down_weight)
    here, there = [
        combine(owns[chunk], back[chunk], ups[chunk][1], tokens, capacity, (f32, bf16)[chunk])
        for chunk in range(2)
    ]
    there, to_send = hold((there, both))
    from_sibling = at.to_sibling(there)
    chip_sum = here + from_sibling.astype(f32)
    routed_total = chip_sum[0]
    for k in range(1, chips):
        routed_total = routed_total + at.along_z(chip_sum[k].astype(bf16), -k).astype(f32)

    mixed = [
        both if dy == 0 and dx == 0 else at.along_tp(to_send, dy, dx)
        for dy in range(n)
        for dx in range(n)
    ]
    token_mixed, shared_total = project(
        at, mixed, attention_output_weight, shared_down_weight, tokens
    )
    channel_mixed = (routed_total + shared_total).astype(bf16)
    return (token_mixed, channel_mixed)


def solution(mesh):
    placed = (
        P("ep", "tp"),
        P("ep", "tp"),
        P("ep", "tp"),
        P("ep", "tp"),
        P("ep", "tp"),
        P("tp"),
        P("tp", "ep"),
        P("tp"),
        P(None, "tp"),
        P("ep", None),
        P(),
        P("ep", None),
        P("ep", None),
        P("ep", None, "tp"),
        P("ep", None, "tp"),
        P("ep", None, "tp"),
        P(None, "tp"),
        P(None, "tp"),
        P(None, "tp"),
    )

    return jax.shard_map(
        local, mesh=mesh, in_specs=placed, out_specs=(P("ep", "tp"), P("ep", "tp")), check_vma=False
    )
```

```python
import math

import jax
import jax.numpy as jnp
from jax import lax
from jax.experimental import pallas as pl
from jax.experimental.pallas import tpu as pltpu
from jax.sharding import PartitionSpec as P


BLOCK = 64
PIECES = 2
epsilon = 1e-06
temper = 16.0
routed_scale = 2.5
highest = lax.Precision.HIGHEST
f32 = jnp.float32
bf16 = jnp.bfloat16
AXES = ("ep", "tp")


class Places:
    def __init__(self):
        self.ep, self.tp = lax.axis_size("ep"), lax.axis_size("tp")
        self.side = math.isqrt(self.tp)
        self.chips = self.ep // 2
        assert self.side * self.side == self.tp and self.chips * 2 == self.ep

    def pairs(self, move):
        n = self.side
        out = []
        for e in range(self.ep):
            for j in range(self.tp):
                z, c, y, x = move(e // 2, e % 2, j // n, j % n)
                if 0 <= z < self.chips:
                    out.append((e * self.tp + j, (z * 2 + c) * self.tp + (y % n) * n + x % n))
        return out

    def send(self, value, move):
        return lax.ppermute(value, AXES, self.pairs(move))

    def along_z(self, value, k):
        return self.send(value, lambda z, c, y, x: ((z + k) % self.chips, c, y, x))

    def up_z(self, value, k):
        return self.send(value, lambda z, c, y, x: (z + k, c, y, x))

    def to_sibling(self, value):
        return self.send(value, lambda z, c, y, x: (z, 1 - c, y, x))

    def along_u(self, value, k):
        return self.send(value, lambda z, c, y, x: (z, c, y, x + k) if c == 0 else (z, c, y + k, x))

    def along_v(self, value, k):
        return self.send(value, lambda z, c, y, x: (z, c, y + k, x) if c == 0 else (z, c, y, x + k))

    def along_tp(self, value, dy, dx):
        return self.send(value, lambda z, c, y, x: (z, c, y + dy, x + dx))


def dot(a, b, precision=None):
    return jnp.dot(a, b, preferred_element_type=f32, precision=precision)


def dot_nt(a, b):
    return lax.dot_general(a, b, (((1,), (1,)), ((), ())), preferred_element_type=f32)


def dot_tn(a, b, precision=None):
    return lax.dot_general(
        a, b, (((0,), (0,)), ((), ())), preferred_element_type=f32, precision=precision
    )


def hold(values):
    return lax.optimization_barrier(values)


def silu(value):
    return value / (1.0 + jnp.exp(-value))


class Here:
    def __init__(self, places):
        n = self.side = places.side
        self.e = lax.axis_index("ep")
        j = lax.axis_index("tp")
        self.z, self.c = lax.div(self.e, 2), lax.rem(self.e, 2)
        self.y, self.x = lax.div(j, n), lax.rem(j, n)
        self.part = lax.rem(self.x + self.y, n)

    def along(self, dy, dx):
        n = self.side
        return lax.rem(self.y + dy % n, n) * n + lax.rem(self.x + dx % n, n)

    def column(self, du, dv):
        return jnp.where(self.c == 0, self.along(dv, du), self.along(du, dv))


def rows_of(ref, block, size):
    return ref[pl.ds(pl.multiple_of(block * size, size), size), :]


def call(body, outs, operands, flops, scratch=(), far=0):
    given = [pltpu.with_memory_space_constraint(v, pltpu.HBM) for v in operands[:far]]
    given += [pltpu.with_memory_space_constraint(v, pltpu.VMEM) for v in operands[far:]]
    return pl.pallas_call(
        body,
        out_shape=jax.tree.map(lambda o: pltpu.VMEM(o.shape, o.dtype), outs),
        in_specs=[pl.BlockSpec(memory_space=pltpu.HBM)] * far
        + [pl.BlockSpec(memory_space=pltpu.VMEM)] * (len(operands) - far),
        out_specs=jax.tree.map(lambda _: pl.BlockSpec(memory_space=pltpu.VMEM), outs),
        scratch_shapes=list(scratch),
        compiler_params=pltpu.CompilerParams(vmem_limit_bytes=12 << 20),
        cost_estimate=pl.CostEstimate(flops=flops, transcendentals=0, bytes_accessed=0),
    )(*given)


def local_attention(q, k, v, decay_pre, bias, added):
    heads, rows = added.shape
    dk, dv = q.shape[1] // heads, v.shape[1] // heads
    blocks = rows // BLOCK
    group = min(max(1, 128 // dk), heads)
    lanes = group * dk

    def body(q_ref, k_ref, v_ref, d_ref, bias_ref, added_ref, o_ref, qd_ref, pack_ref):
        spread = (
            lax.broadcasted_iota(jnp.int32, (heads, heads * dk), 1) // dk
            == lax.broadcasted_iota(jnp.int32, (heads, heads * dk), 0)
        ).astype(f32)
        logits = d_ref[...].astype(f32) + bias_ref[...]
        base = jnp.minimum(logits, 0.0) - jnp.log1p(jnp.exp(-jnp.abs(logits)))
        decay = base / temper + dot_tn(added_ref[...], spread, highest)
        row = lax.broadcasted_iota(jnp.int32, (BLOCK, BLOCK), 0)
        col = lax.broadcasted_iota(jnp.int32, (BLOCK, BLOCK), 1)
        lower = row >= col
        lower_f = lower.astype(f32)
        lane = lax.broadcasted_iota(jnp.int32, (1, lanes), 1)
        masks = [(lane // dk == g).astype(f32) for g in range(group)]
        states = [None] * heads
        lead = jnp.zeros((1, heads * dk), f32)
        for b in range(blocks):
            span = slice(b * BLOCK, (b + 1) * BLOCK)
            running = dot(lower_f, decay[span], highest)
            total = running[BLOCK - 1 : BLOCK, :]
            grow = jnp.exp(running)
            q_dec = q_ref[span, :].astype(f32) * grow
            keys = k_ref[span, :].astype(f32)
            k_up = (keys * jnp.exp(-running)).astype(bf16)
            k_end = (keys * jnp.exp(total - running)).astype(bf16)
            qd_ref[span, :] = (q_dec * jnp.exp(lead)).astype(bf16)
            shrink = jnp.exp(total)
            for h in range(heads):
                at = slice(h // group * lanes, h // group * lanes + lanes)
                q_h = (q_dec[:, at] * masks[h % group]).astype(bf16)
                v_h = v_ref[span, h * dv : (h + 1) * dv]
                scores = jnp.where(lower, dot_nt(q_h, k_up[:, at]), 0.0).astype(bf16)
                value = dot(scores, v_h)
                if b:
                    value = value + dot_nt(q_h, states[h].astype(bf16))
                o_ref[span, h * dv : (h + 1) * dv] = value
                update = dot_tn(v_h, k_end[:, at])
                states[h] = update if b == 0 else states[h] * shrink[:, at] + update
            lead = lead + total
        for h0 in range(0, heads, group):
            packed = states[h0]
            for g in range(1, group):
                packed = jnp.where(lane // dk == g, states[h0 + g], packed)
            pack_ref[0:dv, h0 * dk : h0 * dk + lanes] = packed.astype(bf16)
        pack_ref[dv : dv + 8, :] = jnp.broadcast_to(jnp.exp(lead), (8, heads * dk)).astype(bf16)

    outs = (
        jax.ShapeDtypeStruct((rows, heads * dv), f32),
        jax.ShapeDtypeStruct((rows, heads * dk), bf16),
        jax.ShapeDtypeStruct((dv + 8, heads * dk), bf16),
    )
    return call(body, outs, (q, k, v, decay_pre, bias[None, :], added), 1 << 25)


def finish_attention(
    places, local, qd, states, gate_pre, gain, heads, normed, shared_gate, shared_up
):
    rows = local.shape[0]
    dv, dk = local.shape[1] // heads, qd.shape[1] // heads
    group = min(max(1, 128 // dk), heads)
    lanes = group * dk
    tokens, hidden = normed.shape[0], shared_gate.shape[1]
    sharing = local.shape[1] // hidden
    part = tokens // sharing

    def body(local_ref, qd_ref, gate_ref, gain_ref, normed_ref, sg_ref, su_ref, *refs):
        out_ref = refs[-1]
        here = Here(places)
        first = here.c == 0
        between = jnp.ones((1, heads * dk), f32)
        incoming = jnp.zeros((dv, heads * dk), f32)
        sib = refs[0][...].astype(f32)
        for hop in range(1, (len(refs) - 2) // 2 + 1):
            mine, other = refs[2 * hop - 1][...].astype(f32), refs[2 * hop][...].astype(f32)
            inside = here.z >= hop
            early, late = jnp.where(first, mine, other), jnp.where(first, other, mine)
            decay = late[dv : dv + 1]
            got = early[0:dv] * decay + late[0:dv]
            incoming = incoming + jnp.where(inside, between * got, 0.0)
            between = jnp.where(inside, between * (early[dv : dv + 1] * decay), between)
        incoming = jnp.where(first, incoming, incoming * sib[dv : dv + 1] + sib[0:dv]).astype(bf16)
        lane = lax.broadcasted_iota(jnp.int32, (1, lanes), 1)
        for h in range(heads):
            at = slice(h // group * lanes, h // group * lanes + lanes)
            vs = slice(h * dv, (h + 1) * dv)
            mask = lane // dk == h % group
            q_h = jnp.where(mask, qd_ref[:, at], jnp.zeros((), bf16))
            value = local_ref[:, vs] + dot_nt(q_h, incoming[:, at])
            mean_square = jnp.mean(value * value, axis=1, keepdims=True)
            value = value * lax.rsqrt(mean_square + epsilon) * gain_ref[:, vs]
            out_ref[0:rows, vs] = (value * silu(gate_ref[:, vs].astype(f32))).astype(bf16)
        features = normed_ref[...]
        shared = (silu(dot(features, sg_ref[...])) * dot(features, su_ref[...])).astype(bf16)
        for i in range(sharing):
            out_ref[rows : rows + part, i * hidden : (i + 1) * hidden] = shared[
                i * part : (i + 1) * part
            ]

    out = jax.ShapeDtypeStruct((rows + part, local.shape[1]), bf16)
    operands = (local, qd, gate_pre, gain[None, :], normed, shared_gate, shared_up)
    return call(body, out, operands + tuple(states), 1 << 27)


def project(places, gathered, attention_weight, shared_weight, tokens):
    count = len(gathered)
    folded, width = gathered[0].shape
    hidden, columns = shared_weight.shape[0] // count, shared_weight.shape[1]
    sharing = width // hidden
    part = tokens // sharing
    rows = folded - part

    def body(*refs):
        weight_ref, shared_ref, mixed_ref, out_ref = refs[count:]
        mixed = shared = 0.0
        here = Here(places)
        for i in range(count):
            ref = refs[i]
            block = here.along(-(i // here.side), -(i % here.side))
            mixed = mixed + dot(ref[0:rows, :], rows_of(weight_ref, block, width))
            units = jnp.concatenate(
                [ref[rows:, q * hidden : (q + 1) * hidden] for q in range(sharing)], axis=0
            )
            shared = shared + dot(units, rows_of(shared_ref, block, hidden))
        mixed_ref[...] = mixed.astype(bf16)
        out_ref[...] = shared

    outs = (
        jax.ShapeDtypeStruct((rows, columns), bf16),
        jax.ShapeDtypeStruct((tokens, columns), f32),
    )
    operands = (*gathered, attention_weight, shared_weight)
    return call(body, outs, operands, 2 * folded * width * columns * count)


def prepare_rows(places, parts, rows, gain, index, scores, experts):
    tokens, width = rows.shape
    top = index.shape[1]
    piece = width // parts
    pad = -(-tokens // 128) * 128
    extra = -(-experts // 8) * 8

    def body(rows_hbm, gain_hbm, index_hbm, score_hbm, normed_ref, packed_ref, *scratch):
        rows_ref, gain_ref, index_ref, score_ref, done = scratch
        copies = [
            pltpu.make_async_copy(source, target, done.at[i])
            for i, (source, target) in enumerate(
                zip((rows_hbm, gain_hbm, index_hbm, score_hbm), scratch[:4])
            )
        ]
        for copy in copies:
            copy.start()
        for copy in copies:
            copy.wait()
        here = Here(places)
        value = rows_ref[...].astype(f32)
        mean_square = jnp.mean(value * value, axis=1, keepdims=True)
        normed = (value * lax.rsqrt(mean_square + epsilon) * gain_ref[...]).astype(bf16)
        normed_ref[...] = normed
        for q in range(parts):

            @pl.when(here.part == q)
            def _():
                packed_ref[0:tokens, :] = normed[:, q * piece : (q + 1) * piece]

        scores = score_ref[...]
        weights = routed_scale * scores / jnp.sum(scores, axis=0, keepdims=True)
        expert = lax.broadcasted_iota(jnp.int32, (extra, tokens), 0)
        named = jnp.zeros((extra, tokens), f32)
        weight = jnp.zeros((extra, tokens), f32)
        for k in range(top):
            hit = index_ref[k : k + 1, :] == expert
            named = jnp.where(hit, 1.0, named)
            weight = jnp.where(hit, weights[k : k + 1, :], weight)
        strict = (
            lax.broadcasted_iota(jnp.int32, (tokens, tokens), 0)
            < lax.broadcasted_iota(jnp.int32, (tokens, tokens), 1)
        ).astype(bf16)
        ranks = jnp.where(named > 0, dot(named.astype(bf16), strict), -1.0)
        packed_ref[tokens : tokens + extra, :] = jnp.full((extra, piece), -1.0, bf16)
        packed_ref[tokens : tokens + extra, 0:tokens] = ranks.astype(bf16)
        packed_ref[tokens : tokens + extra, pad : pad + tokens] = weight.astype(bf16)

    outs = (
        jax.ShapeDtypeStruct((tokens, width), bf16),
        jax.ShapeDtypeStruct((tokens + extra, piece), bf16),
    )
    operands = (rows, gain[None, :], index.T, scores.T)
    scratch = [pltpu.VMEM(v.shape, v.dtype) for v in operands]
    scratch.append(pltpu.SemaphoreType.DMA((4,)))
    return call(body, outs, operands, 1 << 22, scratch=scratch, far=4)


def group_of(sources, capacity):
    group = 1
    while group < sources and group * capacity % 16:
        group *= 2
    return group


def expert_up(places, own, far, capacity, gate_weight, up_weight):
    parts = len(far[0])
    tokens, width = own[0].shape
    packed_rows, piece = own[1].shape
    extra = packed_rows - tokens
    pad = -(-tokens // 128) * 128
    sources = 1 + len(far)
    slots = sources * capacity
    group = group_of(sources, capacity)
    hidden = gate_weight.shape[1]
    step = min(256, hidden)
    flat = list(own) + [p for pieces in far for p in pieces]

    def body(*refs):
        row_refs = refs[: len(flat)]
        gate_ref, up_ref, out_ref, info_ref, rows_ref, section_ref = refs[len(flat) :]
        here = Here(places)
        expert = lax.broadcasted_iota(jnp.int32, (extra, 2 * pad), 0) == here.e
        if pad > tokens:
            for s in range(sources):
                rows_ref[s * pad + tokens : (s + 1) * pad, :] = jnp.zeros((pad - tokens, width), bf16)
        rows_ref[0:tokens, :] = row_refs[0][...]
        for q in range(parts):

            @pl.when(here.part == q)
            def _():
                for s in range(1, sources):
                    for i in range(parts):
                        to = (q - i) % parts
                        rows_ref[s * pad : s * pad + tokens, to * piece : (to + 1) * piece] = (
                            row_refs[2 + (s - 1) * parts + i][0:tokens, :]
                        )

        for s0 in range(0, sources, group):
            targets = []
            for s in range(s0, s0 + group):
                table_ref = row_refs[2 + (s - 1) * parts if s else 1]
                table = table_ref[tokens : tokens + extra, 0 : 2 * pad].astype(f32)
                mine = jnp.sum(jnp.where(expert, table, 0.0), axis=0, keepdims=True)
                info_ref[s : s + 1, :] = mine
                rank = mine[:, 0:pad]
                targets.append(jnp.where(rank >= 0, rank + (s - s0) * capacity, -1.0))
            target = jnp.concatenate(targets, axis=1) if group > 1 else targets[0]
            slot = lax.broadcasted_iota(jnp.int32, (group * capacity, group * pad), 0)
            picks = (slot.astype(f32) == target).astype(bf16)
            section_ref[s0 * capacity : (s0 + group) * capacity, :] = dot(
                picks, rows_ref[s0 * pad : (s0 + group) * pad, :]
            ).astype(bf16)
        for h in range(0, hidden, step):
            section = section_ref[...]
            gate_value = dot(section, gate_ref[:, h : h + step])
            up_value = dot(section, up_ref[:, h : h + step])
            out_ref[:, h : h + step] = (silu(gate_value) * up_value).astype(bf16)

    outs = (
        jax.ShapeDtypeStruct((slots, hidden), bf16),
        jax.ShapeDtypeStruct((sources, 2 * pad), f32),
    )
    scratch = (pltpu.VMEM((sources * pad, width), bf16), pltpu.VMEM((slots, width), bf16))
    operands = (*flat, gate_weight, up_weight)
    return call(body, outs, operands, 4 * slots * width * hidden, scratch=scratch)


def take_piece(places, weight, du, dv, piece, hidden):
    size = hidden // PIECES

    def body(in_ref, out_ref, done):
        start = Here(places).column(du, dv) * hidden + piece * size
        copy = pltpu.make_async_copy(
            in_ref.at[pl.ds(pl.multiple_of(start, size), size), :], out_ref, done
        )
        copy.start()
        copy.wait()

    out = jax.ShapeDtypeStruct((size, weight.shape[1]), weight.dtype)
    return call(body, out, (weight,), 1 << 20, scratch=(pltpu.SemaphoreType.DMA,), far=1)


def dot_pieces(ref, pieces):
    size = pieces[0].shape[0]
    return sum(dot(ref[:, p * size : (p + 1) * size], piece[...]) for p, piece in enumerate(pieces))


def down_first(places, hiddens, weight, traded):
    hidden, columns = hiddens[0].shape[1], weight.shape[1]
    chunks, partners = len(hiddens), len(traded)
    traded = [piece for pieces in traded for piece in pieces]

    def body(*refs):
        outs = refs[chunks + 1 + len(traded) :]
        weight = rows_of(refs[chunks], Here(places).column(0, 0), hidden)
        for h in range(chunks):
            outs[h][...] = dot(refs[h][...], weight)
            for w in range(partners):
                first = chunks + 1 + w * PIECES
                outs[(w + 1) * chunks + h][...] = dot_pieces(
                    refs[h], refs[first : first + PIECES]
                )

    shapes = [
        jax.ShapeDtypeStruct((h.shape[0], columns), f32) for _ in range(1 + partners) for h in hiddens
    ]
    flops = 2 * sum(h.shape[0] for h in hiddens) * hidden * columns * (1 + partners)
    outs = call(body, shapes, (*hiddens, weight, *traded), flops)
    return [outs[w * chunks : (w + 1) * chunks] for w in range(1 + partners)]


def down_partner(first, hiddens, weights):
    count = len(hiddens)

    def body(first_ref, *refs):
        total = first_ref[...]
        for i in range(count):
            first = count + i * PIECES
            total = total + dot_pieces(refs[i], refs[first : first + PIECES])
        refs[-1][...] = total.astype(bf16)

    out = jax.ShapeDtypeStruct(first.shape, bf16)
    flops = 2 * first.size * hiddens[0].shape[1] * count
    pieces = [piece for slices in weights for piece in slices]
    return call(body, out, (first, *hiddens, *pieces), flops)


def down_own(places, firsts, gathered, weight):
    count, chunks = len(gathered), len(firsts)
    hidden, columns = gathered[0][0].shape[1], weight.shape[1]

    def body(*refs):
        hidden_refs = refs[chunks : chunks + count * chunks]
        weight_ref = refs[chunks + count * chunks]
        outs = refs[chunks + count * chunks + 1 :]
        here = Here(places)
        for h in range(chunks):
            total = refs[h][...]
            for i in range(count):
                rows = rows_of(weight_ref, here.column(-1 - i, 0), hidden)
                total = total + dot(hidden_refs[i * chunks + h][...], rows)
            outs[h][...] = total

    flat = [h for pieces in gathered for h in pieces]
    outs = [jax.ShapeDtypeStruct(f.shape, f32) for f in firsts]
    flops = 2 * sum(h.shape[0] for h in flat) * hidden * columns
    return call(body, outs, (*firsts, *flat, weight), flops)


def combine(own, back, info, tokens, capacity, out_type):
    slots, columns = own.shape
    sources = slots // capacity
    pad = info.shape[1] // 2
    group = group_of(sources, capacity)

    def body(own_ref, info_ref, *refs):
        out_ref = refs[-1]
        for s0 in range(0, sources, group):
            span = slice(s0 * capacity, (s0 + group) * capacity)
            value = own_ref[span, :]
            for ref in refs[:-1]:
                value = value + ref[span, :].astype(f32)
            value = value.astype(bf16)
            for s in range(s0, s0 + group):
                rank = info_ref[s : s + 1, 0:pad]
                target = jnp.where(rank >= 0, rank + (s - s0) * capacity, -1.0)
                slot = lax.broadcasted_iota(jnp.int32, (group * capacity, pad), 0).astype(f32)
                places = jnp.where(slot == target, info_ref[s : s + 1, pad : 2 * pad], 0.0)
                out_ref[s] = dot_tn(places.astype(bf16), value)[0:tokens].astype(out_type)

    out = jax.ShapeDtypeStruct((sources, tokens, columns), out_type)
    return call(body, out, (own, info, *back), 1 << 26)


def local(
    first_batch_queries,
    first_batch_keys,
    first_batch_values,
    output_gate_preactivation,
    decay_preactivation,
    channel_decay_bias,
    added_log_decay,
    head_norm_gain,
    attention_output_weight,
    second_batch_rows,
    expert_norm_gain,
    routed_expert_index,
    router_chosen_scores,
    expert_gate_weight,
    expert_up_weight,
    expert_down_weight,
    shared_gate_weight,
    shared_up_weight,
    shared_down_weight,
):
    at = Places()
    n, chips, experts = at.side, at.chips, at.ep
    heads = added_log_decay.shape[0]
    tokens, top_count = routed_expert_index.shape
    capacity = tokens * top_count * 3 // (2 * experts)
    gate_weight, up_weight, down_weight = (
        expert_gate_weight[0],
        expert_up_weight[0],
        expert_down_weight[0],
    )
    hidden = gate_weight.shape[1]

    traded = [[[] for _ in range(n)] for _ in range(1, n)]
    lacking = [(i, piece) for i in range(n) for piece in range(PIECES)]

    def trade(quarter):
        share = len(lacking) // 4
        for i, piece in lacking[quarter * share : (quarter + 1) * share]:
            for k in range(1, n):
                taken = take_piece(at, down_weight, -i, k, piece, hidden)
                traded[k - 1][i].append(at.along_v(taken, k))

    normed, packed = prepare_rows(
        at,
        n,
        second_batch_rows,
        expert_norm_gain,
        routed_expert_index,
        router_chosen_scores,
        experts,
    )
    middle = chips // 2
    far = {middle: at.along_z(packed, middle)}
    trade(0)
    far |= {k: at.along_z(packed, k) for k in range(1, chips) if k != middle}
    trade(1)
    trade(2)
    o_local, q_device, own_state = local_attention(
        first_batch_queries,
        first_batch_keys,
        first_batch_values,
        decay_preactivation,
        channel_decay_bias,
        added_log_decay,
    )
    arrived = [at.along_z(own_state, hop) for hop in range(1, chips)]
    states = [at.to_sibling(own_state)]
    for state in arrived:
        states += [state, at.to_sibling(state)]
    parts = [far[k] for k in range(1, chips)]
    far = [[a] + [at.along_u(a, i) for i in range(1, n)] for a in parts]
    other = ((at.to_sibling(normed), at.to_sibling(packed)), [[at.to_sibling(a)] for a in parts])
    for pieces, others in zip(far, other[1]):
        others += [at.to_sibling(p) for p in pieces[1:]]
    trade(3)
    ups = [expert_up(at, (normed, packed), far, capacity, gate_weight, up_weight)]
    gathered_first = [at.along_u(ups[0][0], i) for i in range(1, n)]
    _, other = hold((ups[0][0], other))
    ups.append(expert_up(at, *other, capacity, gate_weight, up_weight))
    hiddens = [up[0] for up in ups]
    gathered_second = [at.along_u(hiddens[1], i) for i in range(1, n)]
    both = finish_attention(
        at,
        o_local,
        q_device,
        states,
        output_gate_preactivation,
        head_norm_gain,
        heads,
        normed,
        shared_gate_weight,
        shared_up_weight,
    )
    firsts = down_first(at, hiddens, down_weight, [t[0] for t in traded])

    def partials(chunk, gathered):
        return [
            down_partner(firsts[k][chunk], gathered, traded[k - 1][1:]) for k in range(1, n)
        ]

    partial = partials(0, gathered_first)
    back = [[at.along_v(partial[k - 1], -k) for k in range(1, n)]]
    gathered_second, both, _ = hold((gathered_second, both, partial))
    partial = partials(1, gathered_second)
    back.append([at.along_v(partial[k - 1], -k) for k in range(1, n)])
    gathered = [list(pair) for pair in zip(gathered_first, gathered_second)]
    owns = down_own(at, firsts[0], gathered, down_weight)
    here = combine(owns[0], back[0], ups[0][1], tokens, capacity, f32)
    there = combine(owns[1], back[1], ups[1][1], tokens, capacity, bf16)
    from_sibling = at.to_sibling(there)
    chip_sum = here + from_sibling.astype(f32)
    routed_total = chip_sum[0]
    for k in range(1, chips):
        routed_total = routed_total + at.along_z(chip_sum[k].astype(bf16), -k).astype(f32)

    mixed = [
        both if dy == 0 and dx == 0 else at.along_tp(both, dy, dx)
        for dy in range(n)
        for dx in range(n)
    ]
    token_mixed, shared_total = project(
        at, mixed, attention_output_weight, shared_down_weight, tokens
    )
    channel_mixed = (routed_total + shared_total).astype(bf16)
    return (token_mixed, channel_mixed)


def solution(mesh):
    placed = (
        P("ep", "tp"),
        P("ep", "tp"),
        P("ep", "tp"),
        P("ep", "tp"),
        P("ep", "tp"),
        P("tp"),
        P("tp", "ep"),
        P("tp"),
        P(None, "tp"),
        P("ep", None),
        P(),
        P("ep", None),
        P("ep", None),
        P("ep", None, "tp"),
        P("ep", None, "tp"),
        P("ep", None, "tp"),
        P(None, "tp"),
        P(None, "tp"),
        P(None, "tp"),
    )

    return jax.shard_map(
        local, mesh=mesh, in_specs=placed, out_specs=(P("ep", "tp"), P("ep", "tp")), check_vma=False
    )
```

```python
import math

import jax
import jax.numpy as jnp
from jax import lax
from jax.experimental import pallas as pl
from jax.experimental.pallas import tpu as pltpu
from jax.sharding import PartitionSpec as P


BLOCK = 64
PIECES = 2
epsilon = 1e-06
temper = 16.0
routed_scale = 2.5
highest = lax.Precision.HIGHEST
f32 = jnp.float32
bf16 = jnp.bfloat16
AXES = ("ep", "tp")


class Places:
    def __init__(self):
        self.ep, self.tp = lax.axis_size("ep"), lax.axis_size("tp")
        self.side = math.isqrt(self.tp)
        self.chips = self.ep // 2
        assert self.side * self.side == self.tp and self.chips * 2 == self.ep

    def pairs(self, move):
        n = self.side
        out = []
        for e in range(self.ep):
            for j in range(self.tp):
                z, c, y, x = move(e // 2, e % 2, j // n, j % n)
                if 0 <= z < self.chips:
                    out.append((e * self.tp + j, (z * 2 + c) * self.tp + (y % n) * n + x % n))
        return out

    def send(self, value, move):
        return lax.ppermute(value, AXES, self.pairs(move))

    def along_z(self, value, k):
        return self.send(value, lambda z, c, y, x: ((z + k) % self.chips, c, y, x))

    def up_z(self, value, k):
        return self.send(value, lambda z, c, y, x: (z + k, c, y, x))

    def to_sibling(self, value):
        return self.send(value, lambda z, c, y, x: (z, 1 - c, y, x))

    def along_u(self, value, k):
        return self.send(value, lambda z, c, y, x: (z, c, y, x + k) if c == 0 else (z, c, y + k, x))

    def along_v(self, value, k):
        return self.send(value, lambda z, c, y, x: (z, c, y + k, x) if c == 0 else (z, c, y, x + k))

    def along_tp(self, value, dy, dx):
        return self.send(value, lambda z, c, y, x: (z, c, y + dy, x + dx))


def dot(a, b, precision=None):
    return jnp.dot(a, b, preferred_element_type=f32, precision=precision)


def dot_nt(a, b):
    return lax.dot_general(a, b, (((1,), (1,)), ((), ())), preferred_element_type=f32)


def dot_tn(a, b, precision=None):
    return lax.dot_general(
        a, b, (((0,), (0,)), ((), ())), preferred_element_type=f32, precision=precision
    )


def hold(values):
    return lax.optimization_barrier(values)


def silu(value):
    return value / (1.0 + jnp.exp(-value))


class Here:
    def __init__(self, places):
        n = self.side = places.side
        self.e = lax.axis_index("ep")
        j = lax.axis_index("tp")
        self.z, self.c = lax.div(self.e, 2), lax.rem(self.e, 2)
        self.y, self.x = lax.div(j, n), lax.rem(j, n)
        self.part = lax.rem(self.x + self.y, n)

    def along(self, dy, dx):
        n = self.side
        return lax.rem(self.y + dy % n, n) * n + lax.rem(self.x + dx % n, n)

    def column(self, du, dv):
        return jnp.where(self.c == 0, self.along(dv, du), self.along(du, dv))


def rows_of(ref, block, size):
    return ref[pl.ds(pl.multiple_of(block * size, size), size), :]


def call(body, outs, operands, flops, scratch=(), far=0):
    given = [pltpu.with_memory_space_constraint(v, pltpu.HBM) for v in operands[:far]]
    given += [pltpu.with_memory_space_constraint(v, pltpu.VMEM) for v in operands[far:]]
    return pl.pallas_call(
        body,
        out_shape=jax.tree.map(lambda o: pltpu.VMEM(o.shape, o.dtype), outs),
        in_specs=[pl.BlockSpec(memory_space=pltpu.HBM)] * far
        + [pl.BlockSpec(memory_space=pltpu.VMEM)] * (len(operands) - far),
        out_specs=jax.tree.map(lambda _: pl.BlockSpec(memory_space=pltpu.VMEM), outs),
        scratch_shapes=list(scratch),
        compiler_params=pltpu.CompilerParams(vmem_limit_bytes=12 << 20),
        cost_estimate=pl.CostEstimate(flops=flops, transcendentals=0, bytes_accessed=0),
    )(*given)


def local_attention(q, k, v, decay_pre, bias, added):
    heads, rows = added.shape
    dk, dv = q.shape[1] // heads, v.shape[1] // heads
    blocks = rows // BLOCK
    group = min(max(1, 128 // dk), heads)
    lanes = group * dk

    def body(q_ref, k_ref, v_ref, d_ref, bias_ref, added_ref, o_ref, qd_ref, pack_ref):
        spread = (
            lax.broadcasted_iota(jnp.int32, (heads, heads * dk), 1) // dk
            == lax.broadcasted_iota(jnp.int32, (heads, heads * dk), 0)
        ).astype(f32)
        logits = d_ref[...].astype(f32) + bias_ref[...]
        base = jnp.minimum(logits, 0.0) - jnp.log1p(jnp.exp(-jnp.abs(logits)))
        decay = base / temper + dot_tn(added_ref[...], spread, highest)
        row = lax.broadcasted_iota(jnp.int32, (BLOCK, BLOCK), 0)
        col = lax.broadcasted_iota(jnp.int32, (BLOCK, BLOCK), 1)
        lower = row >= col
        lower_f = lower.astype(f32)
        lane = lax.broadcasted_iota(jnp.int32, (1, lanes), 1)
        masks = [(lane // dk == g).astype(f32) for g in range(group)]
        states = [None] * heads
        lead = jnp.zeros((1, heads * dk), f32)
        for b in range(blocks):
            span = slice(b * BLOCK, (b + 1) * BLOCK)
            running = dot(lower_f, decay[span], highest)
            total = running[BLOCK - 1 : BLOCK, :]
            grow = jnp.exp(running)
            q_dec = q_ref[span, :].astype(f32) * grow
            keys = k_ref[span, :].astype(f32)
            k_up = (keys * jnp.exp(-running)).astype(bf16)
            k_end = (keys * jnp.exp(total - running)).astype(bf16)
            qd_ref[span, :] = (q_dec * jnp.exp(lead)).astype(bf16)
            shrink = jnp.exp(total)
            for h in range(heads):
                at = slice(h // group * lanes, h // group * lanes + lanes)
                q_h = (q_dec[:, at] * masks[h % group]).astype(bf16)
                v_h = v_ref[span, h * dv : (h + 1) * dv]
                scores = jnp.where(lower, dot_nt(q_h, k_up[:, at]), 0.0).astype(bf16)
                value = dot(scores, v_h)
                if b:
                    value = value + dot_nt(q_h, states[h].astype(bf16))
                o_ref[span, h * dv : (h + 1) * dv] = value
                update = dot_tn(v_h, k_end[:, at])
                states[h] = update if b == 0 else states[h] * shrink[:, at] + update
            lead = lead + total
        for h0 in range(0, heads, group):
            packed = states[h0]
            for g in range(1, group):
                packed = jnp.where(lane // dk == g, states[h0 + g], packed)
            pack_ref[0:dv, h0 * dk : h0 * dk + lanes] = packed.astype(bf16)
        pack_ref[dv : dv + 8, :] = jnp.broadcast_to(jnp.exp(lead), (8, heads * dk)).astype(bf16)

    outs = (
        jax.ShapeDtypeStruct((rows, heads * dv), f32),
        jax.ShapeDtypeStruct((rows, heads * dk), bf16),
        jax.ShapeDtypeStruct((dv + 8, heads * dk), bf16),
    )
    return call(body, outs, (q, k, v, decay_pre, bias[None, :], added), 1 << 25)


def finish_attention(
    places, local, qd, states, gate_pre, gain, heads, normed, shared_gate, shared_up
):
    rows = local.shape[0]
    dv, dk = local.shape[1] // heads, qd.shape[1] // heads
    group = min(max(1, 128 // dk), heads)
    lanes = group * dk
    tokens, hidden = normed.shape[0], shared_gate.shape[1]
    sharing = local.shape[1] // hidden
    part = tokens // sharing

    def body(local_ref, qd_ref, gate_ref, gain_ref, normed_ref, sg_ref, su_ref, *refs):
        out_ref = refs[-1]
        here = Here(places)
        first = here.c == 0
        between = jnp.ones((1, heads * dk), f32)
        incoming = jnp.zeros((dv, heads * dk), f32)
        sib = refs[0][...].astype(f32)
        for hop in range(1, (len(refs) - 2) // 2 + 1):
            mine, other = refs[2 * hop - 1][...].astype(f32), refs[2 * hop][...].astype(f32)
            inside = here.z >= hop
            early, late = jnp.where(first, mine, other), jnp.where(first, other, mine)
            decay = late[dv : dv + 1]
            got = early[0:dv] * decay + late[0:dv]
            incoming = incoming + jnp.where(inside, between * got, 0.0)
            between = jnp.where(inside, between * (early[dv : dv + 1] * decay), between)
        incoming = jnp.where(first, incoming, incoming * sib[dv : dv + 1] + sib[0:dv]).astype(bf16)
        lane = lax.broadcasted_iota(jnp.int32, (1, lanes), 1)
        for h in range(heads):
            at = slice(h // group * lanes, h // group * lanes + lanes)
            vs = slice(h * dv, (h + 1) * dv)
            mask = lane // dk == h % group
            q_h = jnp.where(mask, qd_ref[:, at], jnp.zeros((), bf16))
            value = local_ref[:, vs] + dot_nt(q_h, incoming[:, at])
            mean_square = jnp.mean(value * value, axis=1, keepdims=True)
            value = value * lax.rsqrt(mean_square + epsilon) * gain_ref[:, vs]
            out_ref[0:rows, vs] = (value * silu(gate_ref[:, vs].astype(f32))).astype(bf16)
        features = normed_ref[...]
        shared = (silu(dot(features, sg_ref[...])) * dot(features, su_ref[...])).astype(bf16)
        for i in range(sharing):
            out_ref[rows : rows + part, i * hidden : (i + 1) * hidden] = shared[
                i * part : (i + 1) * part
            ]

    out = jax.ShapeDtypeStruct((rows + part, local.shape[1]), bf16)
    operands = (local, qd, gate_pre, gain[None, :], normed, shared_gate, shared_up)
    return call(body, out, operands + tuple(states), 1 << 27)


def project(places, gathered, attention_weight, shared_weight, tokens):
    count = len(gathered)
    folded, width = gathered[0].shape
    hidden, columns = shared_weight.shape[0] // count, shared_weight.shape[1]
    sharing = width // hidden
    part = tokens // sharing
    rows = folded - part

    def body(*refs):
        weight_ref, shared_ref, mixed_ref, out_ref = refs[count:]
        mixed = shared = 0.0
        here = Here(places)
        for i in range(count):
            ref = refs[i]
            block = here.along(-(i // here.side), -(i % here.side))
            mixed = mixed + dot(ref[0:rows, :], rows_of(weight_ref, block, width))
            units = jnp.concatenate(
                [ref[rows:, q * hidden : (q + 1) * hidden] for q in range(sharing)], axis=0
            )
            shared = shared + dot(units, rows_of(shared_ref, block, hidden))
        mixed_ref[...] = mixed.astype(bf16)
        out_ref[...] = shared

    outs = (
        jax.ShapeDtypeStruct((rows, columns), bf16),
        jax.ShapeDtypeStruct((tokens, columns), f32),
    )
    operands = (*gathered, attention_weight, shared_weight)
    return call(body, outs, operands, 2 * folded * width * columns * count)


def prepare_rows(places, parts, rows, gain, index, scores, experts):
    tokens, width = rows.shape
    top = index.shape[1]
    piece = width // parts
    pad = -(-tokens // 128) * 128
    extra = -(-experts // 8) * 8

    def body(rows_hbm, gain_hbm, index_hbm, score_hbm, normed_ref, packed_ref, *scratch):
        rows_ref, gain_ref, index_ref, score_ref, done = scratch
        copies = [
            pltpu.make_async_copy(source, target, done.at[i])
            for i, (source, target) in enumerate(
                zip((rows_hbm, gain_hbm, index_hbm, score_hbm), scratch[:4])
            )
        ]
        for copy in copies:
            copy.start()
        for copy in copies:
            copy.wait()
        here = Here(places)
        value = rows_ref[...].astype(f32)
        mean_square = jnp.mean(value * value, axis=1, keepdims=True)
        normed = (value * lax.rsqrt(mean_square + epsilon) * gain_ref[...]).astype(bf16)
        normed_ref[...] = normed
        for q in range(parts):

            @pl.when(here.part == q)
            def _():
                packed_ref[0:tokens, :] = normed[:, q * piece : (q + 1) * piece]

        scores = score_ref[...]
        weights = routed_scale * scores / jnp.sum(scores, axis=0, keepdims=True)
        expert = lax.broadcasted_iota(jnp.int32, (extra, tokens), 0)
        named = jnp.zeros((extra, tokens), f32)
        weight = jnp.zeros((extra, tokens), f32)
        for k in range(top):
            hit = index_ref[k : k + 1, :] == expert
            named = jnp.where(hit, 1.0, named)
            weight = jnp.where(hit, weights[k : k + 1, :], weight)
        strict = (
            lax.broadcasted_iota(jnp.int32, (tokens, tokens), 0)
            < lax.broadcasted_iota(jnp.int32, (tokens, tokens), 1)
        ).astype(bf16)
        ranks = jnp.where(named > 0, dot(named.astype(bf16), strict), -1.0)
        packed_ref[tokens : tokens + extra, :] = jnp.full((extra, piece), -1.0, bf16)
        packed_ref[tokens : tokens + extra, 0:tokens] = ranks.astype(bf16)
        packed_ref[tokens : tokens + extra, pad : pad + tokens] = weight.astype(bf16)

    outs = (
        jax.ShapeDtypeStruct((tokens, width), bf16),
        jax.ShapeDtypeStruct((tokens + extra, piece), bf16),
    )
    operands = (rows, gain[None, :], index.T, scores.T)
    scratch = [pltpu.VMEM(v.shape, v.dtype) for v in operands]
    scratch.append(pltpu.SemaphoreType.DMA((4,)))
    return call(body, outs, operands, 1 << 22, scratch=scratch, far=4)


def group_of(sources, capacity):
    group = 1
    while group < sources and group * capacity % 16:
        group *= 2
    return group


def expert_up(places, own, far, capacity, gate_weight, up_weight):
    parts = len(far[0])
    tokens, width = own[0].shape
    packed_rows, piece = own[1].shape
    extra = packed_rows - tokens
    pad = -(-tokens // 128) * 128
    sources = 1 + len(far)
    slots = sources * capacity
    group = group_of(sources, capacity)
    hidden = gate_weight.shape[1]
    step = min(256, hidden)
    flat = list(own) + [p for pieces in far for p in pieces]

    def body(*refs):
        row_refs = refs[: len(flat)]
        gate_ref, up_ref, out_ref, info_ref, rows_ref, section_ref = refs[len(flat) :]
        here = Here(places)
        expert = lax.broadcasted_iota(jnp.int32, (extra, 2 * pad), 0) == here.e
        if pad > tokens:
            for s in range(sources):
                rows_ref[s * pad + tokens : (s + 1) * pad, :] = jnp.zeros((pad - tokens, width), bf16)
        rows_ref[0:tokens, :] = row_refs[0][...]
        for q in range(parts):

            @pl.when(here.part == q)
            def _():
                for s in range(1, sources):
                    for i in range(parts):
                        to = (q - i) % parts
                        rows_ref[s * pad : s * pad + tokens, to * piece : (to + 1) * piece] = (
                            row_refs[2 + (s - 1) * parts + i][0:tokens, :]
                        )

        for s0 in range(0, sources, group):
            targets = []
            for s in range(s0, s0 + group):
                table_ref = row_refs[2 + (s - 1) * parts if s else 1]
                table = table_ref[tokens : tokens + extra, 0 : 2 * pad].astype(f32)
                mine = jnp.sum(jnp.where(expert, table, 0.0), axis=0, keepdims=True)
                info_ref[s : s + 1, :] = mine
                rank = mine[:, 0:pad]
                targets.append(jnp.where(rank >= 0, rank + (s - s0) * capacity, -1.0))
            target = jnp.concatenate(targets, axis=1) if group > 1 else targets[0]
            slot = lax.broadcasted_iota(jnp.int32, (group * capacity, group * pad), 0)
            picks = (slot.astype(f32) == target).astype(bf16)
            section_ref[s0 * capacity : (s0 + group) * capacity, :] = dot(
                picks, rows_ref[s0 * pad : (s0 + group) * pad, :]
            ).astype(bf16)
        for h in range(0, hidden, step):
            section = section_ref[...]
            gate_value = dot(section, gate_ref[:, h : h + step])
            up_value = dot(section, up_ref[:, h : h + step])
            out_ref[:, h : h + step] = (silu(gate_value) * up_value).astype(bf16)

    outs = (
        jax.ShapeDtypeStruct((slots, hidden), bf16),
        jax.ShapeDtypeStruct((sources, 2 * pad), f32),
    )
    scratch = (pltpu.VMEM((sources * pad, width), bf16), pltpu.VMEM((slots, width), bf16))
    operands = (*flat, gate_weight, up_weight)
    return call(body, outs, operands, 4 * slots * width * hidden, scratch=scratch)


def take_pieces(places, weight, wanted, hidden):
    size = hidden // PIECES

    def body(in_ref, *refs):
        outs, done = refs[:-1], refs[-1]
        here = Here(places)
        copies = []
        for i, (du, dv, piece) in enumerate(wanted):
            start = pl.multiple_of(here.column(du, dv) * hidden + piece * size, size)
            copies.append(
                pltpu.make_async_copy(in_ref.at[pl.ds(start, size), :], outs[i], done.at[i])
            )
        for copy in copies:
            copy.start()
        for copy in copies:
            copy.wait()

    outs = [jax.ShapeDtypeStruct((size, weight.shape[1]), weight.dtype) for _ in wanted]
    scratch = (pltpu.SemaphoreType.DMA((len(wanted),)),)
    return call(body, outs, (weight,), 1 << 20, scratch=scratch, far=1)


def dot_pieces(ref, pieces):
    size = pieces[0].shape[0]
    return sum(dot(ref[:, p * size : (p + 1) * size], piece[...]) for p, piece in enumerate(pieces))


def down_first(places, hiddens, weight, traded):
    hidden, columns = hiddens[0].shape[1], weight.shape[1]
    chunks, partners = len(hiddens), len(traded)
    traded = [piece for pieces in traded for piece in pieces]

    def body(*refs):
        outs = refs[chunks + 1 + len(traded) :]
        weight = rows_of(refs[chunks], Here(places).column(0, 0), hidden)
        for h in range(chunks):
            outs[h][...] = dot(refs[h][...], weight)
            for w in range(partners):
                first = chunks + 1 + w * PIECES
                outs[(w + 1) * chunks + h][...] = dot_pieces(
                    refs[h], refs[first : first + PIECES]
                )

    shapes = [
        jax.ShapeDtypeStruct((h.shape[0], columns), f32) for _ in range(1 + partners) for h in hiddens
    ]
    flops = 2 * sum(h.shape[0] for h in hiddens) * hidden * columns * (1 + partners)
    outs = call(body, shapes, (*hiddens, weight, *traded), flops)
    return [outs[w * chunks : (w + 1) * chunks] for w in range(1 + partners)]


def down_partner(first, hiddens, weights):
    count = len(hiddens)

    def body(first_ref, *refs):
        total = first_ref[...]
        for i in range(count):
            first = count + i * PIECES
            total = total + dot_pieces(refs[i], refs[first : first + PIECES])
        refs[-1][...] = total.astype(bf16)

    out = jax.ShapeDtypeStruct(first.shape, bf16)
    flops = 2 * first.size * hiddens[0].shape[1] * count
    pieces = [piece for slices in weights for piece in slices]
    return call(body, out, (first, *hiddens, *pieces), flops)


def down_own(places, firsts, gathered, weight):
    count, chunks = len(gathered), len(firsts)
    hidden, columns = gathered[0][0].shape[1], weight.shape[1]

    def body(*refs):
        hidden_refs = refs[chunks : chunks + count * chunks]
        weight_ref = refs[chunks + count * chunks]
        outs = refs[chunks + count * chunks + 1 :]
        here = Here(places)
        for h in range(chunks):
            total = refs[h][...]
            for i in range(count):
                rows = rows_of(weight_ref, here.column(-1 - i, 0), hidden)
                total = total + dot(hidden_refs[i * chunks + h][...], rows)
            outs[h][...] = total

    flat = [h for pieces in gathered for h in pieces]
    outs = [jax.ShapeDtypeStruct(f.shape, f32) for f in firsts]
    flops = 2 * sum(h.shape[0] for h in flat) * hidden * columns
    return call(body, outs, (*firsts, *flat, weight), flops)


def combine(own, back, info, tokens, capacity, out_type):
    slots, columns = own.shape
    sources = slots // capacity
    pad = info.shape[1] // 2
    group = group_of(sources, capacity)

    def body(own_ref, info_ref, *refs):
        out_ref = refs[-1]
        for s0 in range(0, sources, group):
            span = slice(s0 * capacity, (s0 + group) * capacity)
            value = own_ref[span, :]
            for ref in refs[:-1]:
                value = value + ref[span, :].astype(f32)
            value = value.astype(bf16)
            for s in range(s0, s0 + group):
                rank = info_ref[s : s + 1, 0:pad]
                target = jnp.where(rank >= 0, rank + (s - s0) * capacity, -1.0)
                slot = lax.broadcasted_iota(jnp.int32, (group * capacity, pad), 0).astype(f32)
                places = jnp.where(slot == target, info_ref[s : s + 1, pad : 2 * pad], 0.0)
                out_ref[s] = dot_tn(places.astype(bf16), value)[0:tokens].astype(out_type)

    out = jax.ShapeDtypeStruct((sources, tokens, columns), out_type)
    return call(body, out, (own, info, *back), 1 << 26)


def local(
    first_batch_queries,
    first_batch_keys,
    first_batch_values,
    output_gate_preactivation,
    decay_preactivation,
    channel_decay_bias,
    added_log_decay,
    head_norm_gain,
    attention_output_weight,
    second_batch_rows,
    expert_norm_gain,
    routed_expert_index,
    router_chosen_scores,
    expert_gate_weight,
    expert_up_weight,
    expert_down_weight,
    shared_gate_weight,
    shared_up_weight,
    shared_down_weight,
):
    at = Places()
    n, chips, experts = at.side, at.chips, at.ep
    heads = added_log_decay.shape[0]
    tokens, top_count = routed_expert_index.shape
    capacity = tokens * top_count * 3 // (2 * experts)
    gate_weight, up_weight, down_weight = (
        expert_gate_weight[0],
        expert_up_weight[0],
        expert_down_weight[0],
    )
    hidden = gate_weight.shape[1]

    traded = [[[] for _ in range(n)] for _ in range(1, n)]
    lacking = [(i, piece) for i in range(n) for piece in range(PIECES)]
    wanted = [(i, k, piece) for i, piece in lacking for k in range(1, n)]
    taken = take_pieces(at, down_weight, [(-i, k, p) for i, k, p in wanted], hidden)
    quarter = len(wanted) // 4

    def trade(number):
        for at_piece in range(number * quarter, (number + 1) * quarter):
            i, k, _ = wanted[at_piece]
            traded[k - 1][i].append(at.along_v(taken[at_piece], k))

    normed, packed = prepare_rows(
        at,
        n,
        second_batch_rows,
        expert_norm_gain,
        routed_expert_index,
        router_chosen_scores,
        experts,
    )
    middle = chips // 2
    far = {middle: at.along_z(packed, middle)}
    trade(0)
    trade(1)
    far |= {k: at.along_z(packed, k) for k in range(1, chips) if k != middle}
    trade(2)
    o_local, q_device, own_state = local_attention(
        first_batch_queries,
        first_batch_keys,
        first_batch_values,
        decay_preactivation,
        channel_decay_bias,
        added_log_decay,
    )
    arrived = [at.along_z(own_state, hop) for hop in range(1, chips)]
    states = [at.to_sibling(own_state)]
    for state in arrived:
        states += [state, at.to_sibling(state)]
    parts = [far[k] for k in range(1, chips)]
    far = [[a] + [at.along_u(a, i) for i in range(1, n)] for a in parts]
    other = ((at.to_sibling(normed), at.to_sibling(packed)), [[at.to_sibling(a)] for a in parts])
    for pieces, others in zip(far, other[1]):
        others += [at.to_sibling(p) for p in pieces[1:]]
    trade(3)
    ups = [expert_up(at, (normed, packed), far, capacity, gate_weight, up_weight)]
    gathered_first = [at.along_u(ups[0][0], i) for i in range(1, n)]
    _, other = hold((ups[0][0], other))
    ups.append(expert_up(at, *other, capacity, gate_weight, up_weight))
    hiddens = [up[0] for up in ups]
    gathered_second = [at.along_u(hiddens[1], i) for i in range(1, n)]
    both = finish_attention(
        at,
        o_local,
        q_device,
        states,
        output_gate_preactivation,
        head_norm_gain,
        heads,
        normed,
        shared_gate_weight,
        shared_up_weight,
    )
    firsts = down_first(at, hiddens, down_weight, [t[0] for t in traded])

    def partials(chunk, gathered):
        return [
            down_partner(firsts[k][chunk], gathered, traded[k - 1][1:]) for k in range(1, n)
        ]

    partial = partials(0, gathered_first)
    back = [[at.along_v(partial[k - 1], -k) for k in range(1, n)]]
    gathered_second, _ = hold((gathered_second, partial))
    partial = partials(1, gathered_second)
    back.append([at.along_v(partial[k - 1], -k) for k in range(1, n)])
    gathered = [list(pair) for pair in zip(gathered_first, gathered_second)]
    owns = down_own(at, firsts[0], gathered, down_weight)
    here = combine(owns[0], back[0], ups[0][1], tokens, capacity, f32)
    there = combine(owns[1], back[1], ups[1][1], tokens, capacity, bf16)
    from_sibling = at.to_sibling(there)
    chip_sum = here + from_sibling.astype(f32)
    routed_total = chip_sum[0]
    for k in range(1, chips):
        routed_total = routed_total + at.along_z(chip_sum[k].astype(bf16), -k).astype(f32)

    mixed = [
        both if dy == 0 and dx == 0 else at.along_tp(both, dy, dx)
        for dy in range(n)
        for dx in range(n)
    ]
    token_mixed, shared_total = project(
        at, mixed, attention_output_weight, shared_down_weight, tokens
    )
    channel_mixed = (routed_total + shared_total).astype(bf16)
    return (token_mixed, channel_mixed)


def solution(mesh):
    placed = (
        P("ep", "tp"),
        P("ep", "tp"),
        P("ep", "tp"),
        P("ep", "tp"),
        P("ep", "tp"),
        P("tp"),
        P("tp", "ep"),
        P("tp"),
        P(None, "tp"),
        P("ep", None),
        P(),
        P("ep", None),
        P("ep", None),
        P("ep", None, "tp"),
        P("ep", None, "tp"),
        P("ep", None, "tp"),
        P(None, "tp"),
        P(None, "tp"),
        P(None, "tp"),
    )

    return jax.shard_map(
        local, mesh=mesh, in_specs=placed, out_specs=(P("ep", "tp"), P("ep", "tp")), check_vma=False
    )
```

```python
import math

import jax
import jax.numpy as jnp
from jax import lax
from jax.experimental import pallas as pl
from jax.experimental.pallas import tpu as pltpu
from jax.sharding import PartitionSpec as P


BLOCK = 64
PIECES = 2
epsilon = 1e-06
temper = 16.0
routed_scale = 2.5
highest = lax.Precision.HIGHEST
f32 = jnp.float32
bf16 = jnp.bfloat16
AXES = ("ep", "tp")


class Places:
    def __init__(self):
        self.ep, self.tp = lax.axis_size("ep"), lax.axis_size("tp")
        self.side = math.isqrt(self.tp)
        self.chips = self.ep // 2
        assert self.side * self.side == self.tp and self.chips * 2 == self.ep

    def pairs(self, move):
        n = self.side
        out = []
        for e in range(self.ep):
            for j in range(self.tp):
                z, c, y, x = move(e // 2, e % 2, j // n, j % n)
                if 0 <= z < self.chips:
                    out.append((e * self.tp + j, (z * 2 + c) * self.tp + (y % n) * n + x % n))
        return out

    def send(self, value, move):
        return lax.ppermute(value, AXES, self.pairs(move))

    def along_z(self, value, k):
        return self.send(value, lambda z, c, y, x: ((z + k) % self.chips, c, y, x))

    def up_z(self, value, k):
        return self.send(value, lambda z, c, y, x: (z + k, c, y, x))

    def to_sibling(self, value):
        return self.send(value, lambda z, c, y, x: (z, 1 - c, y, x))

    def along_u(self, value, k):
        return self.send(value, lambda z, c, y, x: (z, c, y, x + k) if c == 0 else (z, c, y + k, x))

    def along_v(self, value, k):
        return self.send(value, lambda z, c, y, x: (z, c, y + k, x) if c == 0 else (z, c, y, x + k))

    def along_tp(self, value, dy, dx):
        return self.send(value, lambda z, c, y, x: (z, c, y + dy, x + dx))


def dot(a, b, precision=None):
    return jnp.dot(a, b, preferred_element_type=f32, precision=precision)


def dot_nt(a, b):
    return lax.dot_general(a, b, (((1,), (1,)), ((), ())), preferred_element_type=f32)


def dot_tn(a, b, precision=None):
    return lax.dot_general(
        a, b, (((0,), (0,)), ((), ())), preferred_element_type=f32, precision=precision
    )


def hold(values):
    return lax.optimization_barrier(values)


def silu(value):
    return value / (1.0 + jnp.exp(-value))


class Here:
    def __init__(self, places):
        n = self.side = places.side
        self.e = lax.axis_index("ep")
        j = lax.axis_index("tp")
        self.z, self.c = lax.div(self.e, 2), lax.rem(self.e, 2)
        self.y, self.x = lax.div(j, n), lax.rem(j, n)
        self.part = lax.rem(self.x + self.y, n)

    def along(self, dy, dx):
        n = self.side
        return lax.rem(self.y + dy % n, n) * n + lax.rem(self.x + dx % n, n)

    def column(self, du, dv):
        return jnp.where(self.c == 0, self.along(dv, du), self.along(du, dv))


def rows_of(ref, block, size):
    return ref[pl.ds(pl.multiple_of(block * size, size), size), :]


def call(body, outs, operands, flops, scratch=(), far=0):
    given = [pltpu.with_memory_space_constraint(v, pltpu.HBM) for v in operands[:far]]
    given += [pltpu.with_memory_space_constraint(v, pltpu.VMEM) for v in operands[far:]]
    return pl.pallas_call(
        body,
        out_shape=jax.tree.map(lambda o: pltpu.VMEM(o.shape, o.dtype), outs),
        in_specs=[pl.BlockSpec(memory_space=pltpu.HBM)] * far
        + [pl.BlockSpec(memory_space=pltpu.VMEM)] * (len(operands) - far),
        out_specs=jax.tree.map(lambda _: pl.BlockSpec(memory_space=pltpu.VMEM), outs),
        scratch_shapes=list(scratch),
        compiler_params=pltpu.CompilerParams(vmem_limit_bytes=12 << 20),
        cost_estimate=pl.CostEstimate(flops=flops, transcendentals=0, bytes_accessed=0),
    )(*given)


def local_attention(q, k, v, decay_pre, bias, added):
    heads, rows = added.shape
    dk, dv = q.shape[1] // heads, v.shape[1] // heads
    blocks = rows // BLOCK
    group = min(max(1, 128 // dk), heads)
    lanes = group * dk

    def body(q_ref, k_ref, v_ref, d_ref, bias_ref, added_ref, o_ref, qd_ref, pack_ref):
        spread = (
            lax.broadcasted_iota(jnp.int32, (heads, heads * dk), 1) // dk
            == lax.broadcasted_iota(jnp.int32, (heads, heads * dk), 0)
        ).astype(f32)
        logits = d_ref[...].astype(f32) + bias_ref[...]
        base = jnp.minimum(logits, 0.0) - jnp.log1p(jnp.exp(-jnp.abs(logits)))
        decay = base / temper + dot_tn(added_ref[...], spread, highest)
        row = lax.broadcasted_iota(jnp.int32, (BLOCK, BLOCK), 0)
        col = lax.broadcasted_iota(jnp.int32, (BLOCK, BLOCK), 1)
        lower = row >= col
        lower_f = lower.astype(f32)
        lane = lax.broadcasted_iota(jnp.int32, (1, lanes), 1)
        masks = [(lane // dk == g).astype(f32) for g in range(group)]
        states = [None] * heads
        lead = jnp.zeros((1, heads * dk), f32)
        for b in range(blocks):
            span = slice(b * BLOCK, (b + 1) * BLOCK)
            running = dot(lower_f, decay[span], highest)
            total = running[BLOCK - 1 : BLOCK, :]
            grow = jnp.exp(running)
            q_dec = q_ref[span, :].astype(f32) * grow
            keys = k_ref[span, :].astype(f32)
            k_up = (keys * jnp.exp(-running)).astype(bf16)
            k_end = (keys * jnp.exp(total - running)).astype(bf16)
            qd_ref[span, :] = (q_dec * jnp.exp(lead)).astype(bf16)
            shrink = jnp.exp(total)
            for h in range(heads):
                at = slice(h // group * lanes, h // group * lanes + lanes)
                q_h = (q_dec[:, at] * masks[h % group]).astype(bf16)
                v_h = v_ref[span, h * dv : (h + 1) * dv]
                scores = jnp.where(lower, dot_nt(q_h, k_up[:, at]), 0.0).astype(bf16)
                value = dot(scores, v_h)
                if b:
                    value = value + dot_nt(q_h, states[h].astype(bf16))
                o_ref[span, h * dv : (h + 1) * dv] = value
                update = dot_tn(v_h, k_end[:, at])
                states[h] = update if b == 0 else states[h] * shrink[:, at] + update
            lead = lead + total
        for h0 in range(0, heads, group):
            packed = states[h0]
            for g in range(1, group):
                packed = jnp.where(lane // dk == g, states[h0 + g], packed)
            pack_ref[0:dv, h0 * dk : h0 * dk + lanes] = packed.astype(bf16)
        pack_ref[dv : dv + 8, :] = jnp.broadcast_to(jnp.exp(lead), (8, heads * dk)).astype(bf16)

    outs = (
        jax.ShapeDtypeStruct((rows, heads * dv), f32),
        jax.ShapeDtypeStruct((rows, heads * dk), bf16),
        jax.ShapeDtypeStruct((dv + 8, heads * dk), bf16),
    )
    return call(body, outs, (q, k, v, decay_pre, bias[None, :], added), 1 << 25)


def finish_attention(
    places, local, qd, states, gate_pre, gain, heads, normed, shared_gate, shared_up
):
    rows = local.shape[0]
    dv, dk = local.shape[1] // heads, qd.shape[1] // heads
    group = min(max(1, 128 // dk), heads)
    lanes = group * dk
    tokens, hidden = normed.shape[0], shared_gate.shape[1]
    sharing = local.shape[1] // hidden
    part = tokens // sharing

    def body(local_ref, qd_ref, gate_ref, gain_ref, normed_ref, sg_ref, su_ref, *refs):
        out_ref = refs[-1]
        here = Here(places)
        first = here.c == 0
        between = jnp.ones((1, heads * dk), f32)
        incoming = jnp.zeros((dv, heads * dk), f32)
        sib = refs[0][...].astype(f32)
        for hop in range(1, (len(refs) - 2) // 2 + 1):
            mine, other = refs[2 * hop - 1][...].astype(f32), refs[2 * hop][...].astype(f32)
            inside = here.z >= hop
            early, late = jnp.where(first, mine, other), jnp.where(first, other, mine)
            decay = late[dv : dv + 1]
            got = early[0:dv] * decay + late[0:dv]
            incoming = incoming + jnp.where(inside, between * got, 0.0)
            between = jnp.where(inside, between * (early[dv : dv + 1] * decay), between)
        incoming = jnp.where(first, incoming, incoming * sib[dv : dv + 1] + sib[0:dv]).astype(bf16)
        lane = lax.broadcasted_iota(jnp.int32, (1, lanes), 1)
        for h in range(heads):
            at = slice(h // group * lanes, h // group * lanes + lanes)
            vs = slice(h * dv, (h + 1) * dv)
            mask = lane // dk == h % group
            q_h = jnp.where(mask, qd_ref[:, at], jnp.zeros((), bf16))
            value = local_ref[:, vs] + dot_nt(q_h, incoming[:, at])
            mean_square = jnp.mean(value * value, axis=1, keepdims=True)
            value = value * lax.rsqrt(mean_square + epsilon) * gain_ref[:, vs]
            out_ref[0:rows, vs] = (value * silu(gate_ref[:, vs].astype(f32))).astype(bf16)
        features = normed_ref[...]
        shared = (silu(dot(features, sg_ref[...])) * dot(features, su_ref[...])).astype(bf16)
        for i in range(sharing):
            out_ref[rows : rows + part, i * hidden : (i + 1) * hidden] = shared[
                i * part : (i + 1) * part
            ]

    out = jax.ShapeDtypeStruct((rows + part, local.shape[1]), bf16)
    operands = (local, qd, gate_pre, gain[None, :], normed, shared_gate, shared_up)
    return call(body, out, operands + tuple(states), 1 << 27)


def project(places, gathered, attention_weight, shared_weight, tokens):
    count = len(gathered)
    folded, width = gathered[0].shape
    hidden, columns = shared_weight.shape[0] // count, shared_weight.shape[1]
    sharing = width // hidden
    part = tokens // sharing
    rows = folded - part

    def body(*refs):
        weight_ref, shared_ref, mixed_ref, out_ref = refs[count:]
        mixed = shared = 0.0
        here = Here(places)
        for i in range(count):
            ref = refs[i]
            block = here.along(-(i // here.side), -(i % here.side))
            mixed = mixed + dot(ref[0:rows, :], rows_of(weight_ref, block, width))
            units = jnp.concatenate(
                [ref[rows:, q * hidden : (q + 1) * hidden] for q in range(sharing)], axis=0
            )
            shared = shared + dot(units, rows_of(shared_ref, block, hidden))
        mixed_ref[...] = mixed.astype(bf16)
        out_ref[...] = shared

    outs = (
        jax.ShapeDtypeStruct((rows, columns), bf16),
        jax.ShapeDtypeStruct((tokens, columns), f32),
    )
    operands = (*gathered, attention_weight, shared_weight)
    return call(body, outs, operands, 2 * folded * width * columns * count)


def prepare_rows(places, parts, rows, gain, index, scores, experts, weight, wanted, hidden):
    size = hidden // PIECES
    tokens, width = rows.shape
    top = index.shape[1]
    part = width // parts
    pad = -(-tokens // 128) * 128
    extra = -(-experts // 8) * 8

    def body(rows_hbm, gain_hbm, index_hbm, score_hbm, weight_hbm, normed_ref, packed_ref, *refs):
        pieces, scratch = refs[: len(wanted)], refs[len(wanted) :]
        rows_ref, gain_ref, index_ref, score_ref, done, taken = scratch
        here = Here(places)
        copies = [
            pltpu.make_async_copy(source, target, done.at[i])
            for i, (source, target) in enumerate(
                zip((rows_hbm, gain_hbm, index_hbm, score_hbm), scratch[:4])
            )
        ]
        takes = []
        for i, (du, dv, piece) in enumerate(wanted):
            start = pl.multiple_of(here.column(du, dv) * hidden + piece * size, size)
            takes.append(
                pltpu.make_async_copy(
                    weight_hbm.at[pl.ds(start, size), :], pieces[i], taken.at[i]
                )
            )
        for copy in copies + takes:
            copy.start()
        for copy in copies:
            copy.wait()
        value = rows_ref[...].astype(f32)
        mean_square = jnp.mean(value * value, axis=1, keepdims=True)
        normed = (value * lax.rsqrt(mean_square + epsilon) * gain_ref[...]).astype(bf16)
        normed_ref[...] = normed
        for q in range(parts):

            @pl.when(here.part == q)
            def _():
                packed_ref[0:tokens, :] = normed[:, q * part : (q + 1) * part]

        scores = score_ref[...]
        weights = routed_scale * scores / jnp.sum(scores, axis=0, keepdims=True)
        expert = lax.broadcasted_iota(jnp.int32, (extra, tokens), 0)
        named = jnp.zeros((extra, tokens), f32)
        share = jnp.zeros((extra, tokens), f32)
        for k in range(top):
            hit = index_ref[k : k + 1, :] == expert
            named = jnp.where(hit, 1.0, named)
            share = jnp.where(hit, weights[k : k + 1, :], share)
        strict = (
            lax.broadcasted_iota(jnp.int32, (tokens, tokens), 0)
            < lax.broadcasted_iota(jnp.int32, (tokens, tokens), 1)
        ).astype(bf16)
        ranks = jnp.where(named > 0, dot(named.astype(bf16), strict), -1.0)
        packed_ref[tokens : tokens + extra, :] = jnp.full((extra, part), -1.0, bf16)
        packed_ref[tokens : tokens + extra, 0:tokens] = ranks.astype(bf16)
        packed_ref[tokens : tokens + extra, pad : pad + tokens] = share.astype(bf16)
        for copy in takes:
            copy.wait()

    outs = [
        jax.ShapeDtypeStruct((tokens, width), bf16),
        jax.ShapeDtypeStruct((tokens + extra, part), bf16),
    ]
    outs += [jax.ShapeDtypeStruct((size, weight.shape[1]), weight.dtype) for _ in wanted]
    operands = (rows, gain[None, :], index.T, scores.T, weight)
    scratch = [pltpu.VMEM(v.shape, v.dtype) for v in operands[:4]]
    scratch += [pltpu.SemaphoreType.DMA((4,)), pltpu.SemaphoreType.DMA((len(wanted),))]
    normed, packed, *taken = call(body, outs, operands, 1 << 22, scratch=scratch, far=5)
    return normed, packed, taken


def group_of(sources, capacity):
    group = 1
    while group < sources and group * capacity % 16:
        group *= 2
    return group


def expert_up(places, own, far, capacity, gate_weight, up_weight):
    parts = len(far[0])
    tokens, width = own[0].shape
    packed_rows, piece = own[1].shape
    extra = packed_rows - tokens
    pad = -(-tokens // 128) * 128
    sources = 1 + len(far)
    slots = sources * capacity
    group = group_of(sources, capacity)
    hidden = gate_weight.shape[1]
    step = min(256, hidden)
    flat = list(own) + [p for pieces in far for p in pieces]

    def body(*refs):
        row_refs = refs[: len(flat)]
        gate_ref, up_ref, out_ref, info_ref, rows_ref, section_ref = refs[len(flat) :]
        here = Here(places)
        expert = lax.broadcasted_iota(jnp.int32, (extra, 2 * pad), 0) == here.e
        if pad > tokens:
            for s in range(sources):
                rows_ref[s * pad + tokens : (s + 1) * pad, :] = jnp.zeros((pad - tokens, width), bf16)
        rows_ref[0:tokens, :] = row_refs[0][...]
        for q in range(parts):

            @pl.when(here.part == q)
            def _():
                for s in range(1, sources):
                    for i in range(parts):
                        to = (q - i) % parts
                        rows_ref[s * pad : s * pad + tokens, to * piece : (to + 1) * piece] = (
                            row_refs[2 + (s - 1) * parts + i][0:tokens, :]
                        )

        for s0 in range(0, sources, group):
            targets = []
            for s in range(s0, s0 + group):
                table_ref = row_refs[2 + (s - 1) * parts if s else 1]
                table = table_ref[tokens : tokens + extra, 0 : 2 * pad].astype(f32)
                mine = jnp.sum(jnp.where(expert, table, 0.0), axis=0, keepdims=True)
                info_ref[s : s + 1, :] = mine
                rank = mine[:, 0:pad]
                targets.append(jnp.where(rank >= 0, rank + (s - s0) * capacity, -1.0))
            target = jnp.concatenate(targets, axis=1) if group > 1 else targets[0]
            slot = lax.broadcasted_iota(jnp.int32, (group * capacity, group * pad), 0)
            picks = (slot.astype(f32) == target).astype(bf16)
            section_ref[s0 * capacity : (s0 + group) * capacity, :] = dot(
                picks, rows_ref[s0 * pad : (s0 + group) * pad, :]
            ).astype(bf16)
        for h in range(0, hidden, step):
            section = section_ref[...]
            gate_value = dot(section, gate_ref[:, h : h + step])
            up_value = dot(section, up_ref[:, h : h + step])
            out_ref[:, h : h + step] = (silu(gate_value) * up_value).astype(bf16)

    outs = (
        jax.ShapeDtypeStruct((slots, hidden), bf16),
        jax.ShapeDtypeStruct((sources, 2 * pad), f32),
    )
    scratch = (pltpu.VMEM((sources * pad, width), bf16), pltpu.VMEM((slots, width), bf16))
    operands = (*flat, gate_weight, up_weight)
    return call(body, outs, operands, 4 * slots * width * hidden, scratch=scratch)


def load(weights):
    count = len(weights)

    def body(*refs):
        done = refs[-1]
        copies = [
            pltpu.make_async_copy(refs[i], refs[count + i], done.at[i]) for i in range(count)
        ]
        for copy in copies:
            copy.start()
        for copy in copies:
            copy.wait()

    outs = [jax.ShapeDtypeStruct(w.shape, w.dtype) for w in weights]
    scratch = (pltpu.SemaphoreType.DMA((count,)),)
    return call(body, outs, weights, 1 << 20, scratch=scratch, far=count)


def dot_pieces(ref, pieces):
    size = pieces[0].shape[0]
    return sum(dot(ref[:, p * size : (p + 1) * size], piece[...]) for p, piece in enumerate(pieces))


def down_first(places, hiddens, weight, traded):
    hidden, columns = hiddens[0].shape[1], weight.shape[1]
    chunks, partners = len(hiddens), len(traded)
    traded = [piece for pieces in traded for piece in pieces]

    def body(*refs):
        outs = refs[chunks + 1 + len(traded) :]
        weight = rows_of(refs[chunks], Here(places).column(0, 0), hidden)
        for h in range(chunks):
            outs[h][...] = dot(refs[h][...], weight)
            for w in range(partners):
                first = chunks + 1 + w * PIECES
                outs[(w + 1) * chunks + h][...] = dot_pieces(
                    refs[h], refs[first : first + PIECES]
                )

    shapes = [
        jax.ShapeDtypeStruct((h.shape[0], columns), f32) for _ in range(1 + partners) for h in hiddens
    ]
    flops = 2 * sum(h.shape[0] for h in hiddens) * hidden * columns * (1 + partners)
    outs = call(body, shapes, (*hiddens, weight, *traded), flops)
    return [outs[w * chunks : (w + 1) * chunks] for w in range(1 + partners)]


def down_partner(first, hiddens, weights):
    count = len(hiddens)

    def body(first_ref, *refs):
        total = first_ref[...]
        for i in range(count):
            first = count + i * PIECES
            total = total + dot_pieces(refs[i], refs[first : first + PIECES])
        refs[-1][...] = total.astype(bf16)

    out = jax.ShapeDtypeStruct(first.shape, bf16)
    flops = 2 * first.size * hiddens[0].shape[1] * count
    pieces = [piece for slices in weights for piece in slices]
    return call(body, out, (first, *hiddens, *pieces), flops)


def down_own(places, firsts, gathered, weight):
    count, chunks = len(gathered), len(firsts)
    hidden, columns = gathered[0][0].shape[1], weight.shape[1]

    def body(*refs):
        hidden_refs = refs[chunks : chunks + count * chunks]
        weight_ref = refs[chunks + count * chunks]
        outs = refs[chunks + count * chunks + 1 :]
        here = Here(places)
        for h in range(chunks):
            total = refs[h][...]
            for i in range(count):
                rows = rows_of(weight_ref, here.column(-1 - i, 0), hidden)
                total = total + dot(hidden_refs[i * chunks + h][...], rows)
            outs[h][...] = total

    flat = [h for pieces in gathered for h in pieces]
    outs = [jax.ShapeDtypeStruct(f.shape, f32) for f in firsts]
    flops = 2 * sum(h.shape[0] for h in flat) * hidden * columns
    return call(body, outs, (*firsts, *flat, weight), flops)


def combine(own, back, info, tokens, capacity, out_type):
    slots, columns = own.shape
    sources = slots // capacity
    pad = info.shape[1] // 2
    group = group_of(sources, capacity)

    def body(own_ref, info_ref, *refs):
        out_ref = refs[-1]
        for s0 in range(0, sources, group):
            span = slice(s0 * capacity, (s0 + group) * capacity)
            value = own_ref[span, :]
            for ref in refs[:-1]:
                value = value + ref[span, :].astype(f32)
            value = value.astype(bf16)
            for s in range(s0, s0 + group):
                rank = info_ref[s : s + 1, 0:pad]
                target = jnp.where(rank >= 0, rank + (s - s0) * capacity, -1.0)
                slot = lax.broadcasted_iota(jnp.int32, (group * capacity, pad), 0).astype(f32)
                places = jnp.where(slot == target, info_ref[s : s + 1, pad : 2 * pad], 0.0)
                out_ref[s] = dot_tn(places.astype(bf16), value)[0:tokens].astype(out_type)

    out = jax.ShapeDtypeStruct((sources, tokens, columns), out_type)
    return call(body, out, (own, info, *back), 1 << 26)


def local(
    first_batch_queries,
    first_batch_keys,
    first_batch_values,
    output_gate_preactivation,
    decay_preactivation,
    channel_decay_bias,
    added_log_decay,
    head_norm_gain,
    attention_output_weight,
    second_batch_rows,
    expert_norm_gain,
    routed_expert_index,
    router_chosen_scores,
    expert_gate_weight,
    expert_up_weight,
    expert_down_weight,
    shared_gate_weight,
    shared_up_weight,
    shared_down_weight,
):
    at = Places()
    n, chips, experts = at.side, at.chips, at.ep
    heads = added_log_decay.shape[0]
    tokens, top_count = routed_expert_index.shape
    capacity = tokens * top_count * 3 // (2 * experts)
    gate_weight, up_weight, down_weight = (
        expert_gate_weight[0],
        expert_up_weight[0],
        expert_down_weight[0],
    )
    hidden = gate_weight.shape[1]

    traded = [[[] for _ in range(n)] for _ in range(1, n)]
    lacking = [(i, piece) for i in range(n) for piece in range(PIECES)]
    wanted = [(i, k, piece) for i, piece in lacking for k in range(1, n)]
    quarter = len(wanted) // 4

    def trade(number):
        for at_piece in range(number * quarter, (number + 1) * quarter):
            i, k, _ = wanted[at_piece]
            traded[k - 1][i].append(at.along_v(taken[at_piece], k))

    normed, packed, taken = prepare_rows(
        at,
        n,
        second_batch_rows,
        expert_norm_gain,
        routed_expert_index,
        router_chosen_scores,
        experts,
        down_weight,
        [(-i, k, piece) for i, k, piece in wanted],
        hidden,
    )
    middle = chips // 2
    far = {middle: at.along_z(packed, middle)}
    trade(0)
    trade(1)
    far |= {k: at.along_z(packed, k) for k in range(1, chips) if k != middle}
    trade(2)
    o_local, q_device, own_state = local_attention(
        first_batch_queries,
        first_batch_keys,
        first_batch_values,
        decay_preactivation,
        channel_decay_bias,
        added_log_decay,
    )
    arrived = [at.along_z(own_state, hop) for hop in range(1, chips)]
    states = [at.to_sibling(own_state)]
    for state in arrived:
        states += [state, at.to_sibling(state)]
    parts = [far[k] for k in range(1, chips)]
    far = [[a] + [at.along_u(a, i) for i in range(1, n)] for a in parts]
    other = ((at.to_sibling(normed), at.to_sibling(packed)), [[at.to_sibling(a)] for a in parts])
    for pieces, others in zip(far, other[1]):
        others += [at.to_sibling(p) for p in pieces[1:]]
    trade(3)
    gate_weight, up_weight = load((gate_weight, up_weight))
    ups = [expert_up(at, (normed, packed), far, capacity, gate_weight, up_weight)]
    gathered_first = [at.along_u(ups[0][0], i) for i in range(1, n)]
    _, other = hold((ups[0][0], other))
    ups.append(expert_up(at, *other, capacity, gate_weight, up_weight))
    hiddens = [up[0] for up in ups]
    gathered_second = [at.along_u(hiddens[1], i) for i in range(1, n)]
    both = finish_attention(
        at,
        o_local,
        q_device,
        states,
        output_gate_preactivation,
        head_norm_gain,
        heads,
        normed,
        shared_gate_weight,
        shared_up_weight,
    )
    firsts = down_first(at, hiddens, down_weight, [t[0] for t in traded])

    def partials(chunk, gathered):
        return [
            down_partner(firsts[k][chunk], gathered, traded[k - 1][1:]) for k in range(1, n)
        ]

    partial = partials(0, gathered_first)
    back = [[at.along_v(partial[k - 1], -k) for k in range(1, n)]]
    gathered_second, both, _ = hold((gathered_second, both, partial))
    partial = partials(1, gathered_second)
    back.append([at.along_v(partial[k - 1], -k) for k in range(1, n)])
    gathered = [list(pair) for pair in zip(gathered_first, gathered_second)]
    owns = down_own(at, firsts[0], gathered, down_weight)
    here = combine(owns[0], back[0], ups[0][1], tokens, capacity, f32)
    there = combine(owns[1], back[1], ups[1][1], tokens, capacity, bf16)
    from_sibling = at.to_sibling(there)
    chip_sum = here + from_sibling.astype(f32)
    routed_total = chip_sum[0]
    for k in range(1, chips):
        routed_total = routed_total + at.along_z(chip_sum[k].astype(bf16), -k).astype(f32)

    mixed = [
        both if dy == 0 and dx == 0 else at.along_tp(both, dy, dx)
        for dy in range(n)
        for dx in range(n)
    ]
    token_mixed, shared_total = project(
        at, mixed, attention_output_weight, shared_down_weight, tokens
    )
    channel_mixed = (routed_total + shared_total).astype(bf16)
    return (token_mixed, channel_mixed)


def solution(mesh):
    placed = (
        P("ep", "tp"),
        P("ep", "tp"),
        P("ep", "tp"),
        P("ep", "tp"),
        P("ep", "tp"),
        P("tp"),
        P("tp", "ep"),
        P("tp"),
        P(None, "tp"),
        P("ep", None),
        P(),
        P("ep", None),
        P("ep", None),
        P("ep", None, "tp"),
        P("ep", None, "tp"),
        P("ep", None, "tp"),
        P(None, "tp"),
        P(None, "tp"),
        P(None, "tp"),
    )

    return jax.shard_map(
        local, mesh=mesh, in_specs=placed, out_specs=(P("ep", "tp"), P("ep", "tp")), check_vma=False
    )
```
